32 devices in a mesh: sp: 8 (over z, core), tp: 4 (over y, x).
Axes of the slice: x: 2, y: 2, z: 4, core: 2. Of those that a mesh axis runs over, the one named last changes fastest.
Arguments:
- moe_input: bfloat16 [1024, 2048], P('sp', 'tp'), may hold values from -6 to 6
- cotangent: bfloat16 [1024, 2048], P('sp', 'tp'), may hold values from -6 to 6
- routes: int32 [1024, 2], P('sp'), may hold values from 0 to 7, all different within a row; in each aligned block of 128 rows (0 to 127, 128 to 255, ...) at most 40 rows name the same one
- route_weights: float32 [1024, 2], P('sp'), may hold values from 0.2 to 1
- gate_branch: bfloat16 [1024, 2560], P('sp', 'tp'), may hold values from -6 to 6
- log_decay: float32 [1024, 2560], P('sp', 'tp'), may hold values from -0.12 to 0
- states: float32 [1024, 2560], P('sp', 'tp'), may hold values from -6 to 6
- w_gate: bfloat16 [8, 2048, 2048], P('sp', None, 'tp'), may hold values from -0.125 to 0.125
- w_up: bfloat16 [8, 2048, 2048], P('sp', None, 'tp'), may hold values from -0.125 to 0.125
- w_down: bfloat16 [8, 2048, 2048], P('sp', 'tp'), may hold values from -0.125 to 0.125
- out_proj: bfloat16 [2048, 2560], P('sp', 'tp'), may hold values from -0.125 to 0.125
Outputs:
- grad_w_gate: float32 [8, 2048, 2048], P('sp', None, 'tp')
- grad_w_up: float32 [8, 2048, 2048], P('sp', None, 'tp')
- grad_w_down: float32 [8, 2048, 2048], P('sp', 'tp')
- grad_out_proj: float32 [2048, 2560], P('sp', 'tp')
- grad_gate_branch: bfloat16 [1024, 2560], P('sp', 'tp')
- grad_log_decay: bfloat16 [1024, 2560], P('sp', 'tp')
- grad_input_term: float32 [1024, 2560], P('sp', 'tp')
The draws below stay inside these ranges and needn't reach their ends.
Inputs may be any that keep to these rules, and one draw needn't show every extreme that they name: `routes`: in the rows of one device no expert is named by more than 40 entries, and in every draw some expert is named by exactly 40 entries of one device's rows.
All inputs are finite; a program needn't handle non-finite values.
Results may differ from the reference program's by a relative error of at most 0.025.
Values may be sent and summed in bfloat16 or wider, within the bound.
A program may use at most 64 MiB of HBM per device.

```python
import math
import jax
import jax.numpy as jnp
import numpy as np
from jax import lax

D = 2048
W = 2560
F = 2048
TOP = 2
TOK_DEV = 128
EXPERTS = 8
TOKENS = 1024
CAP = 40
N_SP = 8
N_TP = 4


def draw_log_decay(key, part):
    key_kind, key_rate, key_block, key_cell = jax.random.split(key, 4)
    slow_share = 50
    slow_mask = jax.random.randint(key_kind, (W,), 0, 100) < slow_share
    slow_rate = jax.random.uniform(key_rate, (W,), jnp.float32, 0.3, 0.5) * math.log(10.0) / TOKENS
    fast_rate = jax.random.uniform(jax.random.fold_in(key_rate, 7), (W,), jnp.float32, 1.0 / 60.0, 1.0 / 25.0)
    chan_rates = jnp.where(slow_mask, slow_rate, fast_rate)
    block_scale = jnp.exp(jax.random.uniform(key_block, (TOKENS // TOK_DEV, W), jnp.float32, -math.log(2.0), math.log(2.0)))
    block_scale = jnp.repeat(block_scale, TOK_DEV, axis=0)
    cell_scale = jax.random.uniform(key_cell, (TOKENS, W), jnp.float32, 0.5, 1.5)
    return -(chan_rates[None, :] * block_scale * cell_scale)


def strengthened(entries, rng, source, target, blocks, factor):
    owner, partner = [(jnp.arange(entries.shape[position]) // (entries.shape[position] // blocks)).reshape([-1 if axis == position else 1 for axis in range(entries.ndim)]) for position in (source, target)]
    chosen = jax.random.permutation(rng, blocks)[partner]
    strong = (owner == chosen) | (owner == (partner + blocks // 2) % blocks)
    return jnp.where(strong, factor * entries, entries)


def shard_levels(key, dims, cuts, smallest, largest):
    loudness, own = 1.0, jax.random.fold_in(key, 6)
    for dim, blocks in cuts:
        heights = jnp.exp(jax.random.uniform(jax.random.fold_in(own, dim), (blocks,), jnp.float32, smallest / len(cuts), largest / len(cuts)))
        loudness = loudness * jnp.repeat(heights, dims[dim] // blocks).reshape([-1 if axis == dim else 1 for axis in range(len(dims))])
    return loudness


def deal_out(own_key, own, number, rows, count, top, bound, lean):
    ranking = jax.random.permutation(own_key, count)
    heavy_load, ordinary = load_shares(count, rows * top, bound, lean, True), load_shares(count, rows * top, bound, lean, False)
    places = jnp.arange(count)

    def named(lengths, turn):
        used = int((lengths > 0).sum())
        fixed = max(1, used // 4)
        moved = fixed + (places - fixed + turn * (used - fixed)) % max(1, count - fixed)
        return jnp.zeros((count,), jnp.int32).at[ranking[jnp.where(places < fixed, places, moved)]].set(jnp.asarray(lengths, jnp.int32))

    lengths = jnp.where(number % 4 == 0, named(heavy_load, number // 4), named(ordinary, number - number // 4 - 1))
    mixed = jax.random.permutation(jax.random.fold_in(own, 3), count)
    source_of, taker = mixed[0:count // 2 * 2:2], mixed[1:count // 2 * 2:2]
    slack = jnp.minimum(lengths[source_of] - 1, bound - lengths[taker]) // 2
    slack = jnp.where((source_of == ranking[0]) | (taker == ranking[0]) | (lengths[taker] == 0), 0, jnp.maximum(slack, 0))
    moved = jax.random.randint(jax.random.fold_in(own, 4), (count // 2,), 0, 1 << 20) % (slack + 1)
    lengths = lengths.at[source_of].add(-moved).at[taker].add(moved)
    items = jnp.searchsorted(jnp.cumsum(lengths), jnp.arange(rows * top), side="right").astype(jnp.int32)
    listing = items.reshape(top, rows).T
    listing = listing[jax.random.permutation(jax.random.fold_in(own, 1), rows)]
    turn = jax.random.randint(jax.random.fold_in(own, 2), (rows, 1), 0, top)
    return jnp.take_along_axis(listing, (jnp.arange(top)[None, :] + turn) % top, axis=1)


def load_shares(amount, total, limit, skew, full):
    weights = [(1 << 20) // math.isqrt(standing ** skew) + 1 for standing in range(1, amount + 1)]
    largest = limit if full else min(limit, max(-(-total // amount), total * weights[0] // sum(weights)))
    least = 1 if total - largest >= amount - 1 else 0
    counts, spare = [largest] + [least] * (amount - 1), total - largest - least * (amount - 1)
    while spare > 0:
        free = [i for i in range(1, amount) if counts[i] < largest] or [i for i in range(1, amount) if counts[i] < limit]
        whole, budget = sum([weights[i] for i in free]), spare
        for i in free:
            extra = min(limit - counts[i], max(1, budget * weights[i] // whole), spare)
            counts[i] = counts[i] + extra
            spare = spare - extra
    return np.array(counts)


def gaussian(stream_key, shape, width, bound, cuts=(), kind=jnp.bfloat16):
    result = width * jax.random.normal(stream_key, shape, jnp.float32)
    if cuts:
        result = result * shard_levels(stream_key, shape, cuts, -0.22, 0.18)
    return jnp.clip(result, -bound, bound).astype(kind)


def noise_with(key, shape, deviation, reach, cuts, heavy, kind=jnp.bfloat16):
    result = deviation * jax.random.normal(key, shape, jnp.float32)
    if cuts:
        result = result * shard_levels(key, shape, cuts, -0.22, 0.18)
    return jnp.clip(strengthened(result, jax.random.fold_in(key, 3), *heavy), -reach, reach).astype(kind)


def setup_inputs(seed: int = 0) -> dict:
    key_list = jax.random.split(jax.random.key(seed), 12)
    moe_input = gaussian(key_list[0], (TOKENS, D), 1.0, 6.0, ((0, 8), (1, 4)))
    cotangent = noise_with(key_list[1], (TOKENS, D), 1.0, 6.0, ((0, 8), (1, 4)), (0, 1, 8, 2.0))
    routes_keys = jax.random.split(jax.random.fold_in(key_list[2], 1), TOKENS // TOK_DEV)
    routes_turns = jax.random.permutation(jax.random.fold_in(key_list[2], 3), TOKENS // TOK_DEV)
    routes = jax.vmap(lambda own, number: deal_out(jax.random.fold_in(key_list[2], 2), own, number, TOK_DEV, EXPERTS, TOP, CAP, 2))(routes_keys, routes_turns).reshape((TOKENS, TOP))
    route_weights = jnp.clip(0.2 + 0.8 * jax.random.uniform(key_list[3], (TOKENS, TOP), jnp.float32) ** shard_levels(key_list[3], (TOKENS, TOP), ((0, 8),), -0.2, 0.2), 0.2, 1.0)
    gate_branch = gaussian(key_list[4], (TOKENS, W), 1.0, 6.0, ((0, 8), (1, 4)))
    log_decay = draw_log_decay(jax.random.fold_in(key_list[11], 71), 0)
    states = gaussian(key_list[6], (TOKENS, W), 1.0, 6.0, ((0, 8), (1, 4)), jnp.float32)
    w_gate = gaussian(key_list[7], (EXPERTS, D, F), D ** -0.5, 0.125, ((0, 8), (2, 4)))
    w_up = gaussian(key_list[8], (EXPERTS, D, F), D ** -0.5, 0.125, ((0, 8), (2, 4)))
    w_down = gaussian(key_list[9], (EXPERTS, F, D), F ** -0.5, 0.125, ((0, 8), (1, 4)))
    out_proj = gaussian(key_list[10], (D, W), W ** -0.5, 0.125, ((0, 8), (1, 4)))
    return dict(moe_input=moe_input, cotangent=cotangent, routes=routes, route_weights=route_weights, gate_branch=gate_branch, log_decay=log_decay, states=states, w_gate=w_gate, w_up=w_up, w_down=w_down, out_proj=out_proj)


def silu_parts(pre_gate):
    sigmoid_val = jax.nn.sigmoid(pre_gate)
    return (pre_gate * sigmoid_val, sigmoid_val * (1.0 + pre_gate * (1.0 - sigmoid_val)))

def combine_pair(left_pair, right_pair):
    return (left_pair[0] * right_pair[0], right_pair[0] * left_pair[1] + right_pair[1])

def expert_backward(row_data, scaled, gate_w, up_w, down_w):
    pre_gate = jnp.dot(row_data, gate_w, preferred_element_type=jnp.float32)
    pre_up = jnp.dot(row_data, up_w, preferred_element_type=jnp.float32)
    active, slope = silu_parts(pre_gate)
    hidden = (active * pre_up).astype(jnp.bfloat16)
    grad_down = jnp.dot(hidden.T, scaled, preferred_element_type=jnp.float32)
    grad_hidden = jnp.dot(scaled, down_w.T, preferred_element_type=jnp.float32)
    grad_pre_gate = (grad_hidden * pre_up * slope).astype(jnp.bfloat16)
    grad_pre_up = (grad_hidden * active).astype(jnp.bfloat16)
    grad_gate_w = jnp.dot(row_data.T, grad_pre_gate, preferred_element_type=jnp.float32)
    grad_up_w = jnp.dot(row_data.T, grad_pre_up, preferred_element_type=jnp.float32)
    row_total = grad_pre_gate.shape[0]
    blocked_gate = grad_pre_gate.reshape(row_total, N_TP, F // N_TP).astype(jnp.float32)
    blocked_up = grad_pre_up.reshape(row_total, N_TP, F // N_TP).astype(jnp.float32)
    weight_gate = gate_w.reshape(D, N_TP, F // N_TP).astype(jnp.float32)
    weight_up = up_w.reshape(D, N_TP, F // N_TP).astype(jnp.float32)
    block_terms = jnp.einsum('nbf,dbf->bnd', blocked_gate, weight_gate) + jnp.einsum('nbf,dbf->bnd', blocked_up, weight_up)
    rounded = lax.optimization_barrier(block_terms.astype(jnp.bfloat16))
    entry_grad = lax.optimization_barrier(jnp.sum(rounded.astype(jnp.float32), axis=0)).astype(jnp.bfloat16)
    return (grad_gate_w, grad_up_w, grad_down, entry_grad)

def reference(moe_input, cotangent, routes, route_weights, gate_branch, log_decay, states, w_gate, w_up, w_down, out_proj):
    flat_routes = routes.reshape(-1).astype(jnp.int32)
    flat_weights = route_weights.reshape(-1)
    owners = jnp.arange(TOKENS * TOP, dtype=jnp.int32) // TOP
    room = N_SP * CAP

    def per_expert(totals, inputs):
        expert, gate_w, up_w, down_w = inputs
        sorted_idx = jnp.argsort((flat_routes != expert).astype(jnp.int32), stable=True)[:room].astype(jnp.int32)
        live_rows = (flat_routes[sorted_idx] == expert).astype(jnp.float32)
        token_idx = owners[sorted_idx]
        row_data = moe_input[token_idx]
        scaled = ((live_rows * flat_weights[sorted_idx])[:, None] * cotangent[token_idx].astype(jnp.float32)).astype(jnp.bfloat16)
        grad_gate_w, grad_up_w, grad_down, entry_grad = expert_backward(row_data, scaled, gate_w, up_w, down_w)
        totals = totals.at[token_idx].add(entry_grad.astype(jnp.float32) * live_rows[:, None])
        return (totals, (grad_gate_w, grad_up_w, grad_down))
    totals, grads = lax.scan(per_expert, jnp.zeros((TOKENS, D), jnp.float32), (jnp.arange(EXPERTS, dtype=jnp.int32), w_gate, w_up, w_down))
    grad_w_gate, grad_w_up, grad_w_down = grads
    grad_tokens = (cotangent.astype(jnp.float32) + totals).astype(jnp.bfloat16)
    active_gate, pullback = jax.vjp(jax.nn.gelu, gate_branch.astype(jnp.float32))
    mixed_in = (active_gate * states).astype(jnp.bfloat16)
    grad_out_proj = jnp.dot(grad_tokens.T, mixed_in, preferred_element_type=jnp.float32)
    grad_mixed = jnp.dot(grad_tokens, out_proj, preferred_element_type=jnp.float32)
    grad_gate_branch = pullback(grad_mixed * states)[0].astype(jnp.bfloat16)
    grad_state = grad_mixed * active_gate
    decays = jnp.exp(log_decay)
    next_decay = jnp.concatenate([decays[1:], jnp.zeros_like(decays[:1])], axis=0)
    _, back_flip = lax.associative_scan(combine_pair, (jnp.flip(next_decay, 0), jnp.flip(grad_state, 0)))
    grad_input_term = jnp.flip(back_flip, 0)
    prev_states = jnp.concatenate([jnp.zeros_like(states[:1]), states[:-1]], axis=0)
    grad_log_decay = (grad_input_term * decays * prev_states).astype(jnp.bfloat16)
    return (grad_w_gate, grad_w_up, grad_w_down, grad_out_proj, grad_gate_branch, grad_log_decay, grad_input_term)
```

```python
import jax
import jax.numpy as jnp
from jax import lax
from jax.experimental import pallas as pl
from jax.experimental.pallas import tpu as pltpu
from jax.sharding import PartitionSpec as P

BF = jnp.bfloat16
F32 = jnp.float32
CORES = 2
GELU_C = 0.7978845608028654
GELU_A = 0.044715


def silu_parts(pre_gate):
    sigmoid_val = jax.nn.sigmoid(pre_gate)
    return (pre_gate * sigmoid_val, sigmoid_val * (1.0 + pre_gate * (1.0 - sigmoid_val)))


def contract_rows(left_mat, right_mat):
    return lax.dot_general(
        left_mat, right_mat, (((0,), (0,)), ((), ())), preferred_element_type=F32
    )


def contract_cols(left_mat, right_mat):
    return lax.dot_general(
        left_mat, right_mat, (((1,), (1,)), ((), ())), preferred_element_type=F32
    )


def gelu_parts(x):
    t = jnp.tanh(GELU_C * (x + GELU_A * (x * x * x)))
    half = 0.5 * (1.0 + t)
    slope = half + 0.5 * x * (1.0 - t * t) * (GELU_C * (1.0 + 3.0 * GELU_A * x * x))
    return x * half, slope


def selection(routes_t, weights_t, groups, room):
    picks, toks = routes_t.shape
    experts = lax.broadcasted_iota(jnp.int32, (groups, toks), 0)
    named = jnp.zeros((groups, toks), F32)
    weight = jnp.zeros((groups, toks), F32)
    for k in range(picks):
        hit = routes_t[k : k + 1, :] == experts
        named = named + jnp.where(hit, 1.0, 0.0)
        weight = weight + jnp.where(hit, weights_t[k : k + 1, :], 0.0)
    rows = lax.broadcasted_iota(jnp.int32, (toks, toks), 0)
    cols = lax.broadcasted_iota(jnp.int32, (toks, toks), 1)
    before = jnp.where(rows < cols, 1.0, 0.0).astype(BF)
    slot = jnp.dot(named.astype(BF), before, preferred_element_type=F32)
    slot = jnp.where(named > 0.5, slot, -1.0)
    place = lax.broadcasted_iota(jnp.int32, (room, toks), 0).astype(F32)
    picked, column = [], []
    for e in range(groups):
        one = jnp.where(slot[e : e + 1, :] == place, 1.0, 0.0)
        picked.append(one)
        column.append(jnp.sum(one * weight[e : e + 1, :], axis=1, keepdims=True))
    return jnp.concatenate(picked, axis=0).astype(BF), jnp.concatenate(column, axis=0)


def greet(groups, parts, mine, col):
    barrier = pltpu.get_barrier_semaphore()
    for d in range(1, groups):
        pl.semaphore_signal(
            barrier, inc=1, device_id={"sp": lax.rem(mine + d, groups)},
            device_id_type=pl.DeviceIdType.MESH,
        )
    for d in range(1, parts):
        pl.semaphore_signal(
            barrier, inc=1, device_id={"tp": lax.rem(col + d, parts)},
            device_id_type=pl.DeviceIdType.MESH,
        )
    pl.semaphore_wait(barrier, groups + parts - 2)


def remote(src, dst, send, recv, axis, peer):
    return pltpu.make_async_remote_copy(
        src_ref=src, dst_ref=dst, send_sem=send, recv_sem=recv,
        device_id={axis: peer}, device_id_type=pl.DeviceIdType.MESH,
    )


def whole_kernel(
    groups, parts, room, chunked,
    routes_ref, weights_ref, x_any, cot_any, gate_any, states_any, decay_any, proj_any,
    wg_any, wu_any, wd_any,
    rx_ref, rc_ref, hid_ref, gpg_ref, gpu_ref, outp_ref, ggate_ref, gdecay_ref, gin_ref,
    x_ref, cot_ref, gate_ref, states_ref, decay_ref, wg, wu, wd,
    out_x, out_c, rows_x, rows_c, proj_all, mixed_all, mix_own, acts,
    terms, shares, summed, back, flipped, blocks, carry_own, carry_in, prev_in,
    a_send, a_recv, t_send, t_recv, z_send, z_recv, c_send, c_recv,
    s_send, s_recv, r_send, r_recv, g_send, g_recv, b_send, b_recv, k_send, k_recv, p_send, p_recv,
    l_sem, w_sem,
):
    mine, col = lax.axis_index("sp"), lax.axis_index("tp")
    toks, width = x_ref.shape
    model = rows_x.shape[2]
    depth = groups // CORES
    z, core = mine // CORES, lax.rem(mine, CORES)
    size = groups * room

    def near(width_of, index):
        return pl.ds(pl.multiple_of(index * width_of, width_of), width_of)

    loads = []
    for i, (s, t) in enumerate((
        (x_any, x_ref), (cot_any, cot_ref), (gate_any, gate_ref), (states_any, states_ref),
        (proj_any, proj_all.at[mine]), (decay_any, decay_ref),
        (wg_any.at[0], wg), (wu_any.at[0], wu), (wd_any.at[0], wd),
    )):
        o = pltpu.make_async_copy(s, t, l_sem.at[i])
        o.start()
        loads.append(o)

    picked, weight = selection(routes_ref[...], weights_ref[...], groups, room)
    loads[0].wait()
    got = jnp.dot(picked, x_ref[...], preferred_element_type=F32).astype(BF)
    for e in range(groups):
        out_x[e] = got[e * room : (e + 1) * room]
    loads[1].wait()
    got_c = jnp.dot(picked, cot_ref[...], preferred_element_type=F32)
    got_c = (got_c * weight).astype(BF)
    for e in range(groups):
        out_c[e] = got_c[e * room : (e + 1) * room]
    greet(groups, parts, mine, col)

    here = near(width, col)
    sends, own = [], []
    arrivals = [[None] * groups for _ in range(2)]
    for a, (src, dst) in enumerate(((out_x, rows_x), (out_c, rows_c))):
        for d in range(1, groups):
            peer = lax.rem(mine + d, groups)
            c = remote(src.at[peer], dst.at[mine, :, here], a_send.at[a, d], a_recv.at[a, d], "sp", peer)
            c.start()
            arrivals[a][d] = c
            sends.append(c)
        o = pltpu.make_async_copy(src.at[mine], dst.at[mine, :, here], w_sem.at[a])
        o.start()
        own.append(o)

    pairs = (proj_all, mixed_all)

    def chain(a, step, wait=False):
        buf = pairs[a]
        right = buf.at[jnp.maximum(z - step, 0) * CORES + core]
        left = buf.at[jnp.minimum(z + step, depth - 1) * CORES + core]
        up = jnp.minimum(z + 1, depth - 1) * CORES + core
        down = jnp.maximum(z - 1, 0) * CORES + core
        for way, ref, peer, ok in (
            (0, right, up, jnp.logical_and(z - step >= 0, z + 1 < depth)),
            (1, left, down, jnp.logical_and(z + step < depth, z >= 1)),
        ):
            @pl.when(ok)
            def _(way=way, ref=ref, peer=peer):
                c = remote(ref, ref, z_send.at[a, way, step], z_recv.at[a, way, step], "sp", peer)
                c.wait_send() if wait else c.start()

    partner = z * CORES + (1 - core)

    def across(a, step, way, mode):
        ok = z - step >= 0 if way == 0 else z + step < depth
        zz = jnp.maximum(z - step, 0) if way == 0 else jnp.minimum(z + step, depth - 1)
        ref = pairs[a].at[zz * CORES + (1 - core if mode == "recv" else core)]

        @pl.when(ok)
        def _():
            c = remote(ref, ref, c_send.at[a, way, step], c_recv.at[a, way, step], "sp", partner)
            if mode == "start":
                c.start()
            elif mode == "send":
                c.wait_send()
            else:
                c.wait_recv()

    def advance(a, step):
        buf = pairs[a]
        from_l = buf.at[jnp.maximum(z - 1 - step, 0) * CORES + core]
        from_r = buf.at[jnp.minimum(z + 1 + step, depth - 1) * CORES + core]
        for way, ok, ref in ((0, z - 1 - step >= 0, from_l), (1, z + 1 + step < depth, from_r)):
            @pl.when(ok)
            def _(way=way, ref=ref):
                remote(ref, ref, z_send.at[a, way, step], z_recv.at[a, way, step],
                       "sp", lax.rem(mine + 1, groups)).wait_recv()
        if step + 1 < depth - 1:
            chain(a, step + 1)
        across(a, step + 1, 0, "start")
        across(a, step + 1, 1, "start")

    def settle(a):
        for step in range(depth - 1):
            chain(a, step, True)
        for step in range(depth):
            for way in range(2):
                if step or not way:
                    across(a, step, way, "send")

    def collected(a):
        for step in range(depth):
            for way in range(2):
                if step or not way:
                    across(a, step, way, "recv")

    loads[4].wait()
    chain(0, 0)
    across(0, 0, 0, "start")

    gathers = [[], []]

    def gather(a, src, dst):
        if chunked:
            for d in range(groups):
                at = lax.rem(mine + groups - d, groups)
                if d:
                    arrivals[a][d].wait_recv()
                for p in range(1, parts):
                    c = remote(dst.at[at, :, here] if d else src.at[mine], dst.at[at, :, here],
                               t_send.at[a, d, p], t_recv.at[a, d, p], "tp", lax.rem(col + p, parts))
                    c.start()
                    gathers[a].append(c)
            own[a].wait()
        else:
            own[a].wait()
            for d in range(1, groups):
                arrivals[a][d].wait_recv()
            for p in range(1, parts):
                c = remote(dst.at[:, :, here], dst.at[:, :, here],
                           t_send.at[a, 0, p], t_recv.at[a, 0, p], "tp", lax.rem(col + p, parts))
                c.start()
                gathers[a].append(c)
        sends.extend(gathers[a])

    gather(0, out_x, rows_x)
    loads[2].wait()
    loads[3].wait()
    act, branch_slope = gelu_parts(gate_ref[...].astype(F32))
    mix_own[...] = (act * states_ref[...]).astype(BF)
    gather(1, out_c, rows_c)
    o = pltpu.make_async_copy(mix_own, mixed_all.at[mine], w_sem.at[3])
    o.start()
    o.wait()
    for i in range(6, 9):
        loads[i].wait()
    for c in gathers[0]:
        c.wait_recv()
    stores = []

    def put(src, dst):
        o = pltpu.make_async_copy(src, dst, w_sem.at[4 + len(stores)])
        o.start()
        stores.append(o)

    put(rows_x, rx_ref)
    row_data = rows_x[...].reshape(size, model)
    pre_gate = jnp.dot(row_data, wg[...], preferred_element_type=F32)
    pre_up = jnp.dot(row_data, wu[...], preferred_element_type=F32)
    active, slope = silu_parts(pre_gate)
    hidden = (active * pre_up).astype(BF)
    acts[0] = hidden
    put(acts.at[0], hid_ref)
    lean = pre_up * slope
    advance(0, 0)
    if depth > 2:
        advance(0, 1)
    for c in gathers[1]:
        c.wait_recv()
    grad_hidden = contract_cols(rows_c[...].reshape(size, model), wd[...])
    grad_pre_gate = (grad_hidden * lean).astype(BF)
    grad_pre_up = (grad_hidden * active).astype(BF)
    acts[1] = grad_pre_gate
    acts[2] = grad_pre_up
    put(rows_c, rc_ref)
    put(acts.at[1], gpg_ref)
    put(acts.at[2], gpu_ref)
    for d in list(range(1, parts)) + [0]:
        part = near(width, lax.rem(col + d, parts))
        term = contract_cols(grad_pre_gate, wg[part, :]) + contract_cols(grad_pre_up, wu[part, :])
        terms[d] = term.astype(BF).reshape(groups, room, width)

    share_copies = {}
    order = list(range(1, groups)) + [0]
    for d in order if chunked else [0]:
        at = lax.rem(mine + d, groups)
        for p in range(1, parts):
            src = terms.at[p, at] if chunked else terms.at[p]
            dst = shares.at[p - 1, at] if chunked else shares.at[p - 1]
            c = remote(src, dst, s_send.at[d, p], s_recv.at[d, p], "tp", lax.rem(col + p, parts))
            c.start()
            share_copies[d, p] = c
            sends.append(c)
    for step in range(2, depth - 1):
        advance(0, step)
    chain(1, 0)
    across(1, 0, 0, "start")

    back_copies = []
    for d in order:
        at = lax.rem(mine + d, groups)
        if chunked or d == 1:
            for p in range(1, parts):
                share_copies[d if chunked else 0, p].wait_recv()
        total = terms[0, at].astype(F32)
        for p in range(1, parts):
            total = total + shares[p - 1, at].astype(F32)
        if d == 0:
            back[mine] = total.astype(BF)
        else:
            summed[d] = total.astype(BF)
            c = remote(summed.at[d], back.at[mine], r_send.at[d], r_recv.at[d], "sp", at)
            c.start()
            back_copies.append(c)
    nxt = lax.rem(mine + 1, groups)
    prev_copy = remote(states_ref.at[pl.ds(toks - 8, 8)], prev_in, p_send, p_recv, "sp", nxt)
    prev_copy.start()
    advance(1, 0)
    rows = lax.broadcasted_iota(jnp.int32, (toks, toks), 0)
    cols = lax.broadcasted_iota(jnp.int32, (toks, toks), 1)
    eye = jnp.where(rows == cols, 1.0, 0.0).astype(BF)
    total = contract_rows(cot_ref[...], eye)
    for c in back_copies:
        c.wait_recv()
    total = total + contract_rows(back[...].reshape(size, width), picked)
    flipped[here, :] = total.astype(BF)
    grad_copies = []
    for d in range(1, parts):
        part = flipped.at[here]
        c = remote(part, part, g_send.at[d], g_recv.at[d], "tp", lax.rem(col + d, parts))
        c.start()
        grad_copies.append(c)
    for step in range(1, depth - 1):
        advance(1, step)
    collected(0)
    loads[5].wait()
    for c in grad_copies:
        c.wait_recv()
    high = model // groups
    block_copies = []
    for d in range(1, groups):
        peer = lax.rem(mine + d, groups)
        c = remote(flipped.at[near(high, peer)], blocks.at[mine], b_send.at[d], b_recv.at[d], "sp", peer)
        c.start()
        block_copies.append(c)
    grad_mixed = contract_rows(flipped[...], proj_all[...].reshape(model, states_ref.shape[1]))
    states = states_ref[...]
    act, branch_slope = gelu_parts(gate_ref[...].astype(F32))
    decays = jnp.exp(decay_ref[...])
    ggate_ref[...] = (grad_mixed * states * branch_slope).astype(BF)
    local = grad_mixed * act
    line = lax.broadcasted_iota(jnp.int32, local.shape, 0)
    span = jnp.where(line < toks - 1, pltpu.roll(decays, toks - 1, 0), 1.0)
    k = 1
    while k < toks:
        inside = line < toks - k
        local = local + span * jnp.where(inside, pltpu.roll(local, toks - k, 0), 0.0)
        span = span * jnp.where(inside, pltpu.roll(span, toks - k, 0), 1.0)
        k *= 2
    eight = lax.broadcasted_iota(jnp.int32, (8, local.shape[1]), 0)
    whole = span[0:1] * decays[0:1]
    entry = local[0:1] * decays[0:1]
    carry_own[...] = jnp.where(eight == 0, whole, entry)
    carry_copies = []
    for d in range(1, groups):
        peer = lax.rem(mine + d, groups)
        c = remote(carry_own, carry_in.at[d - 1], k_send.at[d], k_recv.at[d], "sp", peer)
        c.start()
        carry_copies.append(c)
    collected(1)
    total = jnp.dot(flipped[near(high, mine), :], mixed_all[mine], preferred_element_type=F32)
    for d in range(1, groups):
        block_copies[d - 1].wait_recv()
        at = lax.rem(mine + groups - d, groups)
        total = total + jnp.dot(blocks[at], mixed_all[at], preferred_element_type=F32)
    outp_ref[...] = total
    prev_copy.wait_recv()
    first = jnp.where(mine > 0, prev_in[7:8, :], 0.0)
    prev = jnp.where(line == 0, first, pltpu.roll(states, 1, 0))
    for c in carry_copies:
        c.wait_recv()
    carried = jnp.zeros_like(whole)
    for ahead in range(groups - 1, 0, -1):
        got = carry_in[groups - ahead - 1]
        carried = jnp.where(mine + ahead < groups, got[1:2] + got[0:1] * carried, carried)
    grad_in = local + span * carried
    gin_ref[...] = grad_in
    gdecay_ref[...] = (grad_in * decays * prev).astype(BF)
    settle(0)
    settle(1)
    for c in [prev_copy] + sends + back_copies + grad_copies + block_copies + carry_copies:
        c.wait_send()
    for o in stores:
        o.wait()


def finish_kernel(
    rx, rc, hid, gpg, gpu, outp, ggate, gdecay, gin,
    gg_out, gu_out, gd_out, outp_out, ggate_out, gdecay_out, gin_out,
):
    gg_out[...] = contract_rows(rx[...], gpg[...])
    gu_out[...] = contract_rows(rx[...], gpu[...])
    gd_out[...] = contract_rows(hid[...], rc[...])
    outp_out[...] = outp[...]
    ggate_out[...] = ggate[...]
    gdecay_out[...] = gdecay[...]
    gin_out[...] = gin[...]


def finish(rx, rc, hid, gpg, gpu, *small):
    size, model = rx.shape
    units = hid.shape[1]
    steps = model // 256

    def cols(rows):
        return pl.BlockSpec((rows, 256), lambda i: (0, i))

    def band(array):
        return pl.BlockSpec((array.shape[0] // steps, array.shape[1]), lambda i: (i, 0))

    full = pl.BlockSpec((size, units), lambda i: (0, 0))
    tall = pl.BlockSpec((256, units), lambda i: (i, 0))
    outs = pl.pallas_call(
        finish_kernel,
        grid=(steps,),
        out_shape=[
            jax.ShapeDtypeStruct((model, units), F32),
            jax.ShapeDtypeStruct((model, units), F32),
            jax.ShapeDtypeStruct((units, model), F32),
        ] + [jax.ShapeDtypeStruct(a.shape, a.dtype) for a in small],
        in_specs=[cols(size)] * 2 + [full] * 3 + [band(a) for a in small],
        out_specs=[tall] * 2 + [cols(units)] + [band(a) for a in small],
        compiler_params=pltpu.CompilerParams(vmem_limit_bytes=40 * 1024 * 1024),
        name="finish",
    )(rx, rc, hid, gpg, gpu, *small)
    return tuple(out[None] for out in outs[:3]) + tuple(outs[3:])


def shards(
    moe_input, cotangent, routes, route_weights, gate_branch, log_decay, states,
    w_gate, w_up, w_down, out_proj,
):
    groups, parts = lax.axis_size("sp"), lax.axis_size("tp")
    tok_rows, picks = routes.shape
    width = moe_input.shape[1]
    model = width * parts
    units = w_gate.shape[2]
    chans = states.shape[1]
    room = tok_rows * picks * 5 // (4 * groups)
    room = (room + 7) // 8 * 8
    depth = groups // CORES
    high = out_proj.shape[0]
    chunked = groups * parts <= 64
    chunks = groups if chunked else 1
    vmem = pl.BlockSpec(memory_space=pltpu.VMEM)
    hbm = pl.BlockSpec(memory_space=pl.ANY)
    dma = pltpu.SemaphoreType.DMA

    def run(*refs):
        whole_kernel(groups, parts, room, chunked, *refs)

    def buf(*shape, kind=BF):
        return pltpu.VMEM(shape, kind)

    outs = pl.pallas_call(
        run,
        out_shape=[
            jax.ShapeDtypeStruct((groups, room, model), BF),
            jax.ShapeDtypeStruct((groups, room, model), BF),
            jax.ShapeDtypeStruct((groups * room, units), BF),
            jax.ShapeDtypeStruct((groups * room, units), BF),
            jax.ShapeDtypeStruct((groups * room, units), BF),
            jax.ShapeDtypeStruct((high, chans), F32),
            jax.ShapeDtypeStruct((tok_rows, chans), BF),
            jax.ShapeDtypeStruct((tok_rows, chans), BF),
            jax.ShapeDtypeStruct((tok_rows, chans), F32),
        ],
        in_specs=[vmem] * 2 + [hbm] * 9,
        out_specs=[hbm] * 5 + [vmem] * 4,
        scratch_shapes=[
            buf(tok_rows, width), buf(tok_rows, width), buf(tok_rows, chans),
            buf(tok_rows, chans, kind=F32), buf(tok_rows, chans, kind=F32),
            buf(model, units), buf(model, units), buf(units, model),
            buf(groups, room, width), buf(groups, room, width),
            buf(groups, room, model), buf(groups, room, model),
            buf(groups, high, chans), buf(groups, tok_rows, chans), buf(tok_rows, chans),
            buf(3, groups * room, units),
            buf(parts, groups, room, width), buf(parts - 1, groups, room, width),
            buf(groups, room, width), buf(groups, room, width),
            buf(model, tok_rows), buf(groups, high, tok_rows),
            buf(8, chans, kind=F32), buf(groups - 1, 8, chans, kind=F32), buf(8, chans, kind=F32),
        ]
        + [dma((2, groups))] * 2 + [dma((2, chunks, parts))] * 2 + [dma((2, 2, depth))] * 4
        + [dma((chunks, parts))] * 2 + [dma((groups,))] * 2 + [dma((parts,))] * 2
        + [dma((groups,))] * 4 + [dma(())] * 2 + [dma((9,)), dma((9,))],
        compiler_params=pltpu.CompilerParams(
            collective_id=0, has_side_effects=True, vmem_limit_bytes=60 * 1024 * 1024),
        name="backward",
    )(
        routes.T, route_weights.T, moe_input, cotangent, gate_branch, states, log_decay, out_proj,
        w_gate, w_up, w_down,
    )
    rx, rc = (out.reshape(groups * room, model) for out in outs[:2])
    return finish(rx, rc, *outs[2:])


def solution(mesh):
    return jax.shard_map(
        shards,
        mesh=mesh,
        in_specs=(
            P("sp", "tp"), P("sp", "tp"), P("sp", None), P("sp", None), P("sp", "tp"),
            P("sp", "tp"), P("sp", "tp"), P("sp", None, "tp"), P("sp", None, "tp"),
            P("sp", "tp", None), P("sp", "tp"),
        ),
        out_specs=(
            P("sp", None, "tp"), P("sp", None, "tp"), P("sp", "tp", None), P("sp", "tp"),
            P("sp", "tp"), P("sp", "tp"), P("sp", "tp"),
        ),
        check_vma=False,
    )
```

```python
import jax
import jax.numpy as jnp
from jax import lax
from jax.experimental import pallas as pl
from jax.experimental.pallas import tpu as pltpu
from jax.sharding import PartitionSpec as P

BF = jnp.bfloat16
F32 = jnp.float32
CORES = 2
GELU_C = 0.7978845608028654
GELU_A = 0.044715


def silu_parts(pre_gate):
    sigmoid_val = jax.nn.sigmoid(pre_gate)
    return (pre_gate * sigmoid_val, sigmoid_val * (1.0 + pre_gate * (1.0 - sigmoid_val)))


def contract_rows(left_mat, right_mat):
    return lax.dot_general(
        left_mat, right_mat, (((0,), (0,)), ((), ())), preferred_element_type=F32
    )


def contract_cols(left_mat, right_mat):
    return lax.dot_general(
        left_mat, right_mat, (((1,), (1,)), ((), ())), preferred_element_type=F32
    )


def gelu_parts(x):
    t = jnp.tanh(GELU_C * (x + GELU_A * (x * x * x)))
    half = 0.5 * (1.0 + t)
    slope = half + 0.5 * x * (1.0 - t * t) * (GELU_C * (1.0 + 3.0 * GELU_A * x * x))
    return x * half, slope


def selection(routes_t, weights_t, groups, room):
    picks, toks = routes_t.shape
    experts = lax.broadcasted_iota(jnp.int32, (groups, toks), 0)
    named = jnp.zeros((groups, toks), F32)
    weight = jnp.zeros((groups, toks), F32)
    for k in range(picks):
        hit = routes_t[k : k + 1, :] == experts
        named = named + jnp.where(hit, 1.0, 0.0)
        weight = weight + jnp.where(hit, weights_t[k : k + 1, :], 0.0)
    rows = lax.broadcasted_iota(jnp.int32, (toks, toks), 0)
    cols = lax.broadcasted_iota(jnp.int32, (toks, toks), 1)
    before = jnp.where(rows < cols, 1.0, 0.0).astype(BF)
    slot = jnp.dot(named.astype(BF), before, preferred_element_type=F32)
    slot = jnp.where(named > 0.5, slot, -1.0)
    place = lax.broadcasted_iota(jnp.int32, (room, toks), 0).astype(F32)
    picked, column = [], []
    for e in range(groups):
        one = jnp.where(slot[e : e + 1, :] == place, 1.0, 0.0)
        picked.append(one)
        column.append(jnp.sum(one * weight[e : e + 1, :], axis=1, keepdims=True))
    return jnp.concatenate(picked, axis=0).astype(BF), jnp.concatenate(column, axis=0)


def greet(groups, parts, mine, col):
    barrier = pltpu.get_barrier_semaphore()
    for d in range(1, groups):
        pl.semaphore_signal(
            barrier, inc=1, device_id={"sp": lax.rem(mine + d, groups)},
            device_id_type=pl.DeviceIdType.MESH,
        )
    for d in range(1, parts):
        pl.semaphore_signal(
            barrier, inc=1, device_id={"tp": lax.rem(col + d, parts)},
            device_id_type=pl.DeviceIdType.MESH,
        )
    pl.semaphore_wait(barrier, groups + parts - 2)


def remote(src, dst, send, recv, axis, peer):
    return pltpu.make_async_remote_copy(
        src_ref=src, dst_ref=dst, send_sem=send, recv_sem=recv,
        device_id={axis: peer}, device_id_type=pl.DeviceIdType.MESH,
    )


def whole_kernel(
    groups, parts, room, chunked,
    routes_ref, weights_ref, x_any, cot_any, gate_any, states_any, decay_any, proj_any,
    wg_any, wu_any, wd_any,
    rows_x, rows_c, hid_ref, gpg_ref, gpu_ref, outp_ref, ggate_ref, gdecay_ref, gin_ref,
    x_ref, cot_ref, gate_ref, states_ref, decay_ref, wg, wu, wd,
    out_x, out_c, proj_all, mixed_all, mix_own,
    terms, shares, summed, back, flipped, blocks, carry_own, carry_in, prev_in,
    a_send, a_recv, t_send, t_recv, z_send, z_recv, c_send, c_recv,
    s_send, s_recv, r_send, r_recv, g_send, g_recv, b_send, b_recv, k_send, k_recv, p_send, p_recv,
    l_sem, w_sem,
):
    mine, col = lax.axis_index("sp"), lax.axis_index("tp")
    toks, width = x_ref.shape
    model = rows_x.shape[2]
    depth = groups // CORES
    z, core = mine // CORES, lax.rem(mine, CORES)
    size = groups * room

    def near(width_of, index):
        return pl.ds(pl.multiple_of(index * width_of, width_of), width_of)

    loads = []
    for i, (s, t) in enumerate((
        (x_any, x_ref), (cot_any, cot_ref), (gate_any, gate_ref), (states_any, states_ref),
        (proj_any, proj_all.at[mine]), (decay_any, decay_ref),
        (wg_any.at[0], wg), (wu_any.at[0], wu), (wd_any.at[0], wd),
    )):
        o = pltpu.make_async_copy(s, t, l_sem.at[i])
        o.start()
        loads.append(o)

    picked, weight = selection(routes_ref[...], weights_ref[...], groups, room)
    loads[0].wait()
    got = jnp.dot(picked, x_ref[...], preferred_element_type=F32).astype(BF)
    for e in range(groups):
        out_x[e] = got[e * room : (e + 1) * room]
    loads[1].wait()
    got_c = jnp.dot(picked, cot_ref[...], preferred_element_type=F32)
    got_c = (got_c * weight).astype(BF)
    for e in range(groups):
        out_c[e] = got_c[e * room : (e + 1) * room]
    greet(groups, parts, mine, col)

    here = near(width, col)
    sends, own = [], []
    arrivals = [[None] * groups for _ in range(2)]
    for a, (src, dst) in enumerate(((out_x, rows_x), (out_c, rows_c))):
        for d in range(1, groups):
            peer = lax.rem(mine + d, groups)
            c = remote(src.at[peer], dst.at[mine, :, here], a_send.at[a, d], a_recv.at[a, d], "sp", peer)
            c.start()
            arrivals[a][d] = c
            sends.append(c)
        o = pltpu.make_async_copy(src.at[mine], dst.at[mine, :, here], w_sem.at[a])
        o.start()
        own.append(o)

    pairs = (proj_all, mixed_all)

    def chain(a, step, wait=False):
        buf = pairs[a]
        right = buf.at[jnp.maximum(z - step, 0) * CORES + core]
        left = buf.at[jnp.minimum(z + step, depth - 1) * CORES + core]
        up = jnp.minimum(z + 1, depth - 1) * CORES + core
        down = jnp.maximum(z - 1, 0) * CORES + core
        for way, ref, peer, ok in (
            (0, right, up, jnp.logical_and(z - step >= 0, z + 1 < depth)),
            (1, left, down, jnp.logical_and(z + step < depth, z >= 1)),
        ):
            @pl.when(ok)
            def _(way=way, ref=ref, peer=peer):
                c = remote(ref, ref, z_send.at[a, way, step], z_recv.at[a, way, step], "sp", peer)
                c.wait_send() if wait else c.start()

    partner = z * CORES + (1 - core)

    def across(a, step, way, mode):
        ok = z - step >= 0 if way == 0 else z + step < depth
        zz = jnp.maximum(z - step, 0) if way == 0 else jnp.minimum(z + step, depth - 1)
        ref = pairs[a].at[zz * CORES + (1 - core if mode == "recv" else core)]

        @pl.when(ok)
        def _():
            c = remote(ref, ref, c_send.at[a, way, step], c_recv.at[a, way, step], "sp", partner)
            if mode == "start":
                c.start()
            elif mode == "send":
                c.wait_send()
            else:
                c.wait_recv()

    def advance(a, step):
        buf = pairs[a]
        from_l = buf.at[jnp.maximum(z - 1 - step, 0) * CORES + core]
        from_r = buf.at[jnp.minimum(z + 1 + step, depth - 1) * CORES + core]
        for way, ok, ref in ((0, z - 1 - step >= 0, from_l), (1, z + 1 + step < depth, from_r)):
            @pl.when(ok)
            def _(way=way, ref=ref):
                remote(ref, ref, z_send.at[a, way, step], z_recv.at[a, way, step],
                       "sp", lax.rem(mine + 1, groups)).wait_recv()
        if step + 1 < depth - 1:
            chain(a, step + 1)
        across(a, step + 1, 0, "start")
        across(a, step + 1, 1, "start")

    def settle(a):
        for step in range(depth - 1):
            chain(a, step, True)
        for step in range(depth):
            for way in range(2):
                if step or not way:
                    across(a, step, way, "send")

    def collected(a):
        for step in range(depth):
            for way in range(2):
                if step or not way:
                    across(a, step, way, "recv")

    loads[4].wait()
    chain(0, 0)
    across(0, 0, 0, "start")

    gathers = [[], []]

    def gather(a, src, dst):
        if chunked:
            for d in range(groups):
                at = lax.rem(mine + groups - d, groups)
                if d:
                    arrivals[a][d].wait_recv()
                for p in range(1, parts):
                    c = remote(dst.at[at, :, here] if d else src.at[mine], dst.at[at, :, here],
                               t_send.at[a, d, p], t_recv.at[a, d, p], "tp", lax.rem(col + p, parts))
                    c.start()
                    gathers[a].append(c)
            own[a].wait()
        else:
            own[a].wait()
            for d in range(1, groups):
                arrivals[a][d].wait_recv()
            for p in range(1, parts):
                c = remote(dst.at[:, :, here], dst.at[:, :, here],
                           t_send.at[a, 0, p], t_recv.at[a, 0, p], "tp", lax.rem(col + p, parts))
                c.start()
                gathers[a].append(c)
        sends.extend(gathers[a])

    gather(0, out_x, rows_x)
    loads[2].wait()
    loads[3].wait()
    act, branch_slope = gelu_parts(gate_ref[...].astype(F32))
    mix_own[...] = (act * states_ref[...]).astype(BF)
    gather(1, out_c, rows_c)
    o = pltpu.make_async_copy(mix_own, mixed_all.at[mine], w_sem.at[3])
    o.start()
    o.wait()
    for i in range(6, 9):
        loads[i].wait()
    for c in gathers[0]:
        c.wait_recv()
    row_data = rows_x[...].reshape(size, model)
    pre_gate = jnp.dot(row_data, wg[...], preferred_element_type=F32)
    pre_up = jnp.dot(row_data, wu[...], preferred_element_type=F32)
    active, slope = silu_parts(pre_gate)
    hidden = (active * pre_up).astype(BF)
    hid_ref[...] = hidden
    lean = pre_up * slope
    advance(0, 0)
    if depth > 2:
        advance(0, 1)
    for c in gathers[1]:
        c.wait_recv()
    grad_hidden = contract_cols(rows_c[...].reshape(size, model), wd[...])
    grad_pre_gate = (grad_hidden * lean).astype(BF)
    grad_pre_up = (grad_hidden * active).astype(BF)
    gpg_ref[...] = grad_pre_gate
    gpu_ref[...] = grad_pre_up
    for d in list(range(1, parts)) + [0]:
        part = near(width, lax.rem(col + d, parts))
        term = contract_cols(grad_pre_gate, wg[part, :]) + contract_cols(grad_pre_up, wu[part, :])
        terms[d] = term.astype(BF).reshape(groups, room, width)

    share_copies = {}
    order = list(range(1, groups)) + [0]
    for d in order if chunked else [0]:
        at = lax.rem(mine + d, groups)
        for p in range(1, parts):
            src = terms.at[p, at] if chunked else terms.at[p]
            dst = shares.at[p - 1, at] if chunked else shares.at[p - 1]
            c = remote(src, dst, s_send.at[d, p], s_recv.at[d, p], "tp", lax.rem(col + p, parts))
            c.start()
            share_copies[d, p] = c
            sends.append(c)
    for step in range(2, depth - 1):
        advance(0, step)
    chain(1, 0)
    across(1, 0, 0, "start")

    back_copies = []
    for d in order:
        at = lax.rem(mine + d, groups)
        if chunked or d == 1:
            for p in range(1, parts):
                share_copies[d if chunked else 0, p].wait_recv()
        total = terms[0, at].astype(F32)
        for p in range(1, parts):
            total = total + shares[p - 1, at].astype(F32)
        if d == 0:
            back[mine] = total.astype(BF)
        else:
            summed[d] = total.astype(BF)
            c = remote(summed.at[d], back.at[mine], r_send.at[d], r_recv.at[d], "sp", at)
            c.start()
            back_copies.append(c)
    nxt = lax.rem(mine + 1, groups)
    prev_copy = remote(states_ref.at[pl.ds(toks - 8, 8)], prev_in, p_send, p_recv, "sp", nxt)
    prev_copy.start()
    advance(1, 0)
    rows = lax.broadcasted_iota(jnp.int32, (toks, toks), 0)
    cols = lax.broadcasted_iota(jnp.int32, (toks, toks), 1)
    eye = jnp.where(rows == cols, 1.0, 0.0).astype(BF)
    total = contract_rows(cot_ref[...], eye)
    for c in back_copies:
        c.wait_recv()
    total = total + contract_rows(back[...].reshape(size, width), picked)
    flipped[here, :] = total.astype(BF)
    grad_copies = []
    for d in range(1, parts):
        part = flipped.at[here]
        c = remote(part, part, g_send.at[d], g_recv.at[d], "tp", lax.rem(col + d, parts))
        c.start()
        grad_copies.append(c)
    for step in range(1, depth - 1):
        advance(1, step)
    collected(0)
    loads[5].wait()
    for c in grad_copies:
        c.wait_recv()
    high = model // groups
    block_copies = []
    for d in range(1, groups):
        peer = lax.rem(mine + d, groups)
        c = remote(flipped.at[near(high, peer)], blocks.at[mine], b_send.at[d], b_recv.at[d], "sp", peer)
        c.start()
        block_copies.append(c)
    grad_mixed = contract_rows(flipped[...], proj_all[...].reshape(model, states_ref.shape[1]))
    states = states_ref[...]
    act, branch_slope = gelu_parts(gate_ref[...].astype(F32))
    decays = jnp.exp(decay_ref[...])
    ggate_ref[...] = (grad_mixed * states * branch_slope).astype(BF)
    local = grad_mixed * act
    line = lax.broadcasted_iota(jnp.int32, local.shape, 0)
    span = jnp.where(line < toks - 1, pltpu.roll(decays, toks - 1, 0), 1.0)
    k = 1
    while k < toks:
        inside = line < toks - k
        local = local + span * jnp.where(inside, pltpu.roll(local, toks - k, 0), 0.0)
        span = span * jnp.where(inside, pltpu.roll(span, toks - k, 0), 1.0)
        k *= 2
    eight = lax.broadcasted_iota(jnp.int32, (8, local.shape[1]), 0)
    whole = span[0:1] * decays[0:1]
    entry = local[0:1] * decays[0:1]
    carry_own[...] = jnp.where(eight == 0, whole, entry)
    carry_copies = []
    for d in range(1, groups):
        peer = lax.rem(mine + d, groups)
        c = remote(carry_own, carry_in.at[d - 1], k_send.at[d], k_recv.at[d], "sp", peer)
        c.start()
        carry_copies.append(c)
    collected(1)
    total = jnp.dot(flipped[near(high, mine), :], mixed_all[mine], preferred_element_type=F32)
    for d in range(1, groups):
        block_copies[d - 1].wait_recv()
        at = lax.rem(mine + groups - d, groups)
        total = total + jnp.dot(blocks[at], mixed_all[at], preferred_element_type=F32)
    outp_ref[...] = total
    prev_copy.wait_recv()
    first = jnp.where(mine > 0, prev_in[7:8, :], 0.0)
    prev = jnp.where(line == 0, first, pltpu.roll(states, 1, 0))
    for c in carry_copies:
        c.wait_recv()
    carried = jnp.zeros_like(whole)
    for ahead in range(groups - 1, 0, -1):
        got = carry_in[groups - ahead - 1]
        carried = jnp.where(mine + ahead < groups, got[1:2] + got[0:1] * carried, carried)
    grad_in = local + span * carried
    gin_ref[...] = grad_in
    gdecay_ref[...] = (grad_in * decays * prev).astype(BF)
    settle(0)
    settle(1)
    for c in [prev_copy] + sends + back_copies + grad_copies + block_copies + carry_copies:
        c.wait_send()


def finish_kernel(
    rx, rc, hid, gpg, gpu, outp, ggate, gdecay, gin,
    gg_out, gu_out, gd_out, outp_out, ggate_out, gdecay_out, gin_out,
):
    gg_out[...] = contract_rows(rx[...], gpg[...])
    gu_out[...] = contract_rows(rx[...], gpu[...])
    gd_out[...] = contract_rows(hid[...], rc[...])
    outp_out[...] = outp[...]
    ggate_out[...] = ggate[...]
    gdecay_out[...] = gdecay[...]
    gin_out[...] = gin[...]


def finish(rx, rc, hid, gpg, gpu, *small):
    size, model = rx.shape
    units = hid.shape[1]
    steps = model // 256

    def cols(rows):
        return pl.BlockSpec((rows, 256), lambda i: (0, i))

    def band(array):
        return pl.BlockSpec((array.shape[0] // steps, array.shape[1]), lambda i: (i, 0))

    full = pl.BlockSpec((size, units), lambda i: (0, 0))
    tall = pl.BlockSpec((256, units), lambda i: (i, 0))
    outs = pl.pallas_call(
        finish_kernel,
        grid=(steps,),
        out_shape=[
            jax.ShapeDtypeStruct((model, units), F32),
            jax.ShapeDtypeStruct((model, units), F32),
            jax.ShapeDtypeStruct((units, model), F32),
        ] + [jax.ShapeDtypeStruct(a.shape, a.dtype) for a in small],
        in_specs=[cols(size)] * 2 + [full] * 3 + [band(a) for a in small],
        out_specs=[tall] * 2 + [cols(units)] + [band(a) for a in small],
        compiler_params=pltpu.CompilerParams(vmem_limit_bytes=40 * 1024 * 1024),
        name="finish",
    )(rx, rc, hid, gpg, gpu, *small)
    return tuple(out[None] for out in outs[:3]) + tuple(outs[3:])


def shards(
    moe_input, cotangent, routes, route_weights, gate_branch, log_decay, states,
    w_gate, w_up, w_down, out_proj,
):
    groups, parts = lax.axis_size("sp"), lax.axis_size("tp")
    tok_rows, picks = routes.shape
    width = moe_input.shape[1]
    model = width * parts
    units = w_gate.shape[2]
    chans = states.shape[1]
    room = tok_rows * picks * 5 // (4 * groups)
    room = (room + 7) // 8 * 8
    depth = groups // CORES
    high = out_proj.shape[0]
    chunked = groups * parts <= 64
    chunks = groups if chunked else 1
    vmem = pl.BlockSpec(memory_space=pltpu.VMEM)
    hbm = pl.BlockSpec(memory_space=pltpu.HBM)
    dma = pltpu.SemaphoreType.DMA

    def run(*refs):
        whole_kernel(groups, parts, room, chunked, *refs)

    def buf(*shape, kind=BF):
        return pltpu.VMEM(shape, kind)

    outs = pl.pallas_call(
        run,
        out_shape=[
            jax.ShapeDtypeStruct((groups, room, model), BF),
            jax.ShapeDtypeStruct((groups, room, model), BF),
            jax.ShapeDtypeStruct((groups * room, units), BF),
            jax.ShapeDtypeStruct((groups * room, units), BF),
            jax.ShapeDtypeStruct((groups * room, units), BF),
            jax.ShapeDtypeStruct((high, chans), F32),
            jax.ShapeDtypeStruct((tok_rows, chans), BF),
            jax.ShapeDtypeStruct((tok_rows, chans), BF),
            jax.ShapeDtypeStruct((tok_rows, chans), F32),
        ],
        in_specs=[vmem] * 2 + [hbm] * 9,
        out_specs=[vmem] * 9,
        scratch_shapes=[
            buf(tok_rows, width), buf(tok_rows, width), buf(tok_rows, chans),
            buf(tok_rows, chans, kind=F32), buf(tok_rows, chans, kind=F32),
            buf(model, units), buf(model, units), buf(units, model),
            buf(groups, room, width), buf(groups, room, width),
            buf(groups, high, chans), buf(groups, tok_rows, chans), buf(tok_rows, chans),
            buf(parts, groups, room, width), buf(parts - 1, groups, room, width),
            buf(groups, room, width), buf(groups, room, width),
            buf(model, tok_rows), buf(groups, high, tok_rows),
            buf(8, chans, kind=F32), buf(groups - 1, 8, chans, kind=F32), buf(8, chans, kind=F32),
        ]
        + [dma((2, groups))] * 2 + [dma((2, chunks, parts))] * 2 + [dma((2, 2, depth))] * 4
        + [dma((chunks, parts))] * 2 + [dma((groups,))] * 2 + [dma((parts,))] * 2
        + [dma((groups,))] * 4 + [dma(())] * 2 + [dma((9,)), dma((4,))],
        compiler_params=pltpu.CompilerParams(
            collective_id=0, has_side_effects=True, vmem_limit_bytes=40 * 1024 * 1024),
        name="backward",
    )(
        routes.T, route_weights.T,
        *(pltpu.with_memory_space_constraint(a, pltpu.HBM) for a in (
            moe_input, cotangent, gate_branch, states, log_decay, out_proj, w_gate, w_up, w_down)),
    )
    rx, rc = (out.reshape(groups * room, model) for out in outs[:2])
    return finish(rx, rc, *outs[2:])


def solution(mesh):
    return jax.shard_map(
        shards,
        mesh=mesh,
        in_specs=(
            P("sp", "tp"), P("sp", "tp"), P("sp", None), P("sp", None), P("sp", "tp"),
            P("sp", "tp"), P("sp", "tp"), P("sp", None, "tp"), P("sp", None, "tp"),
            P("sp", "tp", None), P("sp", "tp"),
        ),
        out_specs=(
            P("sp", None, "tp"), P("sp", None, "tp"), P("sp", "tp", None), P("sp", "tp"),
            P("sp", "tp"), P("sp", "tp"), P("sp", "tp"),
        ),
        check_vma=False,
    )
```

```python
import jax
import jax.numpy as jnp
from jax import lax
from jax.experimental import pallas as pl
from jax.experimental.pallas import tpu as pltpu
from jax.sharding import PartitionSpec as P

BF = jnp.bfloat16
F32 = jnp.float32
CORES = 2
GELU_C = 0.7978845608028654
GELU_A = 0.044715


def silu_parts(pre_gate):
    sigmoid_val = jax.nn.sigmoid(pre_gate)
    return (pre_gate * sigmoid_val, sigmoid_val * (1.0 + pre_gate * (1.0 - sigmoid_val)))


def contract_rows(left_mat, right_mat):
    return lax.dot_general(
        left_mat, right_mat, (((0,), (0,)), ((), ())), preferred_element_type=F32
    )


def contract_cols(left_mat, right_mat):
    return lax.dot_general(
        left_mat, right_mat, (((1,), (1,)), ((), ())), preferred_element_type=F32
    )


def gelu_parts(x):
    t = jnp.tanh(GELU_C * (x + GELU_A * (x * x * x)))
    half = 0.5 * (1.0 + t)
    slope = half + 0.5 * x * (1.0 - t * t) * (GELU_C * (1.0 + 3.0 * GELU_A * x * x))
    return x * half, slope


def selection(routes_t, weights_t, groups, room):
    picks, toks = routes_t.shape
    experts = lax.broadcasted_iota(jnp.int32, (groups, toks), 0)
    named = jnp.zeros((groups, toks), F32)
    weight = jnp.zeros((groups, toks), F32)
    for k in range(picks):
        hit = routes_t[k : k + 1, :] == experts
        named = named + jnp.where(hit, 1.0, 0.0)
        weight = weight + jnp.where(hit, weights_t[k : k + 1, :], 0.0)
    rows = lax.broadcasted_iota(jnp.int32, (toks, toks), 0)
    cols = lax.broadcasted_iota(jnp.int32, (toks, toks), 1)
    before = jnp.where(rows < cols, 1.0, 0.0).astype(BF)
    slot = jnp.dot(named.astype(BF), before, preferred_element_type=F32)
    slot = jnp.where(named > 0.5, slot, -1.0)
    place = lax.broadcasted_iota(jnp.int32, (room, toks), 0).astype(F32)
    picked, column = [], []
    for e in range(groups):
        one = jnp.where(slot[e : e + 1, :] == place, 1.0, 0.0)
        picked.append(one)
        column.append(jnp.sum(one * weight[e : e + 1, :], axis=1, keepdims=True))
    return jnp.concatenate(picked, axis=0).astype(BF), jnp.concatenate(column, axis=0)


def greet(groups, parts, mine, col):
    barrier = pltpu.get_barrier_semaphore()
    for d in range(1, groups):
        pl.semaphore_signal(
            barrier, inc=1, device_id={"sp": lax.rem(mine + d, groups)},
            device_id_type=pl.DeviceIdType.MESH,
        )
    for d in range(1, parts):
        pl.semaphore_signal(
            barrier, inc=1, device_id={"tp": lax.rem(col + d, parts)},
            device_id_type=pl.DeviceIdType.MESH,
        )
    pl.semaphore_wait(barrier, groups + parts - 2)


def remote(src, dst, send, recv, axis, peer):
    return pltpu.make_async_remote_copy(
        src_ref=src, dst_ref=dst, send_sem=send, recv_sem=recv,
        device_id={axis: peer}, device_id_type=pl.DeviceIdType.MESH,
    )


def whole_kernel(
    groups, parts, room, chunked,
    routes_ref, weights_ref, x_any, cot_any, gate_any, states_any, decay_any, proj_any,
    wg_any, wu_any, wd_any,
    rows_x, rows_c, hid_ref, gpg_ref, gpu_ref, outp_ref, ggate_ref, gdecay_ref, gin_ref,
    x_ref, cot_ref, gate_ref, states_ref, decay_ref, wg, wu, wd,
    out_x, out_c, proj_all, mixed_all, mix_own,
    terms, shares, summed, back, flipped, blocks, carry_own, carry_in, prev_in,
    a_send, a_recv, t_send, t_recv, z_send, z_recv, c_send, c_recv,
    s_send, s_recv, r_send, r_recv, g_send, g_recv, b_send, b_recv, k_send, k_recv, p_send, p_recv,
    l_sem, w_sem,
):
    mine, col = lax.axis_index("sp"), lax.axis_index("tp")
    toks, width = x_ref.shape
    model = rows_x.shape[2]
    depth = groups // CORES
    z, core = mine // CORES, lax.rem(mine, CORES)
    size = groups * room

    def near(width_of, index):
        return pl.ds(pl.multiple_of(index * width_of, width_of), width_of)

    loads = []
    for i, (s, t) in enumerate((
        (x_any, x_ref), (cot_any, cot_ref), (gate_any, gate_ref), (states_any, states_ref),
        (proj_any, proj_all.at[mine]), (decay_any, decay_ref),
        (wg_any.at[0], wg), (wu_any.at[0], wu), (wd_any.at[0], wd),
    )):
        o = pltpu.make_async_copy(s, t, l_sem.at[i])
        o.start()
        loads.append(o)

    picked, weight = selection(routes_ref[...], weights_ref[...], groups, room)
    loads[0].wait()
    got = jnp.dot(picked, x_ref[...], preferred_element_type=F32).astype(BF)
    for e in range(groups):
        out_x[e] = got[e * room : (e + 1) * room]
    loads[1].wait()
    got_c = jnp.dot(picked, cot_ref[...], preferred_element_type=F32)
    got_c = (got_c * weight).astype(BF)
    for e in range(groups):
        out_c[e] = got_c[e * room : (e + 1) * room]
    greet(groups, parts, mine, col)

    here = near(width, col)
    sends, own = [], []
    arrivals = [[None] * groups for _ in range(2)]
    for a, (src, dst) in enumerate(((out_x, rows_x), (out_c, rows_c))):
        for d in range(1, groups):
            peer = lax.rem(mine + d, groups)
            c = remote(src.at[peer], dst.at[mine, :, here], a_send.at[a, d], a_recv.at[a, d], "sp", peer)
            c.start()
            arrivals[a][d] = c
            sends.append(c)
        o = pltpu.make_async_copy(src.at[mine], dst.at[mine, :, here], w_sem.at[a])
        o.start()
        own.append(o)

    pairs = (proj_all, mixed_all)

    def chain(a, step, wait=False):
        buf = pairs[a]
        right = buf.at[jnp.maximum(z - step, 0) * CORES + core]
        left = buf.at[jnp.minimum(z + step, depth - 1) * CORES + core]
        up = jnp.minimum(z + 1, depth - 1) * CORES + core
        down = jnp.maximum(z - 1, 0) * CORES + core
        for way, ref, peer, ok in (
            (0, right, up, jnp.logical_and(z - step >= 0, z + 1 < depth)),
            (1, left, down, jnp.logical_and(z + step < depth, z >= 1)),
        ):
            @pl.when(ok)
            def _(way=way, ref=ref, peer=peer):
                c = remote(ref, ref, z_send.at[a, way, step], z_recv.at[a, way, step], "sp", peer)
                c.wait_send() if wait else c.start()

    partner = z * CORES + (1 - core)

    def across(a, step, way, mode):
        ok = z - step >= 0 if way == 0 else z + step < depth
        zz = jnp.maximum(z - step, 0) if way == 0 else jnp.minimum(z + step, depth - 1)
        ref = pairs[a].at[zz * CORES + (1 - core if mode == "recv" else core)]

        @pl.when(ok)
        def _():
            c = remote(ref, ref, c_send.at[a, way, step], c_recv.at[a, way, step], "sp", partner)
            if mode == "start":
                c.start()
            elif mode == "send":
                c.wait_send()
            else:
                c.wait_recv()

    def advance(a, step):
        buf = pairs[a]
        from_l = buf.at[jnp.maximum(z - 1 - step, 0) * CORES + core]
        from_r = buf.at[jnp.minimum(z + 1 + step, depth - 1) * CORES + core]
        for way, ok, ref in ((0, z - 1 - step >= 0, from_l), (1, z + 1 + step < depth, from_r)):
            @pl.when(ok)
            def _(way=way, ref=ref):
                remote(ref, ref, z_send.at[a, way, step], z_recv.at[a, way, step],
                       "sp", lax.rem(mine + 1, groups)).wait_recv()
        if step + 1 < depth - 1:
            chain(a, step + 1)
        across(a, step + 1, 0, "start")
        across(a, step + 1, 1, "start")

    def settle(a):
        for step in range(depth - 1):
            chain(a, step, True)
        for step in range(depth):
            for way in range(2):
                if step or not way:
                    across(a, step, way, "send")

    def collected(a):
        for step in range(depth):
            for way in range(2):
                if step or not way:
                    across(a, step, way, "recv")

    loads[4].wait()
    chain(0, 0)
    across(0, 0, 0, "start")

    gathers = [[], []]

    def gather(a, src, dst):
        if chunked:
            for d in range(groups):
                at = lax.rem(mine + groups - d, groups)
                if d:
                    arrivals[a][d].wait_recv()
                for p in range(1, parts):
                    c = remote(dst.at[at, :, here] if d else src.at[mine], dst.at[at, :, here],
                               t_send.at[a, d, p], t_recv.at[a, d, p], "tp", lax.rem(col + p, parts))
                    c.start()
                    gathers[a].append(c)
            own[a].wait()
        else:
            own[a].wait()
            for d in range(1, groups):
                arrivals[a][d].wait_recv()
            for p in range(1, parts):
                c = remote(dst.at[:, :, here], dst.at[:, :, here],
                           t_send.at[a, 0, p], t_recv.at[a, 0, p], "tp", lax.rem(col + p, parts))
                c.start()
                gathers[a].append(c)
        sends.extend(gathers[a])

    gather(0, out_x, rows_x)
    loads[2].wait()
    loads[3].wait()
    act, branch_slope = gelu_parts(gate_ref[...].astype(F32))
    mix_own[...] = (act * states_ref[...]).astype(BF)
    gather(1, out_c, rows_c)
    o = pltpu.make_async_copy(mix_own, mixed_all.at[mine], w_sem.at[3])
    o.start()
    o.wait()
    for i in range(6, 9):
        loads[i].wait()
    for c in gathers[0]:
        c.wait_recv()
    row_data = rows_x[...].reshape(size, model)
    pre_gate = jnp.dot(row_data, wg[...], preferred_element_type=F32)
    pre_up = jnp.dot(row_data, wu[...], preferred_element_type=F32)
    active, slope = silu_parts(pre_gate)
    hidden = (active * pre_up).astype(BF)
    hid_ref[...] = hidden
    lean = pre_up * slope
    advance(0, 0)
    if depth > 2:
        advance(0, 1)
    for c in gathers[1]:
        c.wait_recv()
    grad_hidden = contract_cols(rows_c[...].reshape(size, model), wd[...])
    grad_pre_gate = (grad_hidden * lean).astype(BF)
    grad_pre_up = (grad_hidden * active).astype(BF)
    gpg_ref[...] = grad_pre_gate
    gpu_ref[...] = grad_pre_up
    for d in list(range(1, parts)) + [0]:
        part = near(width, lax.rem(col + d, parts))
        term = contract_cols(grad_pre_gate, wg[part, :]) + contract_cols(grad_pre_up, wu[part, :])
        terms[d] = term.astype(BF).reshape(groups, room, width)

    share_copies = {}
    order = list(range(1, groups)) + [0]
    for d in order if chunked else [0]:
        at = lax.rem(mine + d, groups)
        for p in range(1, parts):
            src = terms.at[p, at] if chunked else terms.at[p]
            dst = shares.at[p - 1, at] if chunked else shares.at[p - 1]
            c = remote(src, dst, s_send.at[d, p], s_recv.at[d, p], "tp", lax.rem(col + p, parts))
            c.start()
            share_copies[d, p] = c
            sends.append(c)
    for step in range(2, depth - 1):
        advance(0, step)
    chain(1, 0)
    across(1, 0, 0, "start")

    back_copies = []
    for d in order:
        at = lax.rem(mine + d, groups)
        if chunked or d == 1:
            for p in range(1, parts):
                share_copies[d if chunked else 0, p].wait_recv()
        total = terms[0, at].astype(F32)
        for p in range(1, parts):
            total = total + shares[p - 1, at].astype(F32)
        if d == 0:
            back[mine] = total.astype(BF)
        else:
            summed[d] = total.astype(BF)
            c = remote(summed.at[d], back.at[mine], r_send.at[d], r_recv.at[d], "sp", at)
            c.start()
            back_copies.append(c)
    nxt = lax.rem(mine + 1, groups)
    prev_copy = remote(states_ref.at[pl.ds(toks - 8, 8)], prev_in, p_send, p_recv, "sp", nxt)
    prev_copy.start()
    advance(1, 0)
    rows = lax.broadcasted_iota(jnp.int32, (toks, toks), 0)
    cols = lax.broadcasted_iota(jnp.int32, (toks, toks), 1)
    eye = jnp.where(rows == cols, 1.0, 0.0).astype(BF)
    total = contract_rows(cot_ref[...], eye)
    for c in back_copies:
        c.wait_recv()
    total = total + contract_rows(back[...].reshape(size, width), picked)
    flipped[here, :] = total.astype(BF)
    grad_copies = []
    for d in range(1, parts):
        part = flipped.at[here]
        c = remote(part, part, g_send.at[d], g_recv.at[d], "tp", lax.rem(col + d, parts))
        c.start()
        grad_copies.append(c)
    for step in range(1, depth - 1):
        advance(1, step)
    collected(0)
    loads[5].wait()
    for c in grad_copies:
        c.wait_recv()
    high = model // groups
    block_copies = []
    for d in range(1, groups):
        peer = lax.rem(mine + d, groups)
        c = remote(flipped.at[near(high, peer)], blocks.at[mine], b_send.at[d], b_recv.at[d], "sp", peer)
        c.start()
        block_copies.append(c)
    grad_mixed = contract_rows(flipped[...], proj_all[...].reshape(model, states_ref.shape[1]))
    states = states_ref[...]
    act, branch_slope = gelu_parts(gate_ref[...].astype(F32))
    decays = jnp.exp(decay_ref[...])
    ggate_ref[...] = (grad_mixed * states * branch_slope).astype(BF)
    local = grad_mixed * act
    line = lax.broadcasted_iota(jnp.int32, local.shape, 0)
    span = jnp.where(line < toks - 1, pltpu.roll(decays, toks - 1, 0), 1.0)
    k = 1
    while k < toks:
        inside = line < toks - k
        local = local + span * jnp.where(inside, pltpu.roll(local, toks - k, 0), 0.0)
        span = span * jnp.where(inside, pltpu.roll(span, toks - k, 0), 1.0)
        k *= 2
    eight = lax.broadcasted_iota(jnp.int32, (8, local.shape[1]), 0)
    whole = span[0:1] * decays[0:1]
    entry = local[0:1] * decays[0:1]
    carry_own[...] = jnp.where(eight == 0, whole, entry)
    carry_copies = []
    for d in range(1, groups):
        peer = lax.rem(mine + d, groups)
        c = remote(carry_own, carry_in.at[d - 1], k_send.at[d], k_recv.at[d], "sp", peer)
        c.start()
        carry_copies.append(c)
    collected(1)
    total = jnp.dot(flipped[near(high, mine), :], mixed_all[mine], preferred_element_type=F32)
    for d in range(1, groups):
        block_copies[d - 1].wait_recv()
        at = lax.rem(mine + groups - d, groups)
        total = total + jnp.dot(blocks[at], mixed_all[at], preferred_element_type=F32)
    outp_ref[...] = total
    prev_copy.wait_recv()
    first = jnp.where(mine > 0, prev_in[7:8, :], 0.0)
    prev = jnp.where(line == 0, first, pltpu.roll(states, 1, 0))
    for c in carry_copies:
        c.wait_recv()
    carried = jnp.zeros_like(whole)
    for ahead in range(groups - 1, 0, -1):
        got = carry_in[groups - ahead - 1]
        carried = jnp.where(mine + ahead < groups, got[1:2] + got[0:1] * carried, carried)
    grad_in = local + span * carried
    gin_ref[...] = grad_in
    gdecay_ref[...] = (grad_in * decays * prev).astype(BF)
    settle(0)
    settle(1)
    for c in [prev_copy] + sends + back_copies + grad_copies + block_copies + carry_copies:
        c.wait_send()


def finish_kernel(
    rx, rc, hid, gpg, gpu, outp, ggate, gdecay, gin,
    gg_out, gu_out, gd_out, outp_out, ggate_out, gdecay_out, gin_out,
    gg, gu, gd, sems, small_sems,
):
    stores = []
    for i, (src, dst) in enumerate((
        (outp, outp_out), (ggate, ggate_out), (gdecay, gdecay_out), (gin, gin_out),
    )):
        o = pltpu.make_async_copy(src, dst, small_sems.at[i])
        o.start()
        stores.append(o)
    steps = sems.shape[1]
    step = rx.shape[1] // steps
    for i in range(steps):
        part = slice(i * step, (i + 1) * step)
        for kind, grad, buf, out in ((0, gpg, gg, gg_out), (1, gpu, gu, gu_out)):
            buf[part, :] = contract_rows(rx[:, part], grad[...])
            o = pltpu.make_async_copy(buf.at[part], out.at[part], sems.at[kind, i])
            o.start()
            stores.append(o)
        gd[:, part] = contract_rows(hid[...], rc[:, part])
        o = pltpu.make_async_copy(gd.at[:, part], gd_out.at[:, part], sems.at[2, i])
        o.start()
        stores.append(o)
    for o in stores:
        o.wait()


def finish(rx, rc, hid, gpg, gpu, *small):
    size, model = rx.shape
    units = hid.shape[1]
    steps = model // 256
    vmem = pl.BlockSpec(memory_space=pltpu.VMEM)
    hbm = pl.BlockSpec(memory_space=pltpu.HBM)
    grads = [(model, units), (model, units), (units, model)]
    outs = pl.pallas_call(
        finish_kernel,
        out_shape=[jax.ShapeDtypeStruct(g, F32) for g in grads]
        + [jax.ShapeDtypeStruct(a.shape, a.dtype) for a in small],
        in_specs=[vmem] * (5 + len(small)),
        out_specs=[hbm] * (3 + len(small)),
        scratch_shapes=[pltpu.VMEM(g, F32) for g in grads]
        + [pltpu.SemaphoreType.DMA((3, steps)), pltpu.SemaphoreType.DMA((len(small),))],
        compiler_params=pltpu.CompilerParams(vmem_limit_bytes=40 * 1024 * 1024),
        name="finish",
    )(rx, rc, hid, gpg, gpu, *small)
    return tuple(out[None] for out in outs[:3]) + tuple(outs[3:])


def shards(
    moe_input, cotangent, routes, route_weights, gate_branch, log_decay, states,
    w_gate, w_up, w_down, out_proj,
):
    groups, parts = lax.axis_size("sp"), lax.axis_size("tp")
    tok_rows, picks = routes.shape
    width = moe_input.shape[1]
    model = width * parts
    units = w_gate.shape[2]
    chans = states.shape[1]
    room = tok_rows * picks * 5 // (4 * groups)
    room = (room + 7) // 8 * 8
    depth = groups // CORES
    high = out_proj.shape[0]
    chunked = groups * parts <= 64
    chunks = groups if chunked else 1
    vmem = pl.BlockSpec(memory_space=pltpu.VMEM)
    hbm = pl.BlockSpec(memory_space=pltpu.HBM)
    dma = pltpu.SemaphoreType.DMA

    def run(*refs):
        whole_kernel(groups, parts, room, chunked, *refs)

    def buf(*shape, kind=BF):
        return pltpu.VMEM(shape, kind)

    outs = pl.pallas_call(
        run,
        out_shape=[
            jax.ShapeDtypeStruct((groups, room, model), BF),
            jax.ShapeDtypeStruct((groups, room, model), BF),
            jax.ShapeDtypeStruct((groups * room, units), BF),
            jax.ShapeDtypeStruct((groups * room, units), BF),
            jax.ShapeDtypeStruct((groups * room, units), BF),
            jax.ShapeDtypeStruct((high, chans), F32),
            jax.ShapeDtypeStruct((tok_rows, chans), BF),
            jax.ShapeDtypeStruct((tok_rows, chans), BF),
            jax.ShapeDtypeStruct((tok_rows, chans), F32),
        ],
        in_specs=[vmem] * 2 + [hbm] * 9,
        out_specs=[vmem] * 9,
        scratch_shapes=[
            buf(tok_rows, width), buf(tok_rows, width), buf(tok_rows, chans),
            buf(tok_rows, chans, kind=F32), buf(tok_rows, chans, kind=F32),
            buf(model, units), buf(model, units), buf(units, model),
            buf(groups, room, width), buf(groups, room, width),
            buf(groups, high, chans), buf(groups, tok_rows, chans), buf(tok_rows, chans),
            buf(parts, groups, room, width), buf(parts - 1, groups, room, width),
            buf(groups, room, width), buf(groups, room, width),
            buf(model, tok_rows), buf(groups, high, tok_rows),
            buf(8, chans, kind=F32), buf(groups - 1, 8, chans, kind=F32), buf(8, chans, kind=F32),
        ]
        + [dma((2, groups))] * 2 + [dma((2, chunks, parts))] * 2 + [dma((2, 2, depth))] * 4
        + [dma((chunks, parts))] * 2 + [dma((groups,))] * 2 + [dma((parts,))] * 2
        + [dma((groups,))] * 4 + [dma(())] * 2 + [dma((9,)), dma((4,))],
        compiler_params=pltpu.CompilerParams(
            collective_id=0, has_side_effects=True, vmem_limit_bytes=40 * 1024 * 1024),
        name="backward",
    )(
        routes.T, route_weights.T,
        *(pltpu.with_memory_space_constraint(a, pltpu.HBM) for a in (
            moe_input, cotangent, gate_branch, states, log_decay, out_proj, w_gate, w_up, w_down)),
    )
    rx, rc = (out.reshape(groups * room, model) for out in outs[:2])
    return finish(rx, rc, *outs[2:])


def flip(index, mask, count):
    total, bit = 0, 1
    while bit < count:
        here = lax.rem(lax.div(index, bit), 2)
        total = total + bit * ((1 - here) if mask & bit else here)
        bit *= 2
    return total


def plane_kernel(
    groups, parts, room,
    routes_any, weights_any, x_any, cot_any, gate_any, states_any, decay_any, proj_any,
    wg_any, wu_any, wd_any,
    rows_x, rows_c, hid_ref, gpg_ref, gpu_ref, outp_ref, ggate_ref, gdecay_ref, gin_ref,
    routes_ref, weights_ref, x_ref, cot_ref, gate_ref, states_ref, decay_ref, wg, wu, wd,
    out_x, out_c, picked_ref, proj_all, mixed_all, act_ref, slope_ref, active_ref, lean_ref,
    terms, shares, summed, back, cot_turned, cot_mine, flipped, blocks, levels, span_ref, past_ref,
    carry_own, carry_in, prev_in,
    a_send, a_recv, t_send, t_recv, z_send, z_recv, c_send, c_recv,
    s_send, s_recv, r_send, r_recv, g_send, g_recv, b_send, b_recv, q_send, q_recv, u_send, u_recv,
    k_send, k_recv, p_send, p_recv, l_sem,
):
    mine, col = lax.axis_index("sp"), lax.axis_index("tp")
    toks, width = x_ref.shape
    model = rows_x.shape[2]
    chans = states_ref.shape[1]
    units = hid_ref.shape[2]
    depth = groups // CORES
    z, core = mine // CORES, lax.rem(mine, CORES)
    size = groups * room
    half = groups // 2
    rows_half = half * room
    started = []

    barrier = pltpu.get_barrier_semaphore()
    for d in range(1, groups):
        pl.semaphore_signal(
            barrier, inc=1, device_id={"sp": lax.rem(mine + d, groups)},
            device_id_type=pl.DeviceIdType.MESH,
        )
    for d in range(1, parts):
        pl.semaphore_signal(
            barrier, inc=1, device_id={"tp": lax.rem(col + d, parts)},
            device_id_type=pl.DeviceIdType.MESH,
        )

    loads = []
    for i, (s, t) in enumerate((
        (x_any, x_ref), (cot_any, cot_ref), (gate_any, gate_ref), (states_any, states_ref),
        (proj_any, proj_all.at[mine]), (decay_any, decay_ref),
        (wg_any.at[0], wg), (wu_any.at[0], wu), (wd_any.at[0], wd),
        (routes_any, routes_ref), (weights_any, weights_ref),
    )):
        loads.append(pltpu.make_async_copy(s, t, l_sem.at[i]))
    for i in (9, 10, 0, 1, 4, 2, 3, 6, 7, 8, 5):
        loads[i].start()

    def near(width_of, index):
        return pl.ds(pl.multiple_of(index * width_of, width_of), width_of)

    def send(src, dst, send_sem, recv_sem, axis, peer):
        c = remote(src, dst, send_sem, recv_sem, axis, peer)
        c.start()
        started.append(c)
        return c

    group = [flip(mine, d, groups) for d in range(groups)]
    tile = [flip(col, p, parts) for p in range(parts)]
    here = near(width, col)

    loads[9].wait()
    loads[10].wait()
    picked, weight = selection(routes_ref[...], weights_ref[...], groups, room)
    picked_ref[...] = picked
    arrivals = [[None] * groups for _ in range(2)]
    gathers = [[None] * groups for _ in range(2)]
    sources = ((out_x, rows_x), (out_c, rows_c))

    def spread(a):
        src, dst = sources[a]
        for d in range(1, groups):
            arrivals[a][d] = send(
                src.at[group[d]], dst.at[mine, :, here], a_send.at[a, d], a_recv.at[a, d], "sp", group[d])
        dst[mine, :, here] = src[mine]

    def share_out(a, d):
        src, dst = sources[a]
        if d:
            arrivals[a][d].wait_recv()
        own = dst.at[group[d], :, here] if d else src.at[mine]
        gathers[a][d] = [
            send(own, dst.at[group[d], :, here], t_send.at[a, d, k], t_recv.at[a, d, k], "tp", tile[k + 1])
            for k in range(2)
        ]

    def relay(a, d):
        dst = sources[a][1]
        k = d % 2
        gathers[a][d][k].wait_recv()
        ref = dst.at[group[d], :, near(width, tile[k + 1])]
        gathers[a][d].append(
            send(ref, ref, t_send.at[a, d, 2], t_recv.at[a, d, 2], "tp", tile[2 - k]))

    def landed(a, d):
        gathers[a][d][1 - d % 2].wait_recv()
        gathers[a][d][2].wait_recv()

    loads[0].wait()
    got = jnp.dot(picked, x_ref[...], preferred_element_type=F32).astype(BF)
    for e in range(groups):
        out_x[e] = got[e * room : (e + 1) * room]
    pl.semaphore_wait(barrier, groups + parts - 2)
    spread(0)
    share_out(0, 0)
    loads[1].wait()
    got = jnp.dot(picked, cot_ref[...], preferred_element_type=F32)
    got = (got * weight).astype(BF)
    for e in range(groups):
        out_c[e] = got[e * room : (e + 1) * room]
    spread(1)

    pairs = (proj_all, mixed_all)

    def chain(a, step, wait=False):
        buf = pairs[a]
        right = buf.at[jnp.maximum(z - step, 0) * CORES + core]
        left = buf.at[jnp.minimum(z + step, depth - 1) * CORES + core]
        up = jnp.minimum(z + 1, depth - 1) * CORES + core
        down = jnp.maximum(z - 1, 0) * CORES + core
        for way, ref, peer, ok in (
            (0, right, up, jnp.logical_and(z - step >= 0, z + 1 < depth)),
            (1, left, down, jnp.logical_and(z + step < depth, z >= 1)),
        ):
            @pl.when(ok)
            def _(way=way, ref=ref, peer=peer):
                c = remote(ref, ref, z_send.at[a, way, step], z_recv.at[a, way, step], "sp", peer)
                c.wait_send() if wait else c.start()

    partner = z * CORES + (1 - core)

    def across(a, step, way, mode):
        ok = z - step >= 0 if way == 0 else z + step < depth
        zz = jnp.maximum(z - step, 0) if way == 0 else jnp.minimum(z + step, depth - 1)
        ref = pairs[a].at[zz * CORES + (1 - core if mode == "recv" else core)]

        @pl.when(ok)
        def _():
            c = remote(ref, ref, c_send.at[a, way, step], c_recv.at[a, way, step], "sp", partner)
            if mode == "start":
                c.start()
            elif mode == "send":
                c.wait_send()
            else:
                c.wait_recv()

    def advance(a, step):
        buf = pairs[a]
        from_l = buf.at[jnp.maximum(z - 1 - step, 0) * CORES + core]
        from_r = buf.at[jnp.minimum(z + 1 + step, depth - 1) * CORES + core]
        for way, ok, ref in ((0, z - 1 - step >= 0, from_l), (1, z + 1 + step < depth, from_r)):
            @pl.when(ok)
            def _(way=way, ref=ref):
                remote(ref, ref, z_send.at[a, way, step], z_recv.at[a, way, step],
                       "sp", lax.rem(mine + 1, groups)).wait_recv()
        if step + 1 < depth - 1:
            chain(a, step + 1)
        across(a, step + 1, 0, "start")
        across(a, step + 1, 1, "start")

    def settle(a):
        for step in range(depth - 1):
            chain(a, step, True)
        for step in range(depth):
            for way in range(2):
                if step or not way:
                    across(a, step, way, "send")

    def collected(a):
        for step in range(depth):
            for way in range(2):
                if step or not way:
                    across(a, step, way, "recv")

    loads[4].wait()
    chain(0, 0)
    across(0, 0, 0, "start")
    loads[3].wait()
    prev_copy = send(
        states_ref.at[pl.ds(toks - 8, 8)], prev_in, p_send, p_recv, "sp", lax.rem(mine + 1, groups))

    share_out(0, 1)
    loads[2].wait()
    act, branch_slope = gelu_parts(gate_ref[...].astype(F32))
    states = states_ref[...]
    act_ref[...] = act
    slope_ref[...] = branch_slope * states
    mixed_all[mine] = (act * states).astype(BF)
    for d in range(2, groups):
        share_out(0, d)
        relay(0, d - 2)
    share_out(1, 0)
    relay(0, groups - 2)
    share_out(1, 1)
    relay(0, groups - 1)

    first = [lax.div(mine, half) * half, (1 - lax.div(mine, half)) * half]

    def forward(h):
        for d in range(h * half, (h + 1) * half):
            landed(0, d)
        at = pl.ds(first[h], half)
        data = rows_x[at].reshape(rows_half, model)
        pre_gate = jnp.dot(data, wg[...].reshape(model, units), preferred_element_type=F32)
        pre_up = jnp.dot(data, wu[...].reshape(model, units), preferred_element_type=F32)
        active, slope = silu_parts(pre_gate)
        hid_ref[at] = (active * pre_up).astype(BF).reshape(half, room, units)
        active_ref[h] = active
        lean_ref[h] = pre_up * slope

    def hidden_grads(h):
        for d in range(h * half, (h + 1) * half):
            landed(1, d)
        at = pl.ds(first[h], half)
        grad_hidden = contract_cols(rows_c[at].reshape(rows_half, model), wd[...])
        gpg_ref[at] = (grad_hidden * lean_ref[h]).astype(BF).reshape(half, room, units)
        gpu_ref[at] = (grad_hidden * active_ref[h]).astype(BF).reshape(half, room, units)

    def input_grads(h):
        at = pl.ds(first[h], half)
        gate_part = gpg_ref[at].reshape(rows_half, units)
        up_part = gpu_ref[at].reshape(rows_half, units)
        for p in list(range(1, parts)) + [0]:
            term = contract_cols(gate_part, wg[:, tile[p]].reshape(width, units))
            term = term + contract_cols(up_part, wu[:, tile[p]].reshape(width, units))
            terms[p, at] = term.astype(BF).reshape(half, room, width)

    share_copies = {}

    def reduce_out(d):
        for p in range(1, parts):
            share_copies[d, p] = send(
                terms.at[p, group[d]], shares.at[p - 1, group[d]],
                s_send.at[d, p], s_recv.at[d, p], "tp", tile[p])

    late = list(range(2, groups))
    waiting = list(range(groups))

    def pump(count):
        for _ in range(count):
            if late:
                share_out(1, late.pop(0))
            if waiting and (not late or waiting[0] <= late[0] - 3):
                relay(1, waiting.pop(0))

    pump(2)
    for i in (6, 7, 8):
        loads[i].wait()
    forward(0)
    pump(2)
    forward(1)
    pump(2)

    rows = lax.broadcasted_iota(jnp.int32, (toks, toks), 0)
    cols = lax.broadcasted_iota(jnp.int32, (toks, toks), 1)
    eye = jnp.where(rows == cols, 1.0, 0.0).astype(BF)
    fine = cot_turned.shape[2]
    cot_turned[...] = contract_rows(cot_ref[...], eye).astype(BF).reshape(cot_turned.shape)
    cot_mine[col] = cot_turned[:, col]

    while len(waiting) > 2:
        relay(1, waiting.pop(0))
    hidden_grads(0)
    while waiting:
        relay(1, waiting.pop(0))
    cot_copies = [
        send(cot_turned.at[:, tile[p]], cot_mine.at[col], u_send.at[p], u_recv.at[p], "tp", tile[p])
        for p in range(1, parts)
    ]
    input_grads(0)
    for d in range(1, half):
        reduce_out(d)
    hidden_grads(1)
    input_grads(1)
    for d in list(range(half, groups)) + [0]:
        reduce_out(d)
    advance(0, 0)

    loads[5].wait()
    prev_copy.wait_recv()
    decays = jnp.exp(decay_ref[...])
    line = lax.broadcasted_iota(jnp.int32, decays.shape, 0)
    before = jnp.where(mine > 0, prev_in[7:8, :], 0.0)
    past_ref[...] = decays * jnp.where(line == 0, before, pltpu.roll(states_ref[...], 1, 0))
    span = jnp.where(line < toks - 1, pltpu.roll(decays, toks - 1, 0), 1.0)
    k, level = 1, 0
    while k < toks:
        inside = line < toks - k
        levels[level] = jnp.where(inside, span, 0.0)
        span = span * jnp.where(inside, pltpu.roll(span, toks - k, 0), 1.0)
        k *= 2
        level += 1
    span_ref[...] = span
    head = decays[0:1]

    for i, d in enumerate(list(range(1, groups)) + [0]):
        for p in range(1, parts):
            share_copies[d, p].wait_recv()
        total = terms[0, group[d]].astype(F32)
        for p in range(1, parts):
            total = total + shares[p - 1, group[d]].astype(F32)
        if d == 0:
            back[mine] = total.astype(BF)
        else:
            summed[d] = total.astype(BF)
            arrivals[0][d] = send(
                summed.at[d], back.at[mine], r_send.at[d], r_recv.at[d], "sp", group[d])
        if i == half:
            for step in range(1, depth - 1):
                advance(0, step)
            chain(1, 0)
            across(1, 0, 0, "start")
    advance(1, 0)
    for c in cot_copies:
        c.wait_recv()
    total = cot_mine[...].reshape(width, toks).astype(F32)
    for d in range(1, groups):
        arrivals[0][d].wait_recv()
    total = total + contract_rows(back[...].reshape(size, width), picked_ref[...])
    flipped[:, col] = total.astype(BF).reshape(groups, fine, toks)
    grad_copies = []
    for p in range(1, parts):
        part = flipped.at[:, col]
        grad_copies.append(send(part, part, g_send.at[p], g_recv.at[p], "tp", tile[p]))
    block_copies = [
        send(flipped.at[group[d], col], blocks.at[mine, col], b_send.at[d], b_recv.at[d], "sp", group[d])
        for d in range(1, groups)
    ]
    blocks[mine, col] = flipped[mine, col]
    for step in range(1, depth - 1):
        advance(1, step)
    for c in block_copies:
        c.wait_recv()
    plane_copies = []
    for p in range(1, parts):
        part = blocks.at[:, col]
        plane_copies.append(send(part, part, q_send.at[p], q_recv.at[p], "tp", tile[p]))
    collected(0)
    for c in grad_copies:
        c.wait_recv()
    grad_mixed = contract_rows(flipped[...].reshape(model, toks), proj_all[...].reshape(model, chans))
    ggate_ref[...] = (grad_mixed * slope_ref[...]).astype(BF)
    local = grad_mixed * act_ref[...]
    k, level = 1, 0
    while k < toks:
        local = local + levels[level] * pltpu.roll(local, toks - k, 0)
        k *= 2
        level += 1
    eight = lax.broadcasted_iota(jnp.int32, (8, chans), 0)
    carry_own[...] = jnp.where(eight == 0, span_ref[0:1, :] * head, local[0:1] * head)
    carry_copies = []
    for d in range(1, groups):
        peer = lax.rem(mine + d, groups)
        carry_copies.append(
            send(carry_own, carry_in.at[d - 1], k_send.at[d], k_recv.at[d], "sp", peer))
    collected(1)
    for c in plane_copies:
        c.wait_recv()
    high = blocks.shape[1] * blocks.shape[2]
    total = jnp.zeros((high, chans), F32)
    for t in range(groups):
        total = total + jnp.dot(
            blocks[t].reshape(high, toks), mixed_all[t], preferred_element_type=F32)
    outp_ref[...] = total
    for c in carry_copies:
        c.wait_recv()
    carried = jnp.zeros((1, chans), F32)
    for ahead in range(groups - 1, 0, -1):
        got = carry_in[groups - ahead - 1]
        carried = jnp.where(mine + ahead < groups, got[1:2] + got[0:1] * carried, carried)
    grad_in = local + span_ref[...] * carried
    gin_ref[...] = grad_in
    gdecay_ref[...] = (grad_in * past_ref[...]).astype(BF)
    settle(0)
    settle(1)
    for c in started:
        c.wait_send()


def plane_shards(
    moe_input, cotangent, routes, route_weights, gate_branch, log_decay, states,
    w_gate, w_up, w_down, out_proj,
):
    groups, parts = lax.axis_size("sp"), lax.axis_size("tp")
    tok_rows, picks = routes.shape
    width = moe_input.shape[1]
    model = width * parts
    units = w_gate.shape[2]
    chans = states.shape[1]
    room = tok_rows * picks * 5 // (4 * groups)
    room = (room + 7) // 8 * 8
    depth = groups // CORES
    high = out_proj.shape[0]
    fine = high // parts
    doublings = (tok_rows - 1).bit_length()
    vmem = pl.BlockSpec(memory_space=pltpu.VMEM)
    hbm = pl.BlockSpec(memory_space=pltpu.HBM)
    dma = pltpu.SemaphoreType.DMA

    def run(*refs):
        plane_kernel(groups, parts, room, *refs)

    def buf(*shape, kind=BF):
        return pltpu.VMEM(shape, kind)

    def split(weight):
        return weight.reshape(1, groups, parts, fine, units)

    outs = pl.pallas_call(
        run,
        out_shape=[
            jax.ShapeDtypeStruct((groups, room, model), BF),
            jax.ShapeDtypeStruct((groups, room, model), BF),
            jax.ShapeDtypeStruct((groups, room, units), BF),
            jax.ShapeDtypeStruct((groups, room, units), BF),
            jax.ShapeDtypeStruct((groups, room, units), BF),
            jax.ShapeDtypeStruct((high, chans), F32),
            jax.ShapeDtypeStruct((tok_rows, chans), BF),
            jax.ShapeDtypeStruct((tok_rows, chans), BF),
            jax.ShapeDtypeStruct((tok_rows, chans), F32),
        ],
        in_specs=[hbm] * 11,
        out_specs=[vmem] * 9,
        scratch_shapes=[
            buf(picks, tok_rows, kind=jnp.int32), buf(picks, tok_rows, kind=F32),
            buf(tok_rows, width), buf(tok_rows, width), buf(tok_rows, chans),
            buf(tok_rows, chans, kind=F32), buf(tok_rows, chans, kind=F32),
            buf(groups, parts, fine, units), buf(groups, parts, fine, units), buf(units, model),
            buf(groups, room, width), buf(groups, room, width), buf(groups * room, tok_rows),
            buf(groups, high, chans), buf(groups, tok_rows, chans),
            buf(tok_rows, chans, kind=F32), buf(tok_rows, chans, kind=F32),
            buf(2, groups // 2 * room, units, kind=F32), buf(2, groups // 2 * room, units, kind=F32),
            buf(parts, groups, room, width), buf(parts - 1, groups, room, width),
            buf(groups, room, width), buf(groups, room, width),
            buf(groups // parts, parts, fine, tok_rows), buf(parts, groups // parts, fine, tok_rows),
            buf(groups, parts, fine, tok_rows), buf(groups, parts, fine, tok_rows),
            buf(doublings, tok_rows, chans, kind=F32), buf(tok_rows, chans, kind=F32),
            buf(tok_rows, chans, kind=F32),
            buf(8, chans, kind=F32), buf(groups - 1, 8, chans, kind=F32), buf(8, chans, kind=F32),
        ]
        + [dma((2, groups))] * 2 + [dma((2, groups, 3))] * 2 + [dma((2, 2, depth))] * 4
        + [dma((groups, parts))] * 2 + [dma((groups,))] * 2 + [dma((parts,))] * 2
        + [dma((groups,))] * 2 + [dma((parts,))] * 4
        + [dma((groups,))] * 2 + [dma(())] * 2 + [dma((11,))],
        compiler_params=pltpu.CompilerParams(
            collective_id=0, has_side_effects=True, vmem_limit_bytes=40 * 1024 * 1024),
        name="backward",
    )(
        *(pltpu.with_memory_space_constraint(a, pltpu.HBM) for a in (
            routes.T, route_weights.T, moe_input, cotangent, gate_branch, states, log_decay, out_proj,
            split(w_gate), split(w_up), w_down)),
    )
    rx, rc = (out.reshape(groups * room, model) for out in outs[:2])
    grads = (out.reshape(groups * room, units) for out in outs[2:5])
    return finish(rx, rc, *grads, *outs[5:])


def solution(mesh):
    groups, parts = mesh.shape["sp"], mesh.shape["tp"]
    plane = parts == 4 and groups % parts == 0 and groups & (groups - 1) == 0
    return jax.shard_map(
        plane_shards if plane else shards,
        mesh=mesh,
        in_specs=(
            P("sp", "tp"), P("sp", "tp"), P("sp", None), P("sp", None), P("sp", "tp"),
            P("sp", "tp"), P("sp", "tp"), P("sp", None, "tp"), P("sp", None, "tp"),
            P("sp", "tp", None), P("sp", "tp"),
        ),
        out_specs=(
            P("sp", None, "tp"), P("sp", None, "tp"), P("sp", "tp", None), P("sp", "tp"),
            P("sp", "tp"), P("sp", "tp"), P("sp", "tp"),
        ),
        check_vma=False,
    )
```

```python
import jax
import jax.numpy as jnp
from jax import lax
from jax.experimental import pallas as pl
from jax.experimental.pallas import tpu as pltpu
from jax.sharding import PartitionSpec as P

BF = jnp.bfloat16
F32 = jnp.float32
CORES = 2
GELU_C = 0.7978845608028654
GELU_A = 0.044715


def silu_parts(pre_gate):
    sigmoid_val = jax.nn.sigmoid(pre_gate)
    return (pre_gate * sigmoid_val, sigmoid_val * (1.0 + pre_gate * (1.0 - sigmoid_val)))


def contract_rows(left_mat, right_mat):
    return lax.dot_general(
        left_mat, right_mat, (((0,), (0,)), ((), ())), preferred_element_type=F32
    )


def contract_cols(left_mat, right_mat):
    return lax.dot_general(
        left_mat, right_mat, (((1,), (1,)), ((), ())), preferred_element_type=F32
    )


def gelu_parts(x):
    t = jnp.tanh(GELU_C * (x + GELU_A * (x * x * x)))
    half = 0.5 * (1.0 + t)
    slope = half + 0.5 * x * (1.0 - t * t) * (GELU_C * (1.0 + 3.0 * GELU_A * x * x))
    return x * half, slope


def selection(routes_t, weights_t, groups, room):
    picks, toks = routes_t.shape
    experts = lax.broadcasted_iota(jnp.int32, (groups, toks), 0)
    named = jnp.zeros((groups, toks), F32)
    weight = jnp.zeros((groups, toks), F32)
    for k in range(picks):
        hit = routes_t[k : k + 1, :] == experts
        named = named + jnp.where(hit, 1.0, 0.0)
        weight = weight + jnp.where(hit, weights_t[k : k + 1, :], 0.0)
    rows = lax.broadcasted_iota(jnp.int32, (toks, toks), 0)
    cols = lax.broadcasted_iota(jnp.int32, (toks, toks), 1)
    before = jnp.where(rows < cols, 1.0, 0.0).astype(BF)
    slot = jnp.dot(named.astype(BF), before, preferred_element_type=F32)
    slot = jnp.where(named > 0.5, slot, -1.0)
    place = lax.broadcasted_iota(jnp.int32, (room, toks), 0).astype(F32)
    picked, column = [], []
    for e in range(groups):
        one = jnp.where(slot[e : e + 1, :] == place, 1.0, 0.0)
        picked.append(one)
        column.append(jnp.sum(one * weight[e : e + 1, :], axis=1, keepdims=True))
    return jnp.concatenate(picked, axis=0).astype(BF), jnp.concatenate(column, axis=0)


def greet(groups, parts, mine, col):
    barrier = pltpu.get_barrier_semaphore()
    for d in range(1, groups):
        pl.semaphore_signal(
            barrier, inc=1, device_id={"sp": lax.rem(mine + d, groups)},
            device_id_type=pl.DeviceIdType.MESH,
        )
    for d in range(1, parts):
        pl.semaphore_signal(
            barrier, inc=1, device_id={"tp": lax.rem(col + d, parts)},
            device_id_type=pl.DeviceIdType.MESH,
        )
    pl.semaphore_wait(barrier, groups + parts - 2)


def remote(src, dst, send, recv, axis, peer):
    return pltpu.make_async_remote_copy(
        src_ref=src, dst_ref=dst, send_sem=send, recv_sem=recv,
        device_id={axis: peer}, device_id_type=pl.DeviceIdType.MESH,
    )


def whole_kernel(
    groups, parts, room, chunked,
    routes_ref, weights_ref, x_any, cot_any, gate_any, states_any, decay_any, proj_any,
    wg_any, wu_any, wd_any,
    rows_x, rows_c, hid_ref, gpg_ref, gpu_ref, outp_ref, ggate_ref, gdecay_ref, gin_ref,
    x_ref, cot_ref, gate_ref, states_ref, decay_ref, wg, wu, wd,
    out_x, out_c, proj_all, mixed_all, mix_own,
    terms, shares, summed, back, flipped, blocks, carry_own, carry_in, prev_in,
    a_send, a_recv, t_send, t_recv, z_send, z_recv, c_send, c_recv,
    s_send, s_recv, r_send, r_recv, g_send, g_recv, b_send, b_recv, k_send, k_recv, p_send, p_recv,
    l_sem, w_sem,
):
    mine, col = lax.axis_index("sp"), lax.axis_index("tp")
    toks, width = x_ref.shape
    model = rows_x.shape[2]
    depth = groups // CORES
    z, core = mine // CORES, lax.rem(mine, CORES)
    size = groups * room

    def near(width_of, index):
        return pl.ds(pl.multiple_of(index * width_of, width_of), width_of)

    loads = []
    for i, (s, t) in enumerate((
        (x_any, x_ref), (cot_any, cot_ref), (gate_any, gate_ref), (states_any, states_ref),
        (proj_any, proj_all.at[mine]), (decay_any, decay_ref),
        (wg_any.at[0], wg), (wu_any.at[0], wu), (wd_any.at[0], wd),
    )):
        o = pltpu.make_async_copy(s, t, l_sem.at[i])
        o.start()
        loads.append(o)

    picked, weight = selection(routes_ref[...], weights_ref[...], groups, room)
    loads[0].wait()
    got = jnp.dot(picked, x_ref[...], preferred_element_type=F32).astype(BF)
    for e in range(groups):
        out_x[e] = got[e * room : (e + 1) * room]
    loads[1].wait()
    got_c = jnp.dot(picked, cot_ref[...], preferred_element_type=F32)
    got_c = (got_c * weight).astype(BF)
    for e in range(groups):
        out_c[e] = got_c[e * room : (e + 1) * room]
    greet(groups, parts, mine, col)

    here = near(width, col)
    sends, own = [], []
    arrivals = [[None] * groups for _ in range(2)]
    for a, (src, dst) in enumerate(((out_x, rows_x), (out_c, rows_c))):
        for d in range(1, groups):
            peer = lax.rem(mine + d, groups)
            c = remote(src.at[peer], dst.at[mine, :, here], a_send.at[a, d], a_recv.at[a, d], "sp", peer)
            c.start()
            arrivals[a][d] = c
            sends.append(c)
        o = pltpu.make_async_copy(src.at[mine], dst.at[mine, :, here], w_sem.at[a])
        o.start()
        own.append(o)

    pairs = (proj_all, mixed_all)

    def chain(a, step, wait=False):
        buf = pairs[a]
        right = buf.at[jnp.maximum(z - step, 0) * CORES + core]
        left = buf.at[jnp.minimum(z + step, depth - 1) * CORES + core]
        up = jnp.minimum(z + 1, depth - 1) * CORES + core
        down = jnp.maximum(z - 1, 0) * CORES + core
        for way, ref, peer, ok in (
            (0, right, up, jnp.logical_and(z - step >= 0, z + 1 < depth)),
            (1, left, down, jnp.logical_and(z + step < depth, z >= 1)),
        ):
            @pl.when(ok)
            def _(way=way, ref=ref, peer=peer):
                c = remote(ref, ref, z_send.at[a, way, step], z_recv.at[a, way, step], "sp", peer)
                c.wait_send() if wait else c.start()

    partner = z * CORES + (1 - core)

    def across(a, step, way, mode):
        ok = z - step >= 0 if way == 0 else z + step < depth
        zz = jnp.maximum(z - step, 0) if way == 0 else jnp.minimum(z + step, depth - 1)
        ref = pairs[a].at[zz * CORES + (1 - core if mode == "recv" else core)]

        @pl.when(ok)
        def _():
            c = remote(ref, ref, c_send.at[a, way, step], c_recv.at[a, way, step], "sp", partner)
            if mode == "start":
                c.start()
            elif mode == "send":
                c.wait_send()
            else:
                c.wait_recv()

    def advance(a, step):
        buf = pairs[a]
        from_l = buf.at[jnp.maximum(z - 1 - step, 0) * CORES + core]
        from_r = buf.at[jnp.minimum(z + 1 + step, depth - 1) * CORES + core]
        for way, ok, ref in ((0, z - 1 - step >= 0, from_l), (1, z + 1 + step < depth, from_r)):
            @pl.when(ok)
            def _(way=way, ref=ref):
                remote(ref, ref, z_send.at[a, way, step], z_recv.at[a, way, step],
                       "sp", lax.rem(mine + 1, groups)).wait_recv()
        if step + 1 < depth - 1:
            chain(a, step + 1)
        across(a, step + 1, 0, "start")
        across(a, step + 1, 1, "start")

    def settle(a):
        for step in range(depth - 1):
            chain(a, step, True)
        for step in range(depth):
            for way in range(2):
                if step or not way:
                    across(a, step, way, "send")

    def collected(a):
        for step in range(depth):
            for way in range(2):
                if step or not way:
                    across(a, step, way, "recv")

    loads[4].wait()
    chain(0, 0)
    across(0, 0, 0, "start")

    gathers = [[], []]

    def gather(a, src, dst):
        if chunked:
            for d in range(groups):
                at = lax.rem(mine + groups - d, groups)
                if d:
                    arrivals[a][d].wait_recv()
                for p in range(1, parts):
                    c = remote(dst.at[at, :, here] if d else src.at[mine], dst.at[at, :, here],
                               t_send.at[a, d, p], t_recv.at[a, d, p], "tp", lax.rem(col + p, parts))
                    c.start()
                    gathers[a].append(c)
            own[a].wait()
        else:
            own[a].wait()
            for d in range(1, groups):
                arrivals[a][d].wait_recv()
            for p in range(1, parts):
                c = remote(dst.at[:, :, here], dst.at[:, :, here],
                           t_send.at[a, 0, p], t_recv.at[a, 0, p], "tp", lax.rem(col + p, parts))
                c.start()
                gathers[a].append(c)
        sends.extend(gathers[a])

    gather(0, out_x, rows_x)
    loads[2].wait()
    loads[3].wait()
    act, branch_slope = gelu_parts(gate_ref[...].astype(F32))
    mix_own[...] = (act * states_ref[...]).astype(BF)
    gather(1, out_c, rows_c)
    o = pltpu.make_async_copy(mix_own, mixed_all.at[mine], w_sem.at[3])
    o.start()
    o.wait()
    for i in range(6, 9):
        loads[i].wait()
    for c in gathers[0]:
        c.wait_recv()
    row_data = rows_x[...].reshape(size, model)
    pre_gate = jnp.dot(row_data, wg[...], preferred_element_type=F32)
    pre_up = jnp.dot(row_data, wu[...], preferred_element_type=F32)
    active, slope = silu_parts(pre_gate)
    hidden = (active * pre_up).astype(BF)
    hid_ref[...] = hidden
    lean = pre_up * slope
    advance(0, 0)
    if depth > 2:
        advance(0, 1)
    for c in gathers[1]:
        c.wait_recv()
    grad_hidden = contract_cols(rows_c[...].reshape(size, model), wd[...])
    grad_pre_gate = (grad_hidden * lean).astype(BF)
    grad_pre_up = (grad_hidden * active).astype(BF)
    gpg_ref[...] = grad_pre_gate
    gpu_ref[...] = grad_pre_up
    for d in list(range(1, parts)) + [0]:
        part = near(width, lax.rem(col + d, parts))
        term = contract_cols(grad_pre_gate, wg[part, :]) + contract_cols(grad_pre_up, wu[part, :])
        terms[d] = term.astype(BF).reshape(groups, room, width)

    share_copies = {}
    order = list(range(1, groups)) + [0]
    for d in order if chunked else [0]:
        at = lax.rem(mine + d, groups)
        for p in range(1, parts):
            src = terms.at[p, at] if chunked else terms.at[p]
            dst = shares.at[p - 1, at] if chunked else shares.at[p - 1]
            c = remote(src, dst, s_send.at[d, p], s_recv.at[d, p], "tp", lax.rem(col + p, parts))
            c.start()
            share_copies[d, p] = c
            sends.append(c)
    for step in range(2, depth - 1):
        advance(0, step)
    chain(1, 0)
    across(1, 0, 0, "start")

    back_copies = []
    for d in order:
        at = lax.rem(mine + d, groups)
        if chunked or d == 1:
            for p in range(1, parts):
                share_copies[d if chunked else 0, p].wait_recv()
        total = terms[0, at].astype(F32)
        for p in range(1, parts):
            total = total + shares[p - 1, at].astype(F32)
        if d == 0:
            back[mine] = total.astype(BF)
        else:
            summed[d] = total.astype(BF)
            c = remote(summed.at[d], back.at[mine], r_send.at[d], r_recv.at[d], "sp", at)
            c.start()
            back_copies.append(c)
    nxt = lax.rem(mine + 1, groups)
    prev_copy = remote(states_ref.at[pl.ds(toks - 8, 8)], prev_in, p_send, p_recv, "sp", nxt)
    prev_copy.start()
    advance(1, 0)
    rows = lax.broadcasted_iota(jnp.int32, (toks, toks), 0)
    cols = lax.broadcasted_iota(jnp.int32, (toks, toks), 1)
    eye = jnp.where(rows == cols, 1.0, 0.0).astype(BF)
    total = contract_rows(cot_ref[...], eye)
    for c in back_copies:
        c.wait_recv()
    total = total + contract_rows(back[...].reshape(size, width), picked)
    flipped[here, :] = total.astype(BF)
    grad_copies = []
    for d in range(1, parts):
        part = flipped.at[here]
        c = remote(part, part, g_send.at[d], g_recv.at[d], "tp", lax.rem(col + d, parts))
        c.start()
        grad_copies.append(c)
    for step in range(1, depth - 1):
        advance(1, step)
    collected(0)
    loads[5].wait()
    for c in grad_copies:
        c.wait_recv()
    high = model // groups
    block_copies = []
    for d in range(1, groups):
        peer = lax.rem(mine + d, groups)
        c = remote(flipped.at[near(high, peer)], blocks.at[mine], b_send.at[d], b_recv.at[d], "sp", peer)
        c.start()
        block_copies.append(c)
    grad_mixed = contract_rows(flipped[...], proj_all[...].reshape(model, states_ref.shape[1]))
    states = states_ref[...]
    act, branch_slope = gelu_parts(gate_ref[...].astype(F32))
    decays = jnp.exp(decay_ref[...])
    ggate_ref[...] = (grad_mixed * states * branch_slope).astype(BF)
    local = grad_mixed * act
    line = lax.broadcasted_iota(jnp.int32, local.shape, 0)
    span = jnp.where(line < toks - 1, pltpu.roll(decays, toks - 1, 0), 1.0)
    k = 1
    while k < toks:
        inside = line < toks - k
        local = local + span * jnp.where(inside, pltpu.roll(local, toks - k, 0), 0.0)
        span = span * jnp.where(inside, pltpu.roll(span, toks - k, 0), 1.0)
        k *= 2
    eight = lax.broadcasted_iota(jnp.int32, (8, local.shape[1]), 0)
    whole = span[0:1] * decays[0:1]
    entry = local[0:1] * decays[0:1]
    carry_own[...] = jnp.where(eight == 0, whole, entry)
    carry_copies = []
    for d in range(1, groups):
        peer = lax.rem(mine + d, groups)
        c = remote(carry_own, carry_in.at[d - 1], k_send.at[d], k_recv.at[d], "sp", peer)
        c.start()
        carry_copies.append(c)
    collected(1)
    total = jnp.dot(flipped[near(high, mine), :], mixed_all[mine], preferred_element_type=F32)
    for d in range(1, groups):
        block_copies[d - 1].wait_recv()
        at = lax.rem(mine + groups - d, groups)
        total = total + jnp.dot(blocks[at], mixed_all[at], preferred_element_type=F32)
    outp_ref[...] = total
    prev_copy.wait_recv()
    first = jnp.where(mine > 0, prev_in[7:8, :], 0.0)
    prev = jnp.where(line == 0, first, pltpu.roll(states, 1, 0))
    for c in carry_copies:
        c.wait_recv()
    carried = jnp.zeros_like(whole)
    for ahead in range(groups - 1, 0, -1):
        got = carry_in[groups - ahead - 1]
        carried = jnp.where(mine + ahead < groups, got[1:2] + got[0:1] * carried, carried)
    grad_in = local + span * carried
    gin_ref[...] = grad_in
    gdecay_ref[...] = (grad_in * decays * prev).astype(BF)
    settle(0)
    settle(1)
    for c in [prev_copy] + sends + back_copies + grad_copies + block_copies + carry_copies:
        c.wait_send()


def finish_kernel(
    rx, rc, hid, gpg, gpu, outp, ggate, gdecay, gin,
    gg_out, gu_out, gd_out, outp_out, ggate_out, gdecay_out, gin_out,
    gg, gu, gd, sems, small_sems,
):
    stores = []
    for i, (src, dst) in enumerate((
        (outp, outp_out), (ggate, ggate_out), (gdecay, gdecay_out), (gin, gin_out),
    )):
        o = pltpu.make_async_copy(src, dst, small_sems.at[i])
        o.start()
        stores.append(o)
    step = 256
    steps = rx.shape[1] // step
    for i in range(steps):
        part = slice(i * step, (i + 1) * step)
        for kind, grad, buf, out in ((0, gpg, gg, gg_out), (1, gpu, gu, gu_out)):
            buf[part, :] = contract_rows(rx[:, part], grad[...])
            pltpu.make_async_copy(buf.at[part], out.at[part], sems.at[kind]).start()
        gd[:, part] = contract_rows(hid[...], rc[:, part])
        pltpu.make_async_copy(gd.at[:, part], gd_out.at[:, part], sems.at[2]).start()
    for kind, (buf, out) in enumerate(((gg, gg_out), (gu, gu_out), (gd, gd_out))):
        pltpu.make_async_copy(buf, out, sems.at[kind]).wait()
    for o in stores:
        o.wait()


def finish(rx, rc, hid, gpg, gpu, *small):
    size, model = rx.shape
    units = hid.shape[1]
    vmem = pl.BlockSpec(memory_space=pltpu.VMEM)
    hbm = pl.BlockSpec(memory_space=pltpu.HBM)
    grads = [(model, units), (model, units), (units, model)]
    outs = pl.pallas_call(
        finish_kernel,
        out_shape=[jax.ShapeDtypeStruct(g, F32) for g in grads]
        + [jax.ShapeDtypeStruct(a.shape, a.dtype) for a in small],
        in_specs=[vmem] * (5 + len(small)),
        out_specs=[hbm] * (3 + len(small)),
        scratch_shapes=[pltpu.VMEM(g, F32) for g in grads]
        + [pltpu.SemaphoreType.DMA((3,)), pltpu.SemaphoreType.DMA((len(small),))],
        compiler_params=pltpu.CompilerParams(vmem_limit_bytes=40 * 1024 * 1024),
        name="finish",
    )(rx, rc, hid, gpg, gpu, *small)
    return tuple(out[None] for out in outs[:3]) + tuple(outs[3:])


def shards(
    moe_input, cotangent, routes, route_weights, gate_branch, log_decay, states,
    w_gate, w_up, w_down, out_proj,
):
    groups, parts = lax.axis_size("sp"), lax.axis_size("tp")
    tok_rows, picks = routes.shape
    width = moe_input.shape[1]
    model = width * parts
    units = w_gate.shape[2]
    chans = states.shape[1]
    room = tok_rows * picks * 5 // (4 * groups)
    room = (room + 7) // 8 * 8
    depth = groups // CORES
    high = out_proj.shape[0]
    chunked = groups * parts <= 64
    chunks = groups if chunked else 1
    vmem = pl.BlockSpec(memory_space=pltpu.VMEM)
    hbm = pl.BlockSpec(memory_space=pltpu.HBM)
    dma = pltpu.SemaphoreType.DMA

    def run(*refs):
        whole_kernel(groups, parts, room, chunked, *refs)

    def buf(*shape, kind=BF):
        return pltpu.VMEM(shape, kind)

    outs = pl.pallas_call(
        run,
        out_shape=[
            jax.ShapeDtypeStruct((groups, room, model), BF),
            jax.ShapeDtypeStruct((groups, room, model), BF),
            jax.ShapeDtypeStruct((groups * room, units), BF),
            jax.ShapeDtypeStruct((groups * room, units), BF),
            jax.ShapeDtypeStruct((groups * room, units), BF),
            jax.ShapeDtypeStruct((high, chans), F32),
            jax.ShapeDtypeStruct((tok_rows, chans), BF),
            jax.ShapeDtypeStruct((tok_rows, chans), BF),
            jax.ShapeDtypeStruct((tok_rows, chans), F32),
        ],
        in_specs=[vmem] * 2 + [hbm] * 9,
        out_specs=[vmem] * 9,
        scratch_shapes=[
            buf(tok_rows, width), buf(tok_rows, width), buf(tok_rows, chans),
            buf(tok_rows, chans, kind=F32), buf(tok_rows, chans, kind=F32),
            buf(model, units), buf(model, units), buf(units, model),
            buf(groups, room, width), buf(groups, room, width),
            buf(groups, high, chans), buf(groups, tok_rows, chans), buf(tok_rows, chans),
            buf(parts, groups, room, width), buf(parts - 1, groups, room, width),
            buf(groups, room, width), buf(groups, room, width),
            buf(model, tok_rows), buf(groups, high, tok_rows),
            buf(8, chans, kind=F32), buf(groups - 1, 8, chans, kind=F32), buf(8, chans, kind=F32),
        ]
        + [dma((2, groups))] * 2 + [dma((2, chunks, parts))] * 2 + [dma((2, 2, depth))] * 4
        + [dma((chunks, parts))] * 2 + [dma((groups,))] * 2 + [dma((parts,))] * 2
        + [dma((groups,))] * 4 + [dma(())] * 2 + [dma((9,)), dma((4,))],
        compiler_params=pltpu.CompilerParams(
            collective_id=0, has_side_effects=True, vmem_limit_bytes=40 * 1024 * 1024),
        name="backward",
    )(
        routes.T, route_weights.T,
        *(pltpu.with_memory_space_constraint(a, pltpu.HBM) for a in (
            moe_input, cotangent, gate_branch, states, log_decay, out_proj, w_gate, w_up, w_down)),
    )
    rx, rc = (out.reshape(groups * room, model) for out in outs[:2])
    return finish(rx, rc, *outs[2:])


def flip(index, mask, count):
    total, bit = 0, 1
    while bit < count:
        here = lax.rem(lax.div(index, bit), 2)
        total = total + bit * ((1 - here) if mask & bit else here)
        bit *= 2
    return total


def plane_kernel(
    groups, parts, room,
    routes_any, weights_any, x_any, cot_any, gate_any, states_any, decay_any, proj_any,
    wg_any, wu_any, wd_any,
    rows_x, rows_c, hid_ref, gpg_ref, gpu_ref, outp_ref, ggate_ref, gdecay_ref, gin_ref,
    routes_ref, weights_ref, x_ref, cot_ref, gate_ref, states_ref, decay_ref, wg, wu, wd,
    out_x, out_c, picked_ref, proj_all, mixed_all, act_ref, slope_ref, active_ref, lean_ref,
    terms, shares, passed, summed, back, cot_turned, cot_mine, flipped, blocks, levels, span_ref, past_ref,
    carry_own, carry_in, prev_in,
    o_send, a_recv, t_recv, e_recv, s_recv, m_recv, z_send, z_recv, c_recv, p_send, p_recv, l_sem,
):
    mine, col = lax.axis_index("sp"), lax.axis_index("tp")
    toks, width = x_ref.shape
    model = rows_x.shape[2]
    chans = states_ref.shape[1]
    units = hid_ref.shape[2]
    depth = groups // CORES
    z, core = mine // CORES, lax.rem(mine, CORES)
    size = groups * room
    half = groups // 2
    rows_half = half * room
    inner = jnp.logical_and(z >= 1, z + 1 < depth)

    barrier = pltpu.get_barrier_semaphore()
    for d in range(1, groups):
        pl.semaphore_signal(
            barrier, inc=1, device_id={"sp": lax.rem(mine + d, groups)},
            device_id_type=pl.DeviceIdType.MESH,
        )
    for d in range(1, parts):
        pl.semaphore_signal(
            barrier, inc=1, device_id={"tp": lax.rem(col + d, parts)},
            device_id_type=pl.DeviceIdType.MESH,
        )

    loads = []
    for i, (s, t) in enumerate((
        (x_any, x_ref), (cot_any, cot_ref), (gate_any, gate_ref), (states_any, states_ref),
        (proj_any, proj_all.at[mine]), (decay_any, decay_ref),
        (wg_any.at[0], wg), (wu_any.at[0], wu), (wd_any.at[0], wd),
        (routes_any, routes_ref), (weights_any, weights_ref),
    )):
        loads.append(pltpu.make_async_copy(s, t, l_sem.at[i]))
    for i in (9, 10, 0, 1, 4, 2, 3, 6, 7, 8, 5):
        loads[i].start()

    def near(width_of, index):
        return pl.ds(pl.multiple_of(index * width_of, width_of), width_of)

    def send(src, dst, send_sem, recv_sem, axis, peer):
        c = remote(src, dst, send_sem, recv_sem, axis, peer)
        c.start()
        return c

    def all_sent(ref, sem):
        remote(ref, ref, sem, sem, "tp", tile[1]).wait_send()

    def all_here(ref, sem):
        remote(ref, ref, sem, sem, "tp", tile[1]).wait_recv()

    group = [flip(mine, d, groups) for d in range(groups)]
    tile = [flip(col, p, parts) for p in range(parts)]
    here = near(width, col)

    loads[9].wait()
    loads[10].wait()
    picked, weight = selection(routes_ref[...], weights_ref[...], groups, room)
    picked_ref[...] = picked
    arrivals = [[None] * groups for _ in range(2)]
    gathers = [[None] * groups for _ in range(2)]
    sources = ((out_x, rows_x), (out_c, rows_c))

    def spread(a):
        src, dst = sources[a]
        for d in range(1, groups):
            arrivals[a][d] = send(
                src.at[group[d]], dst.at[mine, :, here], o_send.at[a], a_recv.at[a, d - 1], "sp", group[d])
        dst[mine, :, here] = src[mine]

    def share_out(a, d):
        src, dst = sources[a]
        if d:
            arrivals[a][d].wait_recv()
        own = dst.at[group[d], :, here] if d else src.at[mine]
        gathers[a][d] = [
            send(own, dst.at[group[d], :, here], o_send.at[2 + a],
                 t_recv.at[a, d] if k == d % 2 else e_recv.at[a, d // half], "tp", tile[k + 1])
            for k in range(2)
        ]

    def relay(a, d):
        dst = sources[a][1]
        k = d % 2
        gathers[a][d][k].wait_recv()
        ref = dst.at[group[d], :, near(width, tile[k + 1])]
        send(ref, ref, o_send.at[2 + a], e_recv.at[a, d // half], "tp", tile[2 - k])

    def landed(a, h):
        all_here(sources[a][1].at[pl.ds(0, groups // parts)], e_recv.at[a, h])

    loads[0].wait()
    got = jnp.dot(picked, x_ref[...], preferred_element_type=F32).astype(BF)
    for e in range(groups):
        out_x[e] = got[e * room : (e + 1) * room]
    pl.semaphore_wait(barrier, groups + parts - 2)
    spread(0)
    share_out(0, 0)
    loads[1].wait()
    got = jnp.dot(picked, cot_ref[...], preferred_element_type=F32)
    got = (got * weight).astype(BF)
    for e in range(groups):
        out_c[e] = got[e * room : (e + 1) * room]
    spread(1)

    pairs = (proj_all, mixed_all)

    def chain(a, step, wait=False, middle=None):
        buf = pairs[a]
        right = buf.at[jnp.maximum(z - step, 0) * CORES + core]
        left = buf.at[jnp.minimum(z + step, depth - 1) * CORES + core]
        up = jnp.minimum(z + 1, depth - 1) * CORES + core
        down = jnp.maximum(z - 1, 0) * CORES + core
        for way, ref, peer, ok, within in (
            (0, right, up, jnp.logical_and(z - step >= 0, z + 1 < depth),
             jnp.logical_and(z >= 1, z + 2 < depth)),
            (1, left, down, jnp.logical_and(z + step < depth, z >= 1),
             jnp.logical_and(z >= 2, z + 1 < depth)),
        ):
            if middle is not None:
                ok = jnp.logical_and(ok, within if middle else jnp.logical_not(within))

            @pl.when(ok)
            def _(way=way, ref=ref, peer=peer):
                c = remote(ref, ref, z_send.at[a, way, step], z_recv.at[a, way, step], "sp", peer)
                c.wait_send() if wait else c.start()

    partner = z * CORES + (1 - core)

    def across(a, step, way, start=True, also=None):
        ok = z - step >= 0 if way == 0 else z + step < depth
        if also is not None:
            ok = jnp.logical_and(ok, also)
        zz = jnp.maximum(z - step, 0) if way == 0 else jnp.minimum(z + step, depth - 1)
        ref = pairs[a].at[zz * CORES + (core if start else 1 - core)]
        sem = c_recv.at[1 + way * depth + step if a else 0]

        @pl.when(ok)
        def _():
            c = remote(ref, ref, o_send.at[4 + a], sem, "sp", partner)
            c.start() if start else c.wait_recv()

    def advance(a, step, also=None):
        buf = pairs[a]
        from_l = buf.at[jnp.maximum(z - 1 - step, 0) * CORES + core]
        from_r = buf.at[jnp.minimum(z + 1 + step, depth - 1) * CORES + core]
        for way, ok, ref in ((0, z - 1 - step >= 0, from_l), (1, z + 1 + step < depth, from_r)):
            @pl.when(ok if also is None else jnp.logical_and(ok, also))
            def _(way=way, ref=ref):
                remote(ref, ref, z_send.at[a, way, step], z_recv.at[a, way, step],
                       "sp", lax.rem(mine + 1, groups)).wait_recv()
                if step + 1 < depth - 1:
                    forward_to = (z + 1 < depth) if way == 0 else (z >= 1)
                    peer = jnp.minimum(z + 1, depth - 1) if way == 0 else jnp.maximum(z - 1, 0)

                    @pl.when(forward_to)
                    def _():
                        remote(ref, ref, z_send.at[a, way, step + 1], z_recv.at[a, way, step + 1],
                               "sp", peer * CORES + core).start()
        across(a, step + 1, 0, also=also)
        across(a, step + 1, 1, also=also)

    def settle(a):
        for step in range(depth - 1):
            chain(a, step, True)
        all_sent(pairs[a].at[pl.ds(0, depth)], o_send.at[4 + a])

    def collected(step):
        for way in range(2):
            if step or not way:
                across(1, step, way, start=False)

    loads[4].wait()
    chain(0, 0)
    across(0, 0, 0)
    share_out(1, 0)
    share_out(0, 1)
    loads[3].wait()
    prev_copy = send(
        states_ref.at[pl.ds(toks - 8, 8)], prev_in, p_send, p_recv, "sp", lax.rem(mine + 1, groups))

    loads[2].wait()
    act, branch_slope = gelu_parts(gate_ref[...].astype(F32))
    states = states_ref[...]
    act_ref[...] = act
    slope_ref[...] = branch_slope * states
    mixed_all[mine] = (act * states).astype(BF)
    chain(1, 0, middle=False)
    across(1, 0, 0)
    share_out(1, 1)
    share_out(0, 2)
    share_out(0, 3)
    for a in range(2):
        relay(a, 0)
        relay(a, 1)
    queue = [(0, d) for d in range(2, groups)] + [(1, d) for d in range(2, groups)]
    ahead = queue[2:]

    def pump(count):
        for _ in range(count):
            for _ in range(2):
                if ahead:
                    share_out(*ahead.pop(0))
            for _ in range(2):
                if queue:
                    relay(*queue.pop(0))

    pump(half)

    first = [lax.div(mine, half) * half, (1 - lax.div(mine, half)) * half]

    def forward(h):
        landed(0, h)
        at = pl.ds(first[h], half)
        data = rows_x[at].reshape(rows_half, model)
        pre_gate = jnp.dot(data, wg[...].reshape(model, units), preferred_element_type=F32)
        pre_up = jnp.dot(data, wu[...].reshape(model, units), preferred_element_type=F32)
        active, slope = silu_parts(pre_gate)
        hid_ref[at] = (active * pre_up).astype(BF).reshape(half, room, units)
        active_ref[h] = active
        lean_ref[h] = pre_up * slope

    def hidden_grads(h):
        landed(1, h)
        at = pl.ds(first[h], half)
        grad_hidden = contract_cols(rows_c[at].reshape(rows_half, model), wd[...])
        gpg_ref[at] = (grad_hidden * lean_ref[h]).astype(BF).reshape(half, room, units)
        gpu_ref[at] = (grad_hidden * active_ref[h]).astype(BF).reshape(half, room, units)

    def input_grads(h):
        at = pl.ds(first[h], half)
        gate_part = gpg_ref[at].reshape(rows_half, units)
        up_part = gpu_ref[at].reshape(rows_half, units)
        for p in list(range(1, parts)) + [0]:
            term = contract_cols(gate_part, wg[:, tile[p]].reshape(width, units))
            term = term + contract_cols(up_part, wu[:, tile[p]].reshape(width, units))
            terms[p, at] = term.astype(BF).reshape(half, room, width)

    share_copies = {}

    def reduce_out(d):
        g, near_tile = group[d], 1 + d % 2
        share_copies[d] = [
            send(terms.at[p, g], shares.at[i, g], o_send.at[7], s_recv.at[d, i], "tp", tile[near_tile])
            for i, p in enumerate((3, near_tile))
        ]

    def pass_on(d):
        g, far_tile = group[d], 2 - d % 2
        share_copies[d][0].wait_recv()
        passed[g] = (terms[far_tile, g].astype(F32) + shares[0, g].astype(F32)).astype(BF)
        send(passed.at[g], shares.at[2, g], o_send.at[7], s_recv.at[d, 1], "tp", tile[far_tile])

    def bring_back(d):
        g = group[d]
        all_here(shares.at[pl.ds(1, 2), g], s_recv.at[d, 1])
        total = terms[0, g].astype(F32) + shares[1, g].astype(F32) + shares[2, g].astype(F32)
        if d == 0:
            back[mine] = total.astype(BF)
        else:
            summed[d] = total.astype(BF)
            send(summed.at[d], back.at[mine], o_send.at[8], m_recv.at[1], "sp", g)

    for i in (6, 7, 8):
        loads[i].wait()
    forward(0)
    pump(1)
    advance(0, 0)
    chain(1, 0, middle=True)
    forward(1)

    rows = lax.broadcasted_iota(jnp.int32, (toks, toks), 0)
    cols = lax.broadcasted_iota(jnp.int32, (toks, toks), 1)
    eye = jnp.where(rows == cols, 1.0, 0.0).astype(BF)
    fine = cot_turned.shape[2]
    cot_turned[...] = contract_rows(cot_ref[...], eye).astype(BF).reshape(cot_turned.shape)
    cot_mine[col] = cot_turned[:, col]

    hidden_grads(0)
    pump(1)
    for p in range(1, parts):
        send(cot_turned.at[:, tile[p]], cot_mine.at[col], o_send.at[6], m_recv.at[0], "tp", tile[p])
    input_grads(0)
    order = list(range(2, half)) + [1, 0] + list(range(half, groups))
    early = [d for d in order if d < half]
    for d in early:
        reduce_out(d)
    hidden_grads(1)
    for d in early[:2]:
        pass_on(d)
    input_grads(1)
    for d in order:
        if d not in early:
            reduce_out(d)
    for d in early[2:]:
        pass_on(d)

    loads[5].wait()
    prev_copy.wait_recv()
    decays = jnp.exp(decay_ref[...])
    line = lax.broadcasted_iota(jnp.int32, decays.shape, 0)
    before = jnp.where(mine > 0, prev_in[7:8, :], 0.0)
    past_ref[...] = decays * jnp.where(line == 0, before, pltpu.roll(states_ref[...], 1, 0))
    span = jnp.where(line < toks - 1, pltpu.roll(decays, toks - 1, 0), 1.0)
    k, level = 1, 0
    while k < toks:
        inside = line < toks - k
        levels[level] = jnp.where(inside, span, 0.0)
        span = span * jnp.where(inside, pltpu.roll(span, toks - k, 0), 1.0)
        k *= 2
        level += 1
    span_ref[...] = span
    head = decays[0:1]

    late = [d for d in order if d not in early]
    for d in order:
        if late:
            pass_on(late.pop(0))
        bring_back(d)
    for step in range(1, depth - 2):
        advance(0, step)
    all_here(cot_turned.at[:, pl.ds(0, parts - 1)], m_recv.at[0])
    total = cot_mine[...].reshape(width, toks).astype(F32)
    all_here(back.at[pl.ds(0, groups - 1)], m_recv.at[1])
    total = total + contract_rows(back[...].reshape(size, width), picked_ref[...])
    flipped[:, col] = total.astype(BF).reshape(groups, fine, toks)

    def plane_start(buf, first_sem):
        part = buf.at[:, col]
        return [
            send(part, part, o_send.at[first_sem // 3 + 8], m_recv.at[first_sem + p], "tp", tile[p])
            for p in (1, 2)
        ]

    def plane_relay(buf, copies, first_sem):
        for p in (1, 2):
            copies[p - 1].wait_recv()
            part = buf.at[pl.ds((p - 1) * half, half), tile[p]]
            send(part, part, o_send.at[first_sem // 3 + 8], m_recv.at[first_sem], "tp", tile[3 - p])

    grad_copies = plane_start(flipped, 3)
    for d in range(1, groups):
        send(flipped.at[group[d], col], blocks.at[mine, col], o_send.at[11], m_recv.at[2], "sp", group[d])
    blocks[mine, col] = flipped[mine, col]
    advance(1, 0)
    plane_relay(flipped, grad_copies, 3)
    all_here(blocks.at[pl.ds(0, groups - 1), 0], m_recv.at[2])
    plane_copies = plane_start(blocks, 6)
    advance(0, depth - 2)
    for step in range(1, depth - 2):
        advance(1, step, inner)
    all_here(flipped.at[:, 0], m_recv.at[3])
    all_here(proj_all.at[pl.ds(0, depth)], c_recv.at[0])
    grad_mixed = contract_rows(flipped[...].reshape(model, toks), proj_all[...].reshape(model, chans))
    ggate_ref[...] = (grad_mixed * slope_ref[...]).astype(BF)
    local = grad_mixed * act_ref[...]
    k, level = 1, 0
    while k < toks:
        local = local + levels[level] * pltpu.roll(local, toks - k, 0)
        k *= 2
        level += 1
    eight = lax.broadcasted_iota(jnp.int32, (8, chans), 0)
    carry_own[...] = jnp.where(eight == 0, span_ref[0:1, :] * head, local[0:1] * head)
    for d in range(1, groups):
        send(carry_own, carry_in.at[d - 1], o_send.at[12], m_recv.at[9], "sp", lax.rem(mine + d, groups))
    plane_relay(blocks, plane_copies, 6)
    for step in range(1, depth - 2):
        advance(1, step, jnp.logical_not(inner))
    for step in range(depth - 1):
        collected(step)
    all_here(blocks.at[:, 0], m_recv.at[6])
    high = blocks.shape[1] * blocks.shape[2]

    def out_part(t):
        return jnp.dot(blocks[t].reshape(high, toks), mixed_all[t], preferred_element_type=F32)

    near_part = out_part(group[0])
    for d in range(1, groups - CORES):
        near_part = near_part + out_part(group[d])
    outp_ref[...] = near_part
    all_here(carry_in, m_recv.at[9])
    carried = jnp.zeros((1, chans), F32)
    for ahead in range(groups - 1, 0, -1):
        got = carry_in[groups - ahead - 1]
        carried = jnp.where(mine + ahead < groups, got[1:2] + got[0:1] * carried, carried)
    grad_in = local + span_ref[...] * carried
    gin_ref[...] = grad_in
    gdecay_ref[...] = (grad_in * past_ref[...]).astype(BF)
    advance(1, depth - 2)
    collected(depth - 1)
    far_part = out_part(group[groups - CORES])
    for d in range(groups - CORES + 1, groups):
        far_part = far_part + out_part(group[d])
    outp_ref[...] += far_part
    settle(0)
    settle(1)
    for a in range(2):
        all_sent(rows_x.at[pl.ds(0, groups - 1), :, pl.ds(0, width)], o_send.at[a])
        all_sent(rows_x.at[pl.ds(0, groups * 3 // parts)], o_send.at[2 + a])
    all_sent(cot_turned.at[:, pl.ds(0, parts - 1)], o_send.at[6])
    all_sent(rows_x.at[pl.ds(0, groups * 3 // parts)], o_send.at[7])
    all_sent(back.at[pl.ds(0, groups - 1)], o_send.at[8])
    for i in (9, 10):
        all_sent(flipped.at[:, pl.ds(0, 3)], o_send.at[i])
    all_sent(blocks.at[pl.ds(0, groups - 1), 0], o_send.at[11])
    all_sent(carry_in, o_send.at[12])
    prev_copy.wait_send()


def plane_shards(
    moe_input, cotangent, routes, route_weights, gate_branch, log_decay, states,
    w_gate, w_up, w_down, out_proj,
):
    groups, parts = lax.axis_size("sp"), lax.axis_size("tp")
    tok_rows, picks = routes.shape
    width = moe_input.shape[1]
    model = width * parts
    units = w_gate.shape[2]
    chans = states.shape[1]
    room = tok_rows * picks * 5 // (4 * groups)
    room = (room + 7) // 8 * 8
    depth = groups // CORES
    high = out_proj.shape[0]
    fine = high // parts
    doublings = (tok_rows - 1).bit_length()
    vmem = pl.BlockSpec(memory_space=pltpu.VMEM)
    hbm = pl.BlockSpec(memory_space=pltpu.HBM)
    dma = pltpu.SemaphoreType.DMA

    def run(*refs):
        plane_kernel(groups, parts, room, *refs)

    def buf(*shape, kind=BF):
        return pltpu.VMEM(shape, kind)

    def split(weight):
        return weight.reshape(1, groups, parts, fine, units)

    outs = pl.pallas_call(
        run,
        out_shape=[
            jax.ShapeDtypeStruct((groups, room, model), BF),
            jax.ShapeDtypeStruct((groups, room, model), BF),
            jax.ShapeDtypeStruct((groups, room, units), BF),
            jax.ShapeDtypeStruct((groups, room, units), BF),
            jax.ShapeDtypeStruct((groups, room, units), BF),
            jax.ShapeDtypeStruct((high, chans), F32),
            jax.ShapeDtypeStruct((tok_rows, chans), BF),
            jax.ShapeDtypeStruct((tok_rows, chans), BF),
            jax.ShapeDtypeStruct((tok_rows, chans), F32),
        ],
        in_specs=[hbm] * 11,
        out_specs=[vmem] * 9,
        scratch_shapes=[
            buf(picks, tok_rows, kind=jnp.int32), buf(picks, tok_rows, kind=F32),
            buf(tok_rows, width), buf(tok_rows, width), buf(tok_rows, chans),
            buf(tok_rows, chans, kind=F32), buf(tok_rows, chans, kind=F32),
            buf(groups, parts, fine, units), buf(groups, parts, fine, units), buf(units, model),
            buf(groups, room, width), buf(groups, room, width), buf(groups * room, tok_rows),
            buf(groups, high, chans), buf(groups, tok_rows, chans),
            buf(tok_rows, chans, kind=F32), buf(tok_rows, chans, kind=F32),
            buf(2, groups // 2 * room, units, kind=F32), buf(2, groups // 2 * room, units, kind=F32),
            buf(parts, groups, room, width), buf(parts - 1, groups, room, width),
            buf(groups, room, width), buf(groups, room, width), buf(groups, room, width),
            buf(groups // parts, parts, fine, tok_rows), buf(parts, groups // parts, fine, tok_rows),
            buf(groups, parts, fine, tok_rows), buf(groups, parts, fine, tok_rows),
            buf(doublings, tok_rows, chans, kind=F32), buf(tok_rows, chans, kind=F32),
            buf(tok_rows, chans, kind=F32),
            buf(8, chans, kind=F32), buf(groups - 1, 8, chans, kind=F32), buf(8, chans, kind=F32),
        ]
        + [dma((13,)), dma((2, groups - 1)), dma((2, groups)), dma((2, 2)), dma((groups, 2))]
        + [dma((10,)), dma((2, 2, depth - 1)), dma((2, 2, depth - 1)), dma((1 + 2 * depth,))]
        + [dma(()), dma(()), dma((11,))],
        compiler_params=pltpu.CompilerParams(
            collective_id=0, has_side_effects=True, vmem_limit_bytes=40 * 1024 * 1024),
        name="backward",
    )(
        *(pltpu.with_memory_space_constraint(a, pltpu.HBM) for a in (
            routes.T, route_weights.T, moe_input, cotangent, gate_branch, states, log_decay, out_proj,
            split(w_gate), split(w_up), w_down)),
    )
    rx, rc = (out.reshape(groups * room, model) for out in outs[:2])
    grads = (out.reshape(groups * room, units) for out in outs[2:5])
    return finish(rx, rc, *grads, *outs[5:])


def solution(mesh):
    groups, parts = mesh.shape["sp"], mesh.shape["tp"]
    plane = parts == 4 and groups % parts == 0 and groups & (groups - 1) == 0
    return jax.shard_map(
        plane_shards if plane else shards,
        mesh=mesh,
        in_specs=(
            P("sp", "tp"), P("sp", "tp"), P("sp", None), P("sp", None), P("sp", "tp"),
            P("sp", "tp"), P("sp", "tp"), P("sp", None, "tp"), P("sp", None, "tp"),
            P("sp", "tp", None), P("sp", "tp"),
        ),
        out_specs=(
            P("sp", None, "tp"), P("sp", None, "tp"), P("sp", "tp", None), P("sp", "tp"),
            P("sp", "tp"), P("sp", "tp"), P("sp", "tp"),
        ),
        check_vma=False,
    )
```

```python
import jax
import jax.numpy as jnp
from jax import lax
from jax.experimental import pallas as pl
from jax.experimental.pallas import tpu as pltpu
from jax.sharding import PartitionSpec as P

BF = jnp.bfloat16
F32 = jnp.float32
CORES = 2
GELU_C = 0.7978845608028654
GELU_A = 0.044715


def silu_parts(pre_gate):
    sigmoid_val = jax.nn.sigmoid(pre_gate)
    return (pre_gate * sigmoid_val, sigmoid_val * (1.0 + pre_gate * (1.0 - sigmoid_val)))


def contract_rows(left_mat, right_mat):
    return lax.dot_general(
        left_mat, right_mat, (((0,), (0,)), ((), ())), preferred_element_type=F32
    )


def contract_cols(left_mat, right_mat):
    return lax.dot_general(
        left_mat, right_mat, (((1,), (1,)), ((), ())), preferred_element_type=F32
    )


def gelu_parts(x):
    t = jnp.tanh(GELU_C * (x + GELU_A * (x * x * x)))
    half = 0.5 * (1.0 + t)
    slope = half + 0.5 * x * (1.0 - t * t) * (GELU_C * (1.0 + 3.0 * GELU_A * x * x))
    return x * half, slope


def selection(routes_t, weights_t, groups, room):
    picks, toks = routes_t.shape
    experts = lax.broadcasted_iota(jnp.int32, (groups, toks), 0)
    named = jnp.zeros((groups, toks), F32)
    weight = jnp.zeros((groups, toks), F32)
    for k in range(picks):
        hit = routes_t[k : k + 1, :] == experts
        named = named + jnp.where(hit, 1.0, 0.0)
        weight = weight + jnp.where(hit, weights_t[k : k + 1, :], 0.0)
    rows = lax.broadcasted_iota(jnp.int32, (toks, toks), 0)
    cols = lax.broadcasted_iota(jnp.int32, (toks, toks), 1)
    before = jnp.where(rows < cols, 1.0, 0.0).astype(BF)
    slot = jnp.dot(named.astype(BF), before, preferred_element_type=F32)
    slot = jnp.where(named > 0.5, slot, -1.0)
    place = lax.broadcasted_iota(jnp.int32, (room, toks), 0).astype(F32)
    picked, column = [], []
    for e in range(groups):
        one = jnp.where(slot[e : e + 1, :] == place, 1.0, 0.0)
        picked.append(one)
        column.append(jnp.sum(one * weight[e : e + 1, :], axis=1, keepdims=True))
    return jnp.concatenate(picked, axis=0).astype(BF), jnp.concatenate(column, axis=0)


def greet(groups, parts, mine, col):
    barrier = pltpu.get_barrier_semaphore()
    for d in range(1, groups):
        pl.semaphore_signal(
            barrier, inc=1, device_id={"sp": lax.rem(mine + d, groups)},
            device_id_type=pl.DeviceIdType.MESH,
        )
    for d in range(1, parts):
        pl.semaphore_signal(
            barrier, inc=1, device_id={"tp": lax.rem(col + d, parts)},
            device_id_type=pl.DeviceIdType.MESH,
        )
    pl.semaphore_wait(barrier, groups + parts - 2)


def remote(src, dst, send, recv, axis, peer):
    return pltpu.make_async_remote_copy(
        src_ref=src, dst_ref=dst, send_sem=send, recv_sem=recv,
        device_id={axis: peer}, device_id_type=pl.DeviceIdType.MESH,
    )


def whole_kernel(
    groups, parts, room, chunked,
    routes_ref, weights_ref, x_any, cot_any, gate_any, states_any, decay_any, proj_any,
    wg_any, wu_any, wd_any,
    rows_x, rows_c, hid_ref, gpg_ref, gpu_ref, outp_ref, ggate_ref, gdecay_ref, gin_ref,
    x_ref, cot_ref, gate_ref, states_ref, decay_ref, wg, wu, wd,
    out_x, out_c, proj_all, mixed_all, mix_own,
    terms, shares, summed, back, flipped, blocks, carry_own, carry_in, prev_in,
    a_send, a_recv, t_send, t_recv, z_send, z_recv, c_send, c_recv,
    s_send, s_recv, r_send, r_recv, g_send, g_recv, b_send, b_recv, k_send, k_recv, p_send, p_recv,
    l_sem, w_sem,
):
    mine, col = lax.axis_index("sp"), lax.axis_index("tp")
    toks, width = x_ref.shape
    model = rows_x.shape[2]
    depth = groups // CORES
    z, core = mine // CORES, lax.rem(mine, CORES)
    size = groups * room

    def near(width_of, index):
        return pl.ds(pl.multiple_of(index * width_of, width_of), width_of)

    loads = []
    for i, (s, t) in enumerate((
        (x_any, x_ref), (cot_any, cot_ref), (gate_any, gate_ref), (states_any, states_ref),
        (proj_any, proj_all.at[mine]), (decay_any, decay_ref),
        (wg_any.at[0], wg), (wu_any.at[0], wu), (wd_any.at[0], wd),
    )):
        o = pltpu.make_async_copy(s, t, l_sem.at[i])
        o.start()
        loads.append(o)

    picked, weight = selection(routes_ref[...], weights_ref[...], groups, room)
    loads[0].wait()
    got = jnp.dot(picked, x_ref[...], preferred_element_type=F32).astype(BF)
    for e in range(groups):
        out_x[e] = got[e * room : (e + 1) * room]
    loads[1].wait()
    got_c = jnp.dot(picked, cot_ref[...], preferred_element_type=F32)
    got_c = (got_c * weight).astype(BF)
    for e in range(groups):
        out_c[e] = got_c[e * room : (e + 1) * room]
    greet(groups, parts, mine, col)

    here = near(width, col)
    sends, own = [], []
    arrivals = [[None] * groups for _ in range(2)]
    for a, (src, dst) in enumerate(((out_x, rows_x), (out_c, rows_c))):
        for d in range(1, groups):
            peer = lax.rem(mine + d, groups)
            c = remote(src.at[peer], dst.at[mine, :, here], a_send.at[a, d], a_recv.at[a, d], "sp", peer)
            c.start()
            arrivals[a][d] = c
            sends.append(c)
        o = pltpu.make_async_copy(src.at[mine], dst.at[mine, :, here], w_sem.at[a])
        o.start()
        own.append(o)

    pairs = (proj_all, mixed_all)

    def chain(a, step, wait=False):
        buf = pairs[a]
        right = buf.at[jnp.maximum(z - step, 0) * CORES + core]
        left = buf.at[jnp.minimum(z + step, depth - 1) * CORES + core]
        up = jnp.minimum(z + 1, depth - 1) * CORES + core
        down = jnp.maximum(z - 1, 0) * CORES + core
        for way, ref, peer, ok in (
            (0, right, up, jnp.logical_and(z - step >= 0, z + 1 < depth)),
            (1, left, down, jnp.logical_and(z + step < depth, z >= 1)),
        ):
            @pl.when(ok)
            def _(way=way, ref=ref, peer=peer):
                c = remote(ref, ref, z_send.at[a, way, step], z_recv.at[a, way, step], "sp", peer)
                c.wait_send() if wait else c.start()

    partner = z * CORES + (1 - core)

    def across(a, step, way, mode):
        ok = z - step >= 0 if way == 0 else z + step < depth
        zz = jnp.maximum(z - step, 0) if way == 0 else jnp.minimum(z + step, depth - 1)
        ref = pairs[a].at[zz * CORES + (1 - core if mode == "recv" else core)]

        @pl.when(ok)
        def _():
            c = remote(ref, ref, c_send.at[a, way, step], c_recv.at[a, way, step], "sp", partner)
            if mode == "start":
                c.start()
            elif mode == "send":
                c.wait_send()
            else:
                c.wait_recv()

    def advance(a, step):
        buf = pairs[a]
        from_l = buf.at[jnp.maximum(z - 1 - step, 0) * CORES + core]
        from_r = buf.at[jnp.minimum(z + 1 + step, depth - 1) * CORES + core]
        for way, ok, ref in ((0, z - 1 - step >= 0, from_l), (1, z + 1 + step < depth, from_r)):
            @pl.when(ok)
            def _(way=way, ref=ref):
                remote(ref, ref, z_send.at[a, way, step], z_recv.at[a, way, step],
                       "sp", lax.rem(mine + 1, groups)).wait_recv()
        if step + 1 < depth - 1:
            chain(a, step + 1)
        across(a, step + 1, 0, "start")
        across(a, step + 1, 1, "start")

    def settle(a):
        for step in range(depth - 1):
            chain(a, step, True)
        for step in range(depth):
            for way in range(2):
                if step or not way:
                    across(a, step, way, "send")

    def collected(a):
        for step in range(depth):
            for way in range(2):
                if step or not way:
                    across(a, step, way, "recv")

    loads[4].wait()
    chain(0, 0)
    across(0, 0, 0, "start")

    gathers = [[], []]

    def gather(a, src, dst):
        if chunked:
            for d in range(groups):
                at = lax.rem(mine + groups - d, groups)
                if d:
                    arrivals[a][d].wait_recv()
                for p in range(1, parts):
                    c = remote(dst.at[at, :, here] if d else src.at[mine], dst.at[at, :, here],
                               t_send.at[a, d, p], t_recv.at[a, d, p], "tp", lax.rem(col + p, parts))
                    c.start()
                    gathers[a].append(c)
            own[a].wait()
        else:
            own[a].wait()
            for d in range(1, groups):
                arrivals[a][d].wait_recv()
            for p in range(1, parts):
                c = remote(dst.at[:, :, here], dst.at[:, :, here],
                           t_send.at[a, 0, p], t_recv.at[a, 0, p], "tp", lax.rem(col + p, parts))
                c.start()
                gathers[a].append(c)
        sends.extend(gathers[a])

    gather(0, out_x, rows_x)
    loads[2].wait()
    loads[3].wait()
    act, branch_slope = gelu_parts(gate_ref[...].astype(F32))
    mix_own[...] = (act * states_ref[...]).astype(BF)
    gather(1, out_c, rows_c)
    o = pltpu.make_async_copy(mix_own, mixed_all.at[mine], w_sem.at[3])
    o.start()
    o.wait()
    for i in range(6, 9):
        loads[i].wait()
    for c in gathers[0]:
        c.wait_recv()
    row_data = rows_x[...].reshape(size, model)
    pre_gate = jnp.dot(row_data, wg[...], preferred_element_type=F32)
    pre_up = jnp.dot(row_data, wu[...], preferred_element_type=F32)
    active, slope = silu_parts(pre_gate)
    hidden = (active * pre_up).astype(BF)
    hid_ref[...] = hidden
    lean = pre_up * slope
    advance(0, 0)
    if depth > 2:
        advance(0, 1)
    for c in gathers[1]:
        c.wait_recv()
    grad_hidden = contract_cols(rows_c[...].reshape(size, model), wd[...])
    grad_pre_gate = (grad_hidden * lean).astype(BF)
    grad_pre_up = (grad_hidden * active).astype(BF)
    gpg_ref[...] = grad_pre_gate
    gpu_ref[...] = grad_pre_up
    for d in list(range(1, parts)) + [0]:
        part = near(width, lax.rem(col + d, parts))
        term = contract_cols(grad_pre_gate, wg[part, :]) + contract_cols(grad_pre_up, wu[part, :])
        terms[d] = term.astype(BF).reshape(groups, room, width)

    share_copies = {}
    order = list(range(1, groups)) + [0]
    for d in order if chunked else [0]:
        at = lax.rem(mine + d, groups)
        for p in range(1, parts):
            src = terms.at[p, at] if chunked else terms.at[p]
            dst = shares.at[p - 1, at] if chunked else shares.at[p - 1]
            c = remote(src, dst, s_send.at[d, p], s_recv.at[d, p], "tp", lax.rem(col + p, parts))
            c.start()
            share_copies[d, p] = c
            sends.append(c)
    for step in range(2, depth - 1):
        advance(0, step)
    chain(1, 0)
    across(1, 0, 0, "start")

    back_copies = []
    for d in order:
        at = lax.rem(mine + d, groups)
        if chunked or d == 1:
            for p in range(1, parts):
                share_copies[d if chunked else 0, p].wait_recv()
        total = terms[0, at].astype(F32)
        for p in range(1, parts):
            total = total + shares[p - 1, at].astype(F32)
        if d == 0:
            back[mine] = total.astype(BF)
        else:
            summed[d] = total.astype(BF)
            c = remote(summed.at[d], back.at[mine], r_send.at[d], r_recv.at[d], "sp", at)
            c.start()
            back_copies.append(c)
    nxt = lax.rem(mine + 1, groups)
    prev_copy = remote(states_ref.at[pl.ds(toks - 8, 8)], prev_in, p_send, p_recv, "sp", nxt)
    prev_copy.start()
    advance(1, 0)
    rows = lax.broadcasted_iota(jnp.int32, (toks, toks), 0)
    cols = lax.broadcasted_iota(jnp.int32, (toks, toks), 1)
    eye = jnp.where(rows == cols, 1.0, 0.0).astype(BF)
    total = contract_rows(cot_ref[...], eye)
    for c in back_copies:
        c.wait_recv()
    total = total + contract_rows(back[...].reshape(size, width), picked)
    flipped[here, :] = total.astype(BF)
    grad_copies = []
    for d in range(1, parts):
        part = flipped.at[here]
        c = remote(part, part, g_send.at[d], g_recv.at[d], "tp", lax.rem(col + d, parts))
        c.start()
        grad_copies.append(c)
    for step in range(1, depth - 1):
        advance(1, step)
    collected(0)
    loads[5].wait()
    for c in grad_copies:
        c.wait_recv()
    high = model // groups
    block_copies = []
    for d in range(1, groups):
        peer = lax.rem(mine + d, groups)
        c = remote(flipped.at[near(high, peer)], blocks.at[mine], b_send.at[d], b_recv.at[d], "sp", peer)
        c.start()
        block_copies.append(c)
    grad_mixed = contract_rows(flipped[...], proj_all[...].reshape(model, states_ref.shape[1]))
    states = states_ref[...]
    act, branch_slope = gelu_parts(gate_ref[...].astype(F32))
    decays = jnp.exp(decay_ref[...])
    ggate_ref[...] = (grad_mixed * states * branch_slope).astype(BF)
    local = grad_mixed * act
    line = lax.broadcasted_iota(jnp.int32, local.shape, 0)
    span = jnp.where(line < toks - 1, pltpu.roll(decays, toks - 1, 0), 1.0)
    k = 1
    while k < toks:
        inside = line < toks - k
        local = local + span * jnp.where(inside, pltpu.roll(local, toks - k, 0), 0.0)
        span = span * jnp.where(inside, pltpu.roll(span, toks - k, 0), 1.0)
        k *= 2
    eight = lax.broadcasted_iota(jnp.int32, (8, local.shape[1]), 0)
    whole = span[0:1] * decays[0:1]
    entry = local[0:1] * decays[0:1]
    carry_own[...] = jnp.where(eight == 0, whole, entry)
    carry_copies = []
    for d in range(1, groups):
        peer = lax.rem(mine + d, groups)
        c = remote(carry_own, carry_in.at[d - 1], k_send.at[d], k_recv.at[d], "sp", peer)
        c.start()
        carry_copies.append(c)
    collected(1)
    total = jnp.dot(flipped[near(high, mine), :], mixed_all[mine], preferred_element_type=F32)
    for d in range(1, groups):
        block_copies[d - 1].wait_recv()
        at = lax.rem(mine + groups - d, groups)
        total = total + jnp.dot(blocks[at], mixed_all[at], preferred_element_type=F32)
    outp_ref[...] = total
    prev_copy.wait_recv()
    first = jnp.where(mine > 0, prev_in[7:8, :], 0.0)
    prev = jnp.where(line == 0, first, pltpu.roll(states, 1, 0))
    for c in carry_copies:
        c.wait_recv()
    carried = jnp.zeros_like(whole)
    for ahead in range(groups - 1, 0, -1):
        got = carry_in[groups - ahead - 1]
        carried = jnp.where(mine + ahead < groups, got[1:2] + got[0:1] * carried, carried)
    grad_in = local + span * carried
    gin_ref[...] = grad_in
    gdecay_ref[...] = (grad_in * decays * prev).astype(BF)
    settle(0)
    settle(1)
    for c in [prev_copy] + sends + back_copies + grad_copies + block_copies + carry_copies:
        c.wait_send()


def finish_kernel(
    rx, rc, hid, gpg, gpu, outp, ggate, gdecay, gin,
    gg_out, gu_out, gd_out, outp_out, ggate_out, gdecay_out, gin_out,
    gg, gu, gd, sems, small_sems,
):
    stores = []
    for i, (src, dst) in enumerate((
        (outp, outp_out), (ggate, ggate_out), (gdecay, gdecay_out), (gin, gin_out),
    )):
        o = pltpu.make_async_copy(src, dst, small_sems.at[i])
        o.start()
        stores.append(o)
    step = 256
    steps = rx.shape[1] // step
    for i in range(steps):
        part = slice(i * step, (i + 1) * step)
        for kind, grad, buf, out in ((0, gpg, gg, gg_out), (1, gpu, gu, gu_out)):
            buf[part, :] = contract_rows(rx[:, part], grad[...])
            pltpu.make_async_copy(buf.at[part], out.at[part], sems.at[kind]).start()
        gd[:, part] = contract_rows(hid[...], rc[:, part])
        pltpu.make_async_copy(gd.at[:, part], gd_out.at[:, part], sems.at[2]).start()
    for kind, (buf, out) in enumerate(((gg, gg_out), (gu, gu_out), (gd, gd_out))):
        pltpu.make_async_copy(buf, out, sems.at[kind]).wait()
    for o in stores:
        o.wait()


def finish(rx, rc, hid, gpg, gpu, *small):
    size, model = rx.shape
    units = hid.shape[1]
    vmem = pl.BlockSpec(memory_space=pltpu.VMEM)
    hbm = pl.BlockSpec(memory_space=pltpu.HBM)
    grads = [(model, units), (model, units), (units, model)]
    outs = pl.pallas_call(
        finish_kernel,
        out_shape=[jax.ShapeDtypeStruct(g, F32) for g in grads]
        + [jax.ShapeDtypeStruct(a.shape, a.dtype) for a in small],
        in_specs=[vmem] * (5 + len(small)),
        out_specs=[hbm] * (3 + len(small)),
        scratch_shapes=[pltpu.VMEM(g, F32) for g in grads]
        + [pltpu.SemaphoreType.DMA((3,)), pltpu.SemaphoreType.DMA((len(small),))],
        compiler_params=pltpu.CompilerParams(vmem_limit_bytes=40 * 1024 * 1024),
        name="finish",
    )(rx, rc, hid, gpg, gpu, *small)
    return tuple(out[None] for out in outs[:3]) + tuple(outs[3:])


def shards(
    moe_input, cotangent, routes, route_weights, gate_branch, log_decay, states,
    w_gate, w_up, w_down, out_proj,
):
    groups, parts = lax.axis_size("sp"), lax.axis_size("tp")
    tok_rows, picks = routes.shape
    width = moe_input.shape[1]
    model = width * parts
    units = w_gate.shape[2]
    chans = states.shape[1]
    room = tok_rows * picks * 5 // (4 * groups)
    room = (room + 7) // 8 * 8
    depth = groups // CORES
    high = out_proj.shape[0]
    chunked = groups * parts <= 64
    chunks = groups if chunked else 1
    vmem = pl.BlockSpec(memory_space=pltpu.VMEM)
    hbm = pl.BlockSpec(memory_space=pltpu.HBM)
    dma = pltpu.SemaphoreType.DMA

    def run(*refs):
        whole_kernel(groups, parts, room, chunked, *refs)

    def buf(*shape, kind=BF):
        return pltpu.VMEM(shape, kind)

    outs = pl.pallas_call(
        run,
        out_shape=[
            jax.ShapeDtypeStruct((groups, room, model), BF),
            jax.ShapeDtypeStruct((groups, room, model), BF),
            jax.ShapeDtypeStruct((groups * room, units), BF),
            jax.ShapeDtypeStruct((groups * room, units), BF),
            jax.ShapeDtypeStruct((groups * room, units), BF),
            jax.ShapeDtypeStruct((high, chans), F32),
            jax.ShapeDtypeStruct((tok_rows, chans), BF),
            jax.ShapeDtypeStruct((tok_rows, chans), BF),
            jax.ShapeDtypeStruct((tok_rows, chans), F32),
        ],
        in_specs=[vmem] * 2 + [hbm] * 9,
        out_specs=[vmem] * 9,
        scratch_shapes=[
            buf(tok_rows, width), buf(tok_rows, width), buf(tok_rows, chans),
            buf(tok_rows, chans, kind=F32), buf(tok_rows, chans, kind=F32),
            buf(model, units), buf(model, units), buf(units, model),
            buf(groups, room, width), buf(groups, room, width),
            buf(groups, high, chans), buf(groups, tok_rows, chans), buf(tok_rows, chans),
            buf(parts, groups, room, width), buf(parts - 1, groups, room, width),
            buf(groups, room, width), buf(groups, room, width),
            buf(model, tok_rows), buf(groups, high, tok_rows),
            buf(8, chans, kind=F32), buf(groups - 1, 8, chans, kind=F32), buf(8, chans, kind=F32),
        ]
        + [dma((2, groups))] * 2 + [dma((2, chunks, parts))] * 2 + [dma((2, 2, depth))] * 4
        + [dma((chunks, parts))] * 2 + [dma((groups,))] * 2 + [dma((parts,))] * 2
        + [dma((groups,))] * 4 + [dma(())] * 2 + [dma((9,)), dma((4,))],
        compiler_params=pltpu.CompilerParams(
            collective_id=0, has_side_effects=True, vmem_limit_bytes=40 * 1024 * 1024),
        name="backward",
    )(
        routes.T, route_weights.T,
        *(pltpu.with_memory_space_constraint(a, pltpu.HBM) for a in (
            moe_input, cotangent, gate_branch, states, log_decay, out_proj, w_gate, w_up, w_down)),
    )
    rx, rc = (out.reshape(groups * room, model) for out in outs[:2])
    return finish(rx, rc, *outs[2:])


def flip(index, mask, count):
    total, bit = 0, 1
    while bit < count:
        here = lax.rem(lax.div(index, bit), 2)
        total = total + bit * ((1 - here) if mask & bit else here)
        bit *= 2
    return total


def plane_kernel(
    groups, parts, room,
    routes_any, weights_any, x_any, cot_any, gate_any, states_any, decay_any, proj_any,
    wg_any, wu_any, wd_any,
    rows_x, rows_c, hid_ref, gpg_ref, gpu_ref, outp_ref, ggate_ref, gdecay_ref, gin_ref,
    routes_ref, weights_ref, x_ref, cot_ref, gate_ref, states_ref, decay_ref, wg, wu, wd,
    out_x, out_c, picked_ref, proj_all, mixed_all, act_ref, slope_ref, active_ref, lean_ref,
    terms, shares, passed, summed, back, cot_turned, cot_mine, flipped, blocks, levels, span_ref, past_ref,
    carry_own, carry_in, prev_in,
    o_send, a_recv, t_recv, e_recv, s_recv, m_recv, z_send, z_recv, c_recv, p_send, p_recv, l_sem,
):
    mine, col = lax.axis_index("sp"), lax.axis_index("tp")
    toks, width = x_ref.shape
    model = rows_x.shape[2]
    chans = states_ref.shape[1]
    units = hid_ref.shape[2]
    depth = groups // CORES
    z, core = mine // CORES, lax.rem(mine, CORES)
    size = groups * room
    half = groups // 2
    rows_half = half * room
    inner = jnp.logical_and(z >= 1, z + 1 < depth)

    barrier = pltpu.get_barrier_semaphore()
    for d in range(1, groups):
        pl.semaphore_signal(
            barrier, inc=1, device_id={"sp": lax.rem(mine + d, groups)},
            device_id_type=pl.DeviceIdType.MESH,
        )
    for d in range(1, parts):
        pl.semaphore_signal(
            barrier, inc=1, device_id={"tp": lax.rem(col + d, parts)},
            device_id_type=pl.DeviceIdType.MESH,
        )

    loads = []
    for i, (s, t) in enumerate((
        (x_any, x_ref), (cot_any, cot_ref), (gate_any, gate_ref), (states_any, states_ref),
        (proj_any, proj_all.at[mine]), (decay_any, decay_ref),
        (wg_any.at[0], wg), (wu_any.at[0], wu), (wd_any.at[0], wd),
        (routes_any, routes_ref), (weights_any, weights_ref),
    )):
        loads.append(pltpu.make_async_copy(s, t, l_sem.at[i]))
    for i in (9, 10, 0, 1, 4, 2, 3, 6, 7, 8, 5):
        loads[i].start()

    def near(width_of, index):
        return pl.ds(pl.multiple_of(index * width_of, width_of), width_of)

    def send(src, dst, send_sem, recv_sem, axis, peer):
        c = remote(src, dst, send_sem, recv_sem, axis, peer)
        c.start()
        return c

    def all_sent(ref, sem):
        remote(ref, ref, sem, sem, "tp", tile[1]).wait_send()

    def all_here(ref, sem):
        remote(ref, ref, sem, sem, "tp", tile[1]).wait_recv()

    group = [flip(mine, d, groups) for d in range(groups)]
    tile = [flip(col, p, parts) for p in range(parts)]
    here = near(width, col)

    loads[9].wait()
    loads[10].wait()
    picked, weight = selection(routes_ref[...], weights_ref[...], groups, room)
    picked_ref[...] = picked
    arrivals = [[None] * groups for _ in range(2)]
    gathers = [[None] * groups for _ in range(2)]
    sources = ((out_x, rows_x), (out_c, rows_c))

    def spread(a):
        src, dst = sources[a]
        for d in range(1, groups):
            arrivals[a][d] = send(
                src.at[group[d]], dst.at[mine, :, here], o_send.at[a], a_recv.at[a, d - 1], "sp", group[d])
        dst[mine, :, here] = src[mine]

    def share_out(a, d):
        src, dst = sources[a]
        if d:
            arrivals[a][d].wait_recv()
        own = dst.at[group[d], :, here] if d else src.at[mine]
        gathers[a][d] = [
            send(own, dst.at[group[d], :, here], o_send.at[2 + a],
                 t_recv.at[a, d] if k == d % 2 else e_recv.at[a, d // half], "tp", tile[k + 1])
            for k in range(2)
        ]

    def relay(a, d):
        dst = sources[a][1]
        k = d % 2
        gathers[a][d][k].wait_recv()
        ref = dst.at[group[d], :, near(width, tile[k + 1])]
        send(ref, ref, o_send.at[2 + a], e_recv.at[a, d // half], "tp", tile[2 - k])

    def landed(a, h):
        all_here(sources[a][1].at[pl.ds(0, groups // parts)], e_recv.at[a, h])

    loads[0].wait()
    got = jnp.dot(picked, x_ref[...], preferred_element_type=F32).astype(BF)
    for e in range(groups):
        out_x[e] = got[e * room : (e + 1) * room]
    pl.semaphore_wait(barrier, groups + parts - 2)
    spread(0)
    share_out(0, 0)
    loads[1].wait()
    got = jnp.dot(picked, cot_ref[...], preferred_element_type=F32)
    got = (got * weight).astype(BF)
    for e in range(groups):
        out_c[e] = got[e * room : (e + 1) * room]
    spread(1)

    low = proj_all.shape[1] // 2
    pairs = (proj_all.at[:, pl.ds(0, low)], proj_all.at[:, pl.ds(low, low)], mixed_all)
    last = len(pairs) - 1
    hop_send = (4, 13, 5)

    def chain(a, step, wait=False, middle=None):
        buf = pairs[a]
        right = buf.at[jnp.maximum(z - step, 0) * CORES + core]
        left = buf.at[jnp.minimum(z + step, depth - 1) * CORES + core]
        up = jnp.minimum(z + 1, depth - 1) * CORES + core
        down = jnp.maximum(z - 1, 0) * CORES + core
        for way, ref, peer, ok, within in (
            (0, right, up, jnp.logical_and(z - step >= 0, z + 1 < depth),
             jnp.logical_and(z >= 1, z + 2 < depth)),
            (1, left, down, jnp.logical_and(z + step < depth, z >= 1),
             jnp.logical_and(z >= 2, z + 1 < depth)),
        ):
            if middle is not None:
                ok = jnp.logical_and(ok, within if middle else jnp.logical_not(within))

            @pl.when(ok)
            def _(way=way, ref=ref, peer=peer):
                c = remote(ref, ref, z_send.at[a, way, step], z_recv.at[a, way, step], "sp", peer)
                c.wait_send() if wait else c.start()

    partner = z * CORES + (1 - core)

    def across(a, step, way, start=True, also=None):
        ok = z - step >= 0 if way == 0 else z + step < depth
        if also is not None:
            ok = jnp.logical_and(ok, also)
        zz = jnp.maximum(z - step, 0) if way == 0 else jnp.minimum(z + step, depth - 1)
        ref = pairs[a].at[zz * CORES + (core if start else 1 - core)]
        sem = c_recv.at[last + way * depth + step if a == last else a]

        @pl.when(ok)
        def _():
            c = remote(ref, ref, o_send.at[hop_send[a]], sem, "sp", partner)
            c.start() if start else c.wait_recv()

    def advance(a, step, also=None):
        buf = pairs[a]
        from_l = buf.at[jnp.maximum(z - 1 - step, 0) * CORES + core]
        from_r = buf.at[jnp.minimum(z + 1 + step, depth - 1) * CORES + core]
        for way, ok, ref in ((0, z - 1 - step >= 0, from_l), (1, z + 1 + step < depth, from_r)):
            @pl.when(ok if also is None else jnp.logical_and(ok, also))
            def _(way=way, ref=ref):
                remote(ref, ref, z_send.at[a, way, step], z_recv.at[a, way, step],
                       "sp", lax.rem(mine + 1, groups)).wait_recv()
                if step + 1 < depth - 1:
                    forward_to = (z + 1 < depth) if way == 0 else (z >= 1)
                    peer = jnp.minimum(z + 1, depth - 1) if way == 0 else jnp.maximum(z - 1, 0)

                    @pl.when(forward_to)
                    def _():
                        remote(ref, ref, z_send.at[a, way, step + 1], z_recv.at[a, way, step + 1],
                               "sp", peer * CORES + core).start()
        across(a, step + 1, 0, also=also)
        across(a, step + 1, 1, also=also)

    def settle(a):
        for step in range(depth - 1):
            chain(a, step, True)
        all_sent(pairs[a].at[pl.ds(0, depth)], o_send.at[hop_send[a]])

    def collected(step):
        for way in range(2):
            if step or not way:
                across(last, step, way, start=False)

    loads[4].wait()
    for a in range(last):
        chain(a, 0)
        across(a, 0, 0)
    share_out(1, 0)
    share_out(0, 1)
    loads[3].wait()
    prev_copy = send(
        states_ref.at[pl.ds(toks - 8, 8)], prev_in, p_send, p_recv, "sp", lax.rem(mine + 1, groups))

    loads[2].wait()
    act, branch_slope = gelu_parts(gate_ref[...].astype(F32))
    states = states_ref[...]
    act_ref[...] = act
    slope_ref[...] = branch_slope * states
    mixed_all[mine] = (act * states).astype(BF)
    chain(last, 0, middle=False)
    across(last, 0, 0)
    rows = lax.broadcasted_iota(jnp.int32, (toks, toks), 0)
    cols = lax.broadcasted_iota(jnp.int32, (toks, toks), 1)
    eye = jnp.where(rows == cols, 1.0, 0.0).astype(BF)
    fine = cot_turned.shape[2]
    cot_turned[...] = contract_rows(cot_ref[...], eye).astype(BF).reshape(cot_turned.shape)
    cot_mine[col] = cot_turned[:, col]
    share_out(1, 1)
    for p in range(1, parts):
        send(cot_turned.at[:, tile[p]], cot_mine.at[col], o_send.at[6], m_recv.at[0], "tp", tile[p])
    share_out(0, 2)
    share_out(0, 3)
    for a in range(2):
        relay(a, 0)
        relay(a, 1)
    queue = [(0, d) for d in range(2, groups)] + [(1, d) for d in range(2, groups)]
    ahead = queue[2:]

    def pump(count):
        for _ in range(count):
            for _ in range(2):
                if ahead:
                    share_out(*ahead.pop(0))
            for _ in range(2):
                if queue:
                    relay(*queue.pop(0))

    pump(half)

    first = [lax.div(mine, half) * half, (1 - lax.div(mine, half)) * half]

    def forward(h):
        landed(0, h)
        at = pl.ds(first[h], half)
        data = rows_x[at].reshape(rows_half, model)
        pre_gate = jnp.dot(data, wg[...].reshape(model, units), preferred_element_type=F32)
        pre_up = jnp.dot(data, wu[...].reshape(model, units), preferred_element_type=F32)
        active, slope = silu_parts(pre_gate)
        hid_ref[at] = (active * pre_up).astype(BF).reshape(half, room, units)
        active_ref[h] = active
        lean_ref[h] = pre_up * slope

    def hidden_grads(h):
        landed(1, h)
        at = pl.ds(first[h], half)
        grad_hidden = contract_cols(rows_c[at].reshape(rows_half, model), wd[...])
        gpg_ref[at] = (grad_hidden * lean_ref[h]).astype(BF).reshape(half, room, units)
        gpu_ref[at] = (grad_hidden * active_ref[h]).astype(BF).reshape(half, room, units)

    share_copies = [[None, None] for _ in range(groups)]

    def reduce_out(d, i, p):
        g = group[d]
        share_copies[d][i] = send(
            terms.at[p, g], shares.at[i, g], o_send.at[7], s_recv.at[d, i], "tp", tile[1 + d % 2])

    def input_grads(h, order):
        at = pl.ds(first[h], half)
        gate_part = gpg_ref[at].reshape(rows_half, units)
        up_part = gpu_ref[at].reshape(rows_half, units)
        for p in (3, 1, 2, 0):
            term = contract_cols(gate_part, wg[:, tile[p]].reshape(width, units))
            term = term + contract_cols(up_part, wu[:, tile[p]].reshape(width, units))
            terms[p, at] = term.astype(BF).reshape(half, room, width)
            for d in order:
                if p == 3:
                    reduce_out(d, 0, p)
                elif p == 1 + d % 2:
                    reduce_out(d, 1, p)

    def pass_on(d):
        g, far_tile = group[d], 2 - d % 2
        share_copies[d][0].wait_recv()
        passed[g] = (terms[far_tile, g].astype(F32) + shares[0, g].astype(F32)).astype(BF)
        send(passed.at[g], shares.at[2, g], o_send.at[7], s_recv.at[d, 1], "tp", tile[far_tile])

    def bring_back(d):
        g = group[d]
        all_here(shares.at[pl.ds(1, 2), g], s_recv.at[d, 1])
        total = terms[0, g].astype(F32) + shares[1, g].astype(F32) + shares[2, g].astype(F32)
        if d == 0:
            back[mine] = total.astype(BF)
        else:
            summed[d] = total.astype(BF)
            send(summed.at[d], back.at[mine], o_send.at[8], m_recv.at[1], "sp", g)

    for i in (6, 7, 8):
        loads[i].wait()
    forward(0)
    pump(1)
    for a in range(last):
        advance(a, 0)
    chain(last, 0, middle=True)
    forward(1)

    hidden_grads(0)
    pump(1)
    order = list(range(2, half)) + [1, 0] + list(range(half, groups))
    input_grads(0, order[:half])
    hidden_grads(1)
    for d in order[:2]:
        pass_on(d)
    input_grads(1, order[half:])
    for d in order[2:half]:
        pass_on(d)

    loads[5].wait()
    prev_copy.wait_recv()
    decays = jnp.exp(decay_ref[...])
    line = lax.broadcasted_iota(jnp.int32, decays.shape, 0)
    before = jnp.where(mine > 0, prev_in[7:8, :], 0.0)
    past_ref[...] = decays * jnp.where(line == 0, before, pltpu.roll(states_ref[...], 1, 0))
    span = jnp.where(line < toks - 1, pltpu.roll(decays, toks - 1, 0), 1.0)
    k, level = 1, 0
    while k < toks:
        inside = line < toks - k
        levels[level] = jnp.where(inside, span, 0.0)
        span = span * jnp.where(inside, pltpu.roll(span, toks - k, 0), 1.0)
        k *= 2
        level += 1
    span_ref[...] = span
    head = decays[0:1]

    for step in range(1, depth - 2):
        advance(0, step)
    late = order[half:]
    for d in order:
        if late:
            pass_on(late.pop(0))
        bring_back(d)
    all_here(cot_turned.at[:, pl.ds(0, parts - 1)], m_recv.at[0])
    total = cot_mine[...].reshape(width, toks).astype(F32)
    all_here(back.at[pl.ds(0, groups - 1)], m_recv.at[1])
    total = total + contract_rows(back[...].reshape(size, width), picked_ref[...])
    flipped[:, col] = total.astype(BF).reshape(groups, fine, toks)

    def plane_part(buf, owner, rows, first_sem, to, relayed=0):
        part = buf.at[pl.ds(rows * half, half), owner]
        return send(
            part, part, o_send.at[first_sem // 3 + 8], m_recv.at[first_sem + relayed], "tp", tile[to])

    def plane_start(buf, first_sem):
        copies = [plane_part(buf, col, p - 1, first_sem, p, p) for p in (1, 2)]
        for p in (1, 2):
            plane_part(buf, col, 2 - p, first_sem, p)
        return copies

    def plane_relay(buf, copies, first_sem):
        for p in (1, 2):
            copies[p - 1].wait_recv()
            plane_part(buf, tile[p], p - 1, first_sem, 3 - p)

    grad_copies = plane_start(flipped, 3)
    for d in range(1, groups):
        send(flipped.at[group[d], col], blocks.at[mine, col], o_send.at[11], m_recv.at[2], "sp", group[d])
    blocks[mine, col] = flipped[mine, col]
    for step in range(1, depth - 2):
        advance(1, step)
    advance(last, 0)
    plane_relay(flipped, grad_copies, 3)
    all_here(blocks.at[pl.ds(0, groups - 1), 0], m_recv.at[2])
    plane_copies = plane_start(blocks, 6)
    advance(0, depth - 2)
    for step in range(1, depth - 2):
        advance(last, step, inner)
    all_here(flipped.at[:, pl.ds(0, 2)], m_recv.at[3])
    advance(1, depth - 2)
    for a in range(last):
        all_here(pairs[a].at[pl.ds(0, depth)], c_recv.at[a])
    grad_mixed = contract_rows(flipped[...].reshape(model, toks), proj_all[...].reshape(model, chans))
    ggate_ref[...] = (grad_mixed * slope_ref[...]).astype(BF)
    local = grad_mixed * act_ref[...]
    k, level = 1, 0
    while k < toks:
        local = local + levels[level] * pltpu.roll(local, toks - k, 0)
        k *= 2
        level += 1
    carry_own[0:1] = span_ref[0:1, :] * head
    carry_own[1:2] = local[0:1] * head
    for d in range(1, groups):
        send(carry_own, carry_in.at[d - 1], o_send.at[12], m_recv.at[9], "sp", lax.rem(mine + d, groups))
    plane_relay(blocks, plane_copies, 6)
    for step in range(1, depth - 2):
        advance(last, step, jnp.logical_not(inner))
    for step in range(depth - 1):
        collected(step)
    all_here(blocks.at[:, pl.ds(0, 2)], m_recv.at[6])
    advance(last, depth - 2)
    high = blocks.shape[1] * blocks.shape[2]

    def out_part(t):
        return jnp.dot(blocks[t].reshape(high, toks), mixed_all[t], preferred_element_type=F32)

    near_part = out_part(group[0])
    for d in range(1, groups - CORES):
        near_part = near_part + out_part(group[d])
    outp_ref[...] = near_part
    all_here(carry_in, m_recv.at[9])
    carried = jnp.zeros((1, chans), F32)
    for ahead in range(groups - 1, 0, -1):
        got = carry_in[groups - ahead - 1]
        carried = jnp.where(mine + ahead < groups, got[1:2] + got[0:1] * carried, carried)
    grad_in = local + span_ref[...] * carried
    gin_ref[...] = grad_in
    gdecay_ref[...] = (grad_in * past_ref[...]).astype(BF)
    collected(depth - 1)
    far_part = out_part(group[groups - CORES])
    for d in range(groups - CORES + 1, groups):
        far_part = far_part + out_part(group[d])
    outp_ref[...] += far_part
    for a in range(last + 1):
        settle(a)
    for a in range(2):
        all_sent(rows_x.at[pl.ds(0, groups - 1), :, pl.ds(0, width)], o_send.at[a])
        all_sent(rows_x.at[pl.ds(0, groups * 3 // parts)], o_send.at[2 + a])
    all_sent(cot_turned.at[:, pl.ds(0, parts - 1)], o_send.at[6])
    all_sent(rows_x.at[pl.ds(0, groups * 3 // parts)], o_send.at[7])
    all_sent(back.at[pl.ds(0, groups - 1)], o_send.at[8])
    for i in (9, 10):
        all_sent(flipped.at[:, pl.ds(0, 3)], o_send.at[i])
    all_sent(blocks.at[pl.ds(0, groups - 1), 0], o_send.at[11])
    all_sent(carry_in, o_send.at[12])
    prev_copy.wait_send()


def plane_shards(
    moe_input, cotangent, routes, route_weights, gate_branch, log_decay, states,
    w_gate, w_up, w_down, out_proj,
):
    groups, parts = lax.axis_size("sp"), lax.axis_size("tp")
    tok_rows, picks = routes.shape
    width = moe_input.shape[1]
    model = width * parts
    units = w_gate.shape[2]
    chans = states.shape[1]
    room = tok_rows * picks * 5 // (4 * groups)
    room = (room + 7) // 8 * 8
    depth = groups // CORES
    high = out_proj.shape[0]
    fine = high // parts
    doublings = (tok_rows - 1).bit_length()
    vmem = pl.BlockSpec(memory_space=pltpu.VMEM)
    hbm = pl.BlockSpec(memory_space=pltpu.HBM)
    dma = pltpu.SemaphoreType.DMA

    def run(*refs):
        plane_kernel(groups, parts, room, *refs)

    def buf(*shape, kind=BF):
        return pltpu.VMEM(shape, kind)

    def split(weight):
        return weight.reshape(1, groups, parts, fine, units)

    outs = pl.pallas_call(
        run,
        out_shape=[
            jax.ShapeDtypeStruct((groups, room, model), BF),
            jax.ShapeDtypeStruct((groups, room, model), BF),
            jax.ShapeDtypeStruct((groups, room, units), BF),
            jax.ShapeDtypeStruct((groups, room, units), BF),
            jax.ShapeDtypeStruct((groups, room, units), BF),
            jax.ShapeDtypeStruct((high, chans), F32),
            jax.ShapeDtypeStruct((tok_rows, chans), BF),
            jax.ShapeDtypeStruct((tok_rows, chans), BF),
            jax.ShapeDtypeStruct((tok_rows, chans), F32),
        ],
        in_specs=[hbm] * 11,
        out_specs=[vmem] * 9,
        scratch_shapes=[
            buf(picks, tok_rows, kind=jnp.int32), buf(picks, tok_rows, kind=F32),
            buf(tok_rows, width), buf(tok_rows, width), buf(tok_rows, chans),
            buf(tok_rows, chans, kind=F32), buf(tok_rows, chans, kind=F32),
            buf(groups, parts, fine, units), buf(groups, parts, fine, units), buf(units, model),
            buf(groups, room, width), buf(groups, room, width), buf(groups * room, tok_rows),
            buf(groups, high, chans), buf(groups, tok_rows, chans),
            buf(tok_rows, chans, kind=F32), buf(tok_rows, chans, kind=F32),
            buf(2, groups // 2 * room, units, kind=F32), buf(2, groups // 2 * room, units, kind=F32),
            buf(parts, groups, room, width), buf(parts - 1, groups, room, width),
            buf(groups, room, width), buf(groups, room, width), buf(groups, room, width),
            buf(groups // parts, parts, fine, tok_rows), buf(parts, groups // parts, fine, tok_rows),
            buf(groups, parts, fine, tok_rows), buf(groups, parts, fine, tok_rows),
            buf(doublings, tok_rows, chans, kind=F32), buf(tok_rows, chans, kind=F32),
            buf(tok_rows, chans, kind=F32),
            buf(2, chans, kind=F32), buf(groups - 1, 2, chans, kind=F32), buf(8, chans, kind=F32),
        ]
        + [dma((14,)), dma((2, groups - 1)), dma((2, groups)), dma((2, 2)), dma((groups, 2))]
        + [dma((10,)), dma((3, 2, depth - 1)), dma((3, 2, depth - 1)), dma((2 + 2 * depth,))]
        + [dma(()), dma(()), dma((11,))],
        compiler_params=pltpu.CompilerParams(
            collective_id=0, has_side_effects=True, vmem_limit_bytes=40 * 1024 * 1024),
        name="backward",
    )(
        *(pltpu.with_memory_space_constraint(a, pltpu.HBM) for a in (
            routes.T, route_weights.T, moe_input, cotangent, gate_branch, states, log_decay, out_proj,
            split(w_gate), split(w_up), w_down)),
    )
    rx, rc = (out.reshape(groups * room, model) for out in outs[:2])
    grads = (out.reshape(groups * room, units) for out in outs[2:5])
    return finish(rx, rc, *grads, *outs[5:])


def solution(mesh):
    groups, parts = mesh.shape["sp"], mesh.shape["tp"]
    plane = parts == 4 and groups % parts == 0 and groups & (groups - 1) == 0
    return jax.shard_map(
        plane_shards if plane else shards,
        mesh=mesh,
        in_specs=(
            P("sp", "tp"), P("sp", "tp"), P("sp", None), P("sp", None), P("sp", "tp"),
            P("sp", "tp"), P("sp", "tp"), P("sp", None, "tp"), P("sp", None, "tp"),
            P("sp", "tp", None), P("sp", "tp"),
        ),
        out_specs=(
            P("sp", None, "tp"), P("sp", None, "tp"), P("sp", "tp", None), P("sp", "tp"),
            P("sp", "tp"), P("sp", "tp"), P("sp", "tp"),
        ),
        check_vma=False,
    )
```

```python
import jax
import jax.numpy as jnp
from jax import lax
from jax.experimental import pallas as pl
from jax.experimental.pallas import tpu as pltpu
from jax.sharding import PartitionSpec as P

BF = jnp.bfloat16
F32 = jnp.float32
CORES = 2
GELU_C = 0.7978845608028654
GELU_A = 0.044715


def silu_parts(pre_gate):
    sigmoid_val = jax.nn.sigmoid(pre_gate)
    return (pre_gate * sigmoid_val, sigmoid_val * (1.0 + pre_gate * (1.0 - sigmoid_val)))


def contract_rows(left_mat, right_mat):
    return lax.dot_general(
        left_mat, right_mat, (((0,), (0,)), ((), ())), preferred_element_type=F32
    )


def contract_cols(left_mat, right_mat):
    return lax.dot_general(
        left_mat, right_mat, (((1,), (1,)), ((), ())), preferred_element_type=F32
    )


def gelu_parts(x):
    t = jnp.tanh(GELU_C * (x + GELU_A * (x * x * x)))
    half = 0.5 * (1.0 + t)
    slope = half + 0.5 * x * (1.0 - t * t) * (GELU_C * (1.0 + 3.0 * GELU_A * x * x))
    return x * half, slope


def selection(routes_t, weights_t, groups, room):
    picks, toks = routes_t.shape
    experts = lax.broadcasted_iota(jnp.int32, (groups, toks), 0)
    named = jnp.zeros((groups, toks), F32)
    weight = jnp.zeros((groups, toks), F32)
    for k in range(picks):
        hit = routes_t[k : k + 1, :] == experts
        named = named + jnp.where(hit, 1.0, 0.0)
        weight = weight + jnp.where(hit, weights_t[k : k + 1, :], 0.0)
    rows = lax.broadcasted_iota(jnp.int32, (toks, toks), 0)
    cols = lax.broadcasted_iota(jnp.int32, (toks, toks), 1)
    before = jnp.where(rows < cols, 1.0, 0.0).astype(BF)
    slot = jnp.dot(named.astype(BF), before, preferred_element_type=F32)
    slot = jnp.where(named > 0.5, slot, -1.0)
    place = lax.broadcasted_iota(jnp.int32, (room, toks), 0).astype(F32)
    picked, column = [], []
    for e in range(groups):
        one = jnp.where(slot[e : e + 1, :] == place, 1.0, 0.0)
        picked.append(one)
        column.append(jnp.sum(one * weight[e : e + 1, :], axis=1, keepdims=True))
    return jnp.concatenate(picked, axis=0).astype(BF), jnp.concatenate(column, axis=0)


def greet(groups, parts, mine, col):
    barrier = pltpu.get_barrier_semaphore()
    for d in range(1, groups):
        pl.semaphore_signal(
            barrier, inc=1, device_id={"sp": lax.rem(mine + d, groups)},
            device_id_type=pl.DeviceIdType.MESH,
        )
    for d in range(1, parts):
        pl.semaphore_signal(
            barrier, inc=1, device_id={"tp": lax.rem(col + d, parts)},
            device_id_type=pl.DeviceIdType.MESH,
        )
    pl.semaphore_wait(barrier, groups + parts - 2)


def remote(src, dst, send, recv, axis, peer):
    return pltpu.make_async_remote_copy(
        src_ref=src, dst_ref=dst, send_sem=send, recv_sem=recv,
        device_id={axis: peer}, device_id_type=pl.DeviceIdType.MESH,
    )


def whole_kernel(
    groups, parts, room, chunked,
    routes_ref, weights_ref, x_any, cot_any, gate_any, states_any, decay_any, proj_any,
    wg_any, wu_any, wd_any,
    rows_x, rows_c, hid_ref, gpg_ref, gpu_ref, outp_ref, ggate_ref, gdecay_ref, gin_ref,
    x_ref, cot_ref, gate_ref, states_ref, decay_ref, wg, wu, wd,
    out_x, out_c, proj_all, mixed_all, mix_own,
    terms, shares, summed, back, flipped, blocks, carry_own, carry_in, prev_in,
    a_send, a_recv, t_send, t_recv, z_send, z_recv, c_send, c_recv,
    s_send, s_recv, r_send, r_recv, g_send, g_recv, b_send, b_recv, k_send, k_recv, p_send, p_recv,
    l_sem, w_sem,
):
    mine, col = lax.axis_index("sp"), lax.axis_index("tp")
    toks, width = x_ref.shape
    model = rows_x.shape[2]
    depth = groups // CORES
    z, core = mine // CORES, lax.rem(mine, CORES)
    size = groups * room

    def near(width_of, index):
        return pl.ds(pl.multiple_of(index * width_of, width_of), width_of)

    loads = []
    for i, (s, t) in enumerate((
        (x_any, x_ref), (cot_any, cot_ref), (gate_any, gate_ref), (states_any, states_ref),
        (proj_any, proj_all.at[mine]), (decay_any, decay_ref),
        (wg_any.at[0], wg), (wu_any.at[0], wu), (wd_any.at[0], wd),
    )):
        o = pltpu.make_async_copy(s, t, l_sem.at[i])
        o.start()
        loads.append(o)

    picked, weight = selection(routes_ref[...], weights_ref[...], groups, room)
    loads[0].wait()
    got = jnp.dot(picked, x_ref[...], preferred_element_type=F32).astype(BF)
    for e in range(groups):
        out_x[e] = got[e * room : (e + 1) * room]
    loads[1].wait()
    got_c = jnp.dot(picked, cot_ref[...], preferred_element_type=F32)
    got_c = (got_c * weight).astype(BF)
    for e in range(groups):
        out_c[e] = got_c[e * room : (e + 1) * room]
    greet(groups, parts, mine, col)

    here = near(width, col)
    sends, own = [], []
    arrivals = [[None] * groups for _ in range(2)]
    for a, (src, dst) in enumerate(((out_x, rows_x), (out_c, rows_c))):
        for d in range(1, groups):
            peer = lax.rem(mine + d, groups)
            c = remote(src.at[peer], dst.at[mine, :, here], a_send.at[a, d], a_recv.at[a, d], "sp", peer)
            c.start()
            arrivals[a][d] = c
            sends.append(c)
        o = pltpu.make_async_copy(src.at[mine], dst.at[mine, :, here], w_sem.at[a])
        o.start()
        own.append(o)

    pairs = (proj_all, mixed_all)

    def chain(a, step, wait=False):
        buf = pairs[a]
        right = buf.at[jnp.maximum(z - step, 0) * CORES + core]
        left = buf.at[jnp.minimum(z + step, depth - 1) * CORES + core]
        up = jnp.minimum(z + 1, depth - 1) * CORES + core
        down = jnp.maximum(z - 1, 0) * CORES + core
        for way, ref, peer, ok in (
            (0, right, up, jnp.logical_and(z - step >= 0, z + 1 < depth)),
            (1, left, down, jnp.logical_and(z + step < depth, z >= 1)),
        ):
            @pl.when(ok)
            def _(way=way, ref=ref, peer=peer):
                c = remote(ref, ref, z_send.at[a, way, step], z_recv.at[a, way, step], "sp", peer)
                c.wait_send() if wait else c.start()

    partner = z * CORES + (1 - core)

    def across(a, step, way, mode):
        ok = z - step >= 0 if way == 0 else z + step < depth
        zz = jnp.maximum(z - step, 0) if way == 0 else jnp.minimum(z + step, depth - 1)
        ref = pairs[a].at[zz * CORES + (1 - core if mode == "recv" else core)]

        @pl.when(ok)
        def _():
            c = remote(ref, ref, c_send.at[a, way, step], c_recv.at[a, way, step], "sp", partner)
            if mode == "start":
                c.start()
            elif mode == "send":
                c.wait_send()
            else:
                c.wait_recv()

    def advance(a, step):
        buf = pairs[a]
        from_l = buf.at[jnp.maximum(z - 1 - step, 0) * CORES + core]
        from_r = buf.at[jnp.minimum(z + 1 + step, depth - 1) * CORES + core]
        for way, ok, ref in ((0, z - 1 - step >= 0, from_l), (1, z + 1 + step < depth, from_r)):
            @pl.when(ok)
            def _(way=way, ref=ref):
                remote(ref, ref, z_send.at[a, way, step], z_recv.at[a, way, step],
                       "sp", lax.rem(mine + 1, groups)).wait_recv()
        if step + 1 < depth - 1:
            chain(a, step + 1)
        across(a, step + 1, 0, "start")
        across(a, step + 1, 1, "start")

    def settle(a):
        for step in range(depth - 1):
            chain(a, step, True)
        for step in range(depth):
            for way in range(2):
                if step or not way:
                    across(a, step, way, "send")

    def collected(a):
        for step in range(depth):
            for way in range(2):
                if step or not way:
                    across(a, step, way, "recv")

    loads[4].wait()
    chain(0, 0)
    across(0, 0, 0, "start")

    gathers = [[], []]

    def gather(a, src, dst):
        if chunked:
            for d in range(groups):
                at = lax.rem(mine + groups - d, groups)
                if d:
                    arrivals[a][d].wait_recv()
                for p in range(1, parts):
                    c = remote(dst.at[at, :, here] if d else src.at[mine], dst.at[at, :, here],
                               t_send.at[a, d, p], t_recv.at[a, d, p], "tp", lax.rem(col + p, parts))
                    c.start()
                    gathers[a].append(c)
            own[a].wait()
        else:
            own[a].wait()
            for d in range(1, groups):
                arrivals[a][d].wait_recv()
            for p in range(1, parts):
                c = remote(dst.at[:, :, here], dst.at[:, :, here],
                           t_send.at[a, 0, p], t_recv.at[a, 0, p], "tp", lax.rem(col + p, parts))
                c.start()
                gathers[a].append(c)
        sends.extend(gathers[a])

    gather(0, out_x, rows_x)
    loads[2].wait()
    loads[3].wait()
    act, branch_slope = gelu_parts(gate_ref[...].astype(F32))
    mix_own[...] = (act * states_ref[...]).astype(BF)
    gather(1, out_c, rows_c)
    o = pltpu.make_async_copy(mix_own, mixed_all.at[mine], w_sem.at[3])
    o.start()
    o.wait()
    for i in range(6, 9):
        loads[i].wait()
    for c in gathers[0]:
        c.wait_recv()
    row_data = rows_x[...].reshape(size, model)
    pre_gate = jnp.dot(row_data, wg[...], preferred_element_type=F32)
    pre_up = jnp.dot(row_data, wu[...], preferred_element_type=F32)
    active, slope = silu_parts(pre_gate)
    hidden = (active * pre_up).astype(BF)
    hid_ref[...] = hidden
    lean = pre_up * slope
    advance(0, 0)
    if depth > 2:
        advance(0, 1)
    for c in gathers[1]:
        c.wait_recv()
    grad_hidden = contract_cols(rows_c[...].reshape(size, model), wd[...])
    grad_pre_gate = (grad_hidden * lean).astype(BF)
    grad_pre_up = (grad_hidden * active).astype(BF)
    gpg_ref[...] = grad_pre_gate
    gpu_ref[...] = grad_pre_up
    for d in list(range(1, parts)) + [0]:
        part = near(width, lax.rem(col + d, parts))
        term = contract_cols(grad_pre_gate, wg[part, :]) + contract_cols(grad_pre_up, wu[part, :])
        terms[d] = term.astype(BF).reshape(groups, room, width)

    share_copies = {}
    order = list(range(1, groups)) + [0]
    for d in order if chunked else [0]:
        at = lax.rem(mine + d, groups)
        for p in range(1, parts):
            src = terms.at[p, at] if chunked else terms.at[p]
            dst = shares.at[p - 1, at] if chunked else shares.at[p - 1]
            c = remote(src, dst, s_send.at[d, p], s_recv.at[d, p], "tp", lax.rem(col + p, parts))
            c.start()
            share_copies[d, p] = c
            sends.append(c)
    for step in range(2, depth - 1):
        advance(0, step)
    chain(1, 0)
    across(1, 0, 0, "start")

    back_copies = []
    for d in order:
        at = lax.rem(mine + d, groups)
        if chunked or d == 1:
            for p in range(1, parts):
                share_copies[d if chunked else 0, p].wait_recv()
        total = terms[0, at].astype(F32)
        for p in range(1, parts):
            total = total + shares[p - 1, at].astype(F32)
        if d == 0:
            back[mine] = total.astype(BF)
        else:
            summed[d] = total.astype(BF)
            c = remote(summed.at[d], back.at[mine], r_send.at[d], r_recv.at[d], "sp", at)
            c.start()
            back_copies.append(c)
    nxt = lax.rem(mine + 1, groups)
    prev_copy = remote(states_ref.at[pl.ds(toks - 8, 8)], prev_in, p_send, p_recv, "sp", nxt)
    prev_copy.start()
    advance(1, 0)
    rows = lax.broadcasted_iota(jnp.int32, (toks, toks), 0)
    cols = lax.broadcasted_iota(jnp.int32, (toks, toks), 1)
    eye = jnp.where(rows == cols, 1.0, 0.0).astype(BF)
    total = contract_rows(cot_ref[...], eye)
    for c in back_copies:
        c.wait_recv()
    total = total + contract_rows(back[...].reshape(size, width), picked)
    flipped[here, :] = total.astype(BF)
    grad_copies = []
    for d in range(1, parts):
        part = flipped.at[here]
        c = remote(part, part, g_send.at[d], g_recv.at[d], "tp", lax.rem(col + d, parts))
        c.start()
        grad_copies.append(c)
    for step in range(1, depth - 1):
        advance(1, step)
    collected(0)
    loads[5].wait()
    for c in grad_copies:
        c.wait_recv()
    high = model // groups
    block_copies = []
    for d in range(1, groups):
        peer = lax.rem(mine + d, groups)
        c = remote(flipped.at[near(high, peer)], blocks.at[mine], b_send.at[d], b_recv.at[d], "sp", peer)
        c.start()
        block_copies.append(c)
    grad_mixed = contract_rows(flipped[...], proj_all[...].reshape(model, states_ref.shape[1]))
    states = states_ref[...]
    act, branch_slope = gelu_parts(gate_ref[...].astype(F32))
    decays = jnp.exp(decay_ref[...])
    ggate_ref[...] = (grad_mixed * states * branch_slope).astype(BF)
    local = grad_mixed * act
    line = lax.broadcasted_iota(jnp.int32, local.shape, 0)
    span = jnp.where(line < toks - 1, pltpu.roll(decays, toks - 1, 0), 1.0)
    k = 1
    while k < toks:
        inside = line < toks - k
        local = local + span * jnp.where(inside, pltpu.roll(local, toks - k, 0), 0.0)
        span = span * jnp.where(inside, pltpu.roll(span, toks - k, 0), 1.0)
        k *= 2
    eight = lax.broadcasted_iota(jnp.int32, (8, local.shape[1]), 0)
    whole = span[0:1] * decays[0:1]
    entry = local[0:1] * decays[0:1]
    carry_own[...] = jnp.where(eight == 0, whole, entry)
    carry_copies = []
    for d in range(1, groups):
        peer = lax.rem(mine + d, groups)
        c = remote(carry_own, carry_in.at[d - 1], k_send.at[d], k_recv.at[d], "sp", peer)
        c.start()
        carry_copies.append(c)
    collected(1)
    total = jnp.dot(flipped[near(high, mine), :], mixed_all[mine], preferred_element_type=F32)
    for d in range(1, groups):
        block_copies[d - 1].wait_recv()
        at = lax.rem(mine + groups - d, groups)
        total = total + jnp.dot(blocks[at], mixed_all[at], preferred_element_type=F32)
    outp_ref[...] = total
    prev_copy.wait_recv()
    first = jnp.where(mine > 0, prev_in[7:8, :], 0.0)
    prev = jnp.where(line == 0, first, pltpu.roll(states, 1, 0))
    for c in carry_copies:
        c.wait_recv()
    carried = jnp.zeros_like(whole)
    for ahead in range(groups - 1, 0, -1):
        got = carry_in[groups - ahead - 1]
        carried = jnp.where(mine + ahead < groups, got[1:2] + got[0:1] * carried, carried)
    grad_in = local + span * carried
    gin_ref[...] = grad_in
    gdecay_ref[...] = (grad_in * decays * prev).astype(BF)
    settle(0)
    settle(1)
    for c in [prev_copy] + sends + back_copies + grad_copies + block_copies + carry_copies:
        c.wait_send()


def finish_kernel(
    rx, rc, hid, gpg, gpu, outp, ggate, gdecay, gin,
    gg_out, gu_out, gd_out, outp_out, ggate_out, gdecay_out, gin_out,
    gg, gu, gd, sems, small_sems,
):
    stores = []
    for i, (src, dst) in enumerate((
        (outp, outp_out), (ggate, ggate_out), (gdecay, gdecay_out), (gin, gin_out),
    )):
        o = pltpu.make_async_copy(src, dst, small_sems.at[i])
        o.start()
        stores.append(o)
    step = 256
    steps = rx.shape[1] // step
    units = hid.shape[1]
    down = units // 4
    for i in range(steps):
        part = slice(i * step, (i + 1) * step)
        for kind, grad, buf, out in ((0, gpg, gg, gg_out), (1, gpu, gu, gu_out)):
            buf[part, :] = contract_rows(rx[:, part], grad[...])
            pltpu.make_async_copy(buf.at[part], out.at[part], sems.at[kind]).start()
        if i % (steps // 4) == 0:
            rows = slice(i * 4 // steps * down, (i * 4 // steps + 1) * down)
            gd[rows, :] = contract_rows(hid[:, rows], rc[...])
            pltpu.make_async_copy(gd.at[rows], gd_out.at[rows], sems.at[2]).start()
    for kind, (buf, out) in enumerate(((gg, gg_out), (gu, gu_out), (gd, gd_out))):
        pltpu.make_async_copy(buf, out, sems.at[kind]).wait()
    for o in stores:
        o.wait()


def finish(rx, rc, hid, gpg, gpu, *small):
    size, model = rx.shape
    units = hid.shape[1]
    vmem = pl.BlockSpec(memory_space=pltpu.VMEM)
    hbm = pl.BlockSpec(memory_space=pltpu.HBM)
    grads = [(model, units), (model, units), (units, model)]
    outs = pl.pallas_call(
        finish_kernel,
        out_shape=[jax.ShapeDtypeStruct(g, F32) for g in grads]
        + [jax.ShapeDtypeStruct(a.shape, a.dtype) for a in small],
        in_specs=[vmem] * (5 + len(small)),
        out_specs=[hbm] * (3 + len(small)),
        scratch_shapes=[pltpu.VMEM(g, F32) for g in grads]
        + [pltpu.SemaphoreType.DMA((3,)), pltpu.SemaphoreType.DMA((len(small),))],
        compiler_params=pltpu.CompilerParams(vmem_limit_bytes=40 * 1024 * 1024),
        name="finish",
    )(rx, rc, hid, gpg, gpu, *small)
    return tuple(out[None] for out in outs[:3]) + tuple(outs[3:])


def shards(
    moe_input, cotangent, routes, route_weights, gate_branch, log_decay, states,
    w_gate, w_up, w_down, out_proj,
):
    groups, parts = lax.axis_size("sp"), lax.axis_size("tp")
    tok_rows, picks = routes.shape
    width = moe_input.shape[1]
    model = width * parts
    units = w_gate.shape[2]
    chans = states.shape[1]
    room = tok_rows * picks * 5 // (4 * groups)
    room = (room + 7) // 8 * 8
    depth = groups // CORES
    high = out_proj.shape[0]
    chunked = groups * parts <= 64
    chunks = groups if chunked else 1
    vmem = pl.BlockSpec(memory_space=pltpu.VMEM)
    hbm = pl.BlockSpec(memory_space=pltpu.HBM)
    dma = pltpu.SemaphoreType.DMA

    def run(*refs):
        whole_kernel(groups, parts, room, chunked, *refs)

    def buf(*shape, kind=BF):
        return pltpu.VMEM(shape, kind)

    outs = pl.pallas_call(
        run,
        out_shape=[
            jax.ShapeDtypeStruct((groups, room, model), BF),
            jax.ShapeDtypeStruct((groups, room, model), BF),
            jax.ShapeDtypeStruct((groups * room, units), BF),
            jax.ShapeDtypeStruct((groups * room, units), BF),
            jax.ShapeDtypeStruct((groups * room, units), BF),
            jax.ShapeDtypeStruct((high, chans), F32),
            jax.ShapeDtypeStruct((tok_rows, chans), BF),
            jax.ShapeDtypeStruct((tok_rows, chans), BF),
            jax.ShapeDtypeStruct((tok_rows, chans), F32),
        ],
        in_specs=[vmem] * 2 + [hbm] * 9,
        out_specs=[vmem] * 9,
        scratch_shapes=[
            buf(tok_rows, width), buf(tok_rows, width), buf(tok_rows, chans),
            buf(tok_rows, chans, kind=F32), buf(tok_rows, chans, kind=F32),
            buf(model, units), buf(model, units), buf(units, model),
            buf(groups, room, width), buf(groups, room, width),
            buf(groups, high, chans), buf(groups, tok_rows, chans), buf(tok_rows, chans),
            buf(parts, groups, room, width), buf(parts - 1, groups, room, width),
            buf(groups, room, width), buf(groups, room, width),
            buf(model, tok_rows), buf(groups, high, tok_rows),
            buf(8, chans, kind=F32), buf(groups - 1, 8, chans, kind=F32), buf(8, chans, kind=F32),
        ]
        + [dma((2, groups))] * 2 + [dma((2, chunks, parts))] * 2 + [dma((2, 2, depth))] * 4
        + [dma((chunks, parts))] * 2 + [dma((groups,))] * 2 + [dma((parts,))] * 2
        + [dma((groups,))] * 4 + [dma(())] * 2 + [dma((9,)), dma((4,))],
        compiler_params=pltpu.CompilerParams(
            collective_id=0, has_side_effects=True, vmem_limit_bytes=40 * 1024 * 1024),
        name="backward",
    )(
        routes.T, route_weights.T,
        *(pltpu.with_memory_space_constraint(a, pltpu.HBM) for a in (
            moe_input, cotangent, gate_branch, states, log_decay, out_proj, w_gate, w_up, w_down)),
    )
    rx, rc = (out.reshape(groups * room, model) for out in outs[:2])
    return finish(rx, rc, *outs[2:])


def flip(index, mask, count):
    total, bit = 0, 1
    while bit < count:
        here = lax.rem(lax.div(index, bit), 2)
        total = total + bit * ((1 - here) if mask & bit else here)
        bit *= 2
    return total


def plane_kernel(
    groups, parts, room,
    routes_any, weights_any, x_any, cot_any, gate_any, states_any, decay_any, proj_any,
    wg_any, wu_any, wd_any,
    rows_x, rows_c, hid_ref, gpg_ref, gpu_ref, outp_ref, ggate_ref, gdecay_ref, gin_ref,
    routes_ref, weights_ref, x_ref, cot_ref, gate_ref, states_ref, decay_ref, wg, wu, wd,
    out_x, out_c, picked_ref, proj_all, mixed_all, act_ref, slope_ref, active_ref, lean_ref,
    terms, shares, passed, summed, back, cot_turned, cot_mine, flipped, blocks, levels, span_ref, past_ref,
    carry_own, carry_in, prev_in,
    o_send, a_recv, t_recv, e_recv, s_recv, m_recv, z_send, z_recv, c_recv, p_send, p_recv, l_sem,
):
    mine, col = lax.axis_index("sp"), lax.axis_index("tp")
    toks, width = x_ref.shape
    model = rows_x.shape[2]
    chans = states_ref.shape[1]
    units = hid_ref.shape[2]
    depth = groups // CORES
    z, core = mine // CORES, lax.rem(mine, CORES)
    size = groups * room
    half = groups // 2
    rows_half = half * room
    inner = jnp.logical_and(z >= 1, z + 1 < depth)

    barrier = pltpu.get_barrier_semaphore()
    for d in range(1, groups):
        pl.semaphore_signal(
            barrier, inc=1, device_id={"sp": lax.rem(mine + d, groups)},
            device_id_type=pl.DeviceIdType.MESH,
        )
    for d in range(1, parts):
        pl.semaphore_signal(
            barrier, inc=1, device_id={"tp": lax.rem(col + d, parts)},
            device_id_type=pl.DeviceIdType.MESH,
        )

    loads = []
    for i, (s, t) in enumerate((
        (x_any, x_ref), (cot_any, cot_ref), (gate_any, gate_ref), (states_any, states_ref),
        (proj_any, proj_all.at[mine]), (decay_any, decay_ref),
        (wg_any.at[0], wg), (wu_any.at[0], wu), (wd_any.at[0], wd),
        (routes_any, routes_ref), (weights_any, weights_ref),
    )):
        loads.append(pltpu.make_async_copy(s, t, l_sem.at[i]))
    for i in (9, 10, 0, 1, 4, 2, 3, 6, 7, 8, 5):
        loads[i].start()

    def near(width_of, index):
        return pl.ds(pl.multiple_of(index * width_of, width_of), width_of)

    def send(src, dst, send_sem, recv_sem, axis, peer):
        c = remote(src, dst, send_sem, recv_sem, axis, peer)
        c.start()
        return c

    def all_sent(ref, sem):
        remote(ref, ref, sem, sem, "tp", tile[1]).wait_send()

    def all_here(ref, sem):
        remote(ref, ref, sem, sem, "tp", tile[1]).wait_recv()

    group = [flip(mine, d, groups) for d in range(groups)]
    tile = [flip(col, p, parts) for p in range(parts)]
    here = near(width, col)

    loads[9].wait()
    loads[10].wait()
    picked, weight = selection(routes_ref[...], weights_ref[...], groups, room)
    picked_ref[...] = picked
    arrivals = [[None] * groups for _ in range(2)]
    gathers = [[None] * groups for _ in range(2)]
    sources = ((out_x, rows_x), (out_c, rows_c))

    def spread(a):
        src, dst = sources[a]
        for d in range(1, groups):
            arrivals[a][d] = send(
                src.at[group[d]], dst.at[mine, :, here], o_send.at[a], a_recv.at[a, d - 1], "sp", group[d])
        dst[mine, :, here] = src[mine]

    def share_out(a, d):
        src, dst = sources[a]
        if d:
            arrivals[a][d].wait_recv()
        own = dst.at[group[d], :, here] if d else src.at[mine]
        gathers[a][d] = [
            send(own, dst.at[group[d], :, here], o_send.at[2 + a],
                 t_recv.at[a, d] if k == d % 2 else e_recv.at[a, d // half], "tp", tile[k + 1])
            for k in range(2)
        ]

    def relay(a, d):
        dst = sources[a][1]
        k = d % 2
        gathers[a][d][k].wait_recv()
        ref = dst.at[group[d], :, near(width, tile[k + 1])]
        send(ref, ref, o_send.at[2 + a], e_recv.at[a, d // half], "tp", tile[2 - k])

    def landed(a, h):
        all_here(sources[a][1].at[pl.ds(0, groups // parts)], e_recv.at[a, h])

    loads[0].wait()
    got = jnp.dot(picked, x_ref[...], preferred_element_type=F32).astype(BF)
    for e in range(groups):
        out_x[e] = got[e * room : (e + 1) * room]
    pl.semaphore_wait(barrier, groups + parts - 2)
    spread(0)
    share_out(0, 0)
    loads[1].wait()
    got = jnp.dot(picked, cot_ref[...], preferred_element_type=F32)
    got = (got * weight).astype(BF)
    for e in range(groups):
        out_c[e] = got[e * room : (e + 1) * room]
    spread(1)

    low = proj_all.shape[1] * 3 // 4
    pairs = (
        proj_all.at[:, pl.ds(0, low)], proj_all.at[:, pl.ds(low, proj_all.shape[1] - low)], mixed_all)
    last = len(pairs) - 1
    hop_send = (4, 13, 5)

    def chain(a, step, wait=False, middle=None):
        buf = pairs[a]
        right = buf.at[jnp.maximum(z - step, 0) * CORES + core]
        left = buf.at[jnp.minimum(z + step, depth - 1) * CORES + core]
        up = jnp.minimum(z + 1, depth - 1) * CORES + core
        down = jnp.maximum(z - 1, 0) * CORES + core
        for way, ref, peer, ok, within in (
            (0, right, up, jnp.logical_and(z - step >= 0, z + 1 < depth),
             jnp.logical_and(z >= 1, z + 2 < depth)),
            (1, left, down, jnp.logical_and(z + step < depth, z >= 1),
             jnp.logical_and(z >= 2, z + 1 < depth)),
        ):
            if middle is not None:
                ok = jnp.logical_and(ok, within if middle else jnp.logical_not(within))

            @pl.when(ok)
            def _(way=way, ref=ref, peer=peer):
                c = remote(ref, ref, z_send.at[a, way, step], z_recv.at[a, way, step], "sp", peer)
                c.wait_send() if wait else c.start()

    partner = z * CORES + (1 - core)

    def across(a, step, way, start=True, also=None):
        ok = z - step >= 0 if way == 0 else z + step < depth
        if also is not None:
            ok = jnp.logical_and(ok, also)
        zz = jnp.maximum(z - step, 0) if way == 0 else jnp.minimum(z + step, depth - 1)
        ref = pairs[a].at[zz * CORES + (core if start else 1 - core)]
        sem = c_recv.at[last + way * depth + step if a == last else a]

        @pl.when(ok)
        def _():
            c = remote(ref, ref, o_send.at[hop_send[a]], sem, "sp", partner)
            c.start() if start else c.wait_recv()

    def advance(a, step, also=None, middle=None):
        for way in range(2):
            if way == 0:
                ok, origin, to = z - 1 - step >= 0, jnp.maximum(z - 1 - step, 0), z + 1
                goes_on, within = z + 1 < depth, jnp.logical_and(z >= 1, z + 2 < depth)
            else:
                ok, origin, to = z + 1 + step < depth, jnp.minimum(z + 1 + step, depth - 1), z - 1
                goes_on, within = z >= 1, jnp.logical_and(z >= 2, z + 1 < depth)
            ref = pairs[a].at[origin * CORES + core]
            peer = jnp.clip(to, 0, depth - 1) * CORES + core
            if also is not None:
                ok = jnp.logical_and(ok, also)
            if middle is not None:
                ok = jnp.logical_and(ok, within if middle else jnp.logical_not(within))

            @pl.when(ok)
            def _(way=way, ref=ref, peer=peer, goes_on=goes_on):
                remote(ref, ref, z_send.at[a, way, step], z_recv.at[a, way, step],
                       "sp", lax.rem(mine + 1, groups)).wait_recv()
                if step + 1 < depth - 1:
                    @pl.when(goes_on)
                    def _():
                        remote(ref, ref, z_send.at[a, way, step + 1], z_recv.at[a, way, step + 1],
                               "sp", peer).start()

            across(a, step + 1, way, also=ok)

    def settle(a):
        for step in range(depth - 1):
            chain(a, step, True)
        all_sent(pairs[a].at[pl.ds(0, depth)], o_send.at[hop_send[a]])

    def collected(step):
        for way in range(2):
            if step or not way:
                across(last, step, way, start=False)

    loads[4].wait()
    for a in range(last):
        chain(a, 0)
        across(a, 0, 0)
    share_out(1, 0)
    share_out(0, 1)
    loads[3].wait()
    prev_copy = send(
        states_ref.at[pl.ds(toks - 8, 8)], prev_in, p_send, p_recv, "sp", lax.rem(mine + 1, groups))

    loads[2].wait()
    act, branch_slope = gelu_parts(gate_ref[...].astype(F32))
    states = states_ref[...]
    act_ref[...] = act
    slope_ref[...] = branch_slope * states
    mixed_all[mine] = (act * states).astype(BF)
    chain(last, 0, middle=False)
    across(last, 0, 0)
    rows = lax.broadcasted_iota(jnp.int32, (toks, toks), 0)
    cols = lax.broadcasted_iota(jnp.int32, (toks, toks), 1)
    eye = jnp.where(rows == cols, 1.0, 0.0).astype(BF)
    fine = cot_turned.shape[2]
    cot_turned[...] = contract_rows(cot_ref[...], eye).astype(BF).reshape(cot_turned.shape)
    cot_mine[col] = cot_turned[:, col]
    share_out(1, 1)
    for p in range(1, parts):
        send(cot_turned.at[:, tile[p]], cot_mine.at[col], o_send.at[6], m_recv.at[0], "tp", tile[p])
    share_out(0, 2)
    share_out(0, 3)
    for a in range(2):
        relay(a, 0)
        relay(a, 1)
    queue = [(0, d) for d in range(2, groups)] + [(1, d) for d in range(2, groups)]
    ahead = queue[2:]

    def pump(count):
        for _ in range(count):
            for _ in range(2):
                if ahead:
                    share_out(*ahead.pop(0))
            for _ in range(2):
                if queue:
                    relay(*queue.pop(0))

    pump(half)

    first = [lax.div(mine, half) * half, (1 - lax.div(mine, half)) * half]

    def forward(h):
        landed(0, h)
        at = pl.ds(first[h], half)
        data = rows_x[at].reshape(rows_half, model)
        pre_gate = jnp.dot(data, wg[...].reshape(model, units), preferred_element_type=F32)
        pre_up = jnp.dot(data, wu[...].reshape(model, units), preferred_element_type=F32)
        active, slope = silu_parts(pre_gate)
        hid_ref[at] = (active * pre_up).astype(BF).reshape(half, room, units)
        active_ref[h] = active
        lean_ref[h] = pre_up * slope

    def hidden_grads(h):
        landed(1, h)
        at = pl.ds(first[h], half)
        grad_hidden = contract_cols(rows_c[at].reshape(rows_half, model), wd[...])
        gpg_ref[at] = (grad_hidden * lean_ref[h]).astype(BF).reshape(half, room, units)
        gpu_ref[at] = (grad_hidden * active_ref[h]).astype(BF).reshape(half, room, units)

    share_copies = [[None, None] for _ in range(groups)]

    def reduce_out(d, i, p):
        g = group[d]
        share_copies[d][i] = send(
            terms.at[p, g], shares.at[i, g], o_send.at[7], s_recv.at[d, i], "tp", tile[1 + d % 2])

    def input_grads(h, order):
        at = pl.ds(first[h], half)
        gate_part = gpg_ref[at].reshape(rows_half, units)
        up_part = gpu_ref[at].reshape(rows_half, units)
        for p in (3, 1, 2, 0):
            term = contract_cols(gate_part, wg[:, tile[p]].reshape(width, units))
            term = term + contract_cols(up_part, wu[:, tile[p]].reshape(width, units))
            terms[p, at] = term.astype(BF).reshape(half, room, width)
            for d in order:
                if p == 3:
                    reduce_out(d, 0, p)
                elif p == 1 + d % 2:
                    reduce_out(d, 1, p)

    def pass_on(d):
        g, far_tile = group[d], 2 - d % 2
        share_copies[d][0].wait_recv()
        passed[g] = (terms[far_tile, g].astype(F32) + shares[0, g].astype(F32)).astype(BF)
        send(passed.at[g], shares.at[2, g], o_send.at[7], s_recv.at[d, 1], "tp", tile[far_tile])

    def bring_back(d):
        g = group[d]
        all_here(shares.at[pl.ds(1, 2), g], s_recv.at[d, 1])
        total = terms[0, g].astype(F32) + shares[1, g].astype(F32) + shares[2, g].astype(F32)
        if d == 0:
            back[mine] = total.astype(BF)
        else:
            summed[d] = total.astype(BF)
            send(summed.at[d], back.at[mine], o_send.at[8], m_recv.at[1], "sp", g)

    for i in (6, 7, 8):
        loads[i].wait()
    forward(0)
    advance(0, 0)
    pump(1)
    advance(1, 0)
    chain(last, 0, middle=True)
    forward(1)

    hidden_grads(0)
    pump(1)
    order = list(range(2, half)) + [1, 0] + list(range(half, groups))
    input_grads(0, order[:half])
    hidden_grads(1)
    for d in order[:2]:
        pass_on(d)
    input_grads(1, order[half:])
    for d in order[2:half]:
        pass_on(d)

    loads[5].wait()
    prev_copy.wait_recv()
    decays = jnp.exp(decay_ref[...])
    line = lax.broadcasted_iota(jnp.int32, decays.shape, 0)
    before = jnp.where(mine > 0, prev_in[7:8, :], 0.0)
    past_ref[...] = decays * jnp.where(line == 0, before, pltpu.roll(states_ref[...], 1, 0))
    span = jnp.where(line < toks - 1, pltpu.roll(decays, toks - 1, 0), 1.0)
    k, level = 1, 0
    while k < toks:
        inside = line < toks - k
        levels[level] = jnp.where(inside, span, 0.0)
        span = span * jnp.where(inside, pltpu.roll(span, toks - k, 0), 1.0)
        k *= 2
        level += 1
    span_ref[...] = span
    head = decays[0:1]

    for step in range(1, depth - 2):
        advance(0, step)
    late = order[half:]
    for d in order:
        if late:
            pass_on(late.pop(0))
        bring_back(d)
    advance(last, 0, middle=True)
    all_here(cot_turned.at[:, pl.ds(0, parts - 1)], m_recv.at[0])
    total = cot_mine[...].reshape(width, toks).astype(F32)
    all_here(back.at[pl.ds(0, groups - 1)], m_recv.at[1])
    total = total + contract_rows(back[...].reshape(size, width), picked_ref[...])
    flipped[:, col] = total.astype(BF).reshape(groups, fine, toks)

    def plane_part(buf, owner, rows, first_sem, to, relayed=0):
        part = buf.at[pl.ds(rows * half, half), owner]
        return send(
            part, part, o_send.at[first_sem // 3 + 8], m_recv.at[first_sem + relayed], "tp", tile[to])

    def plane_start(buf, first_sem):
        copies = [plane_part(buf, col, p - 1, first_sem, p, p) for p in (1, 2)]
        for p in (1, 2):
            plane_part(buf, col, 2 - p, first_sem, p)
        return copies

    def plane_relay(buf, copies, first_sem):
        for p in (1, 2):
            copies[p - 1].wait_recv()
            plane_part(buf, tile[p], p - 1, first_sem, 3 - p)

    grad_copies = plane_start(flipped, 3)
    for d in range(1, groups):
        send(flipped.at[group[d], col], blocks.at[mine, col], o_send.at[11], m_recv.at[2], "sp", group[d])
    blocks[mine, col] = flipped[mine, col]
    for step in range(1, depth - 2):
        advance(1, step)
    advance(last, 0, middle=False)
    plane_relay(flipped, grad_copies, 3)
    all_here(blocks.at[pl.ds(0, groups - 1), 0], m_recv.at[2])
    plane_copies = plane_start(blocks, 6)
    advance(0, depth - 2)
    for step in range(1, depth - 2):
        advance(last, step, inner)
    all_here(flipped.at[:, pl.ds(0, 2)], m_recv.at[3])
    advance(1, depth - 2)
    for a in range(last):
        all_here(pairs[a].at[pl.ds(0, depth)], c_recv.at[a])
    grad_mixed = contract_rows(flipped[...].reshape(model, toks), proj_all[...].reshape(model, chans))
    ggate_ref[...] = (grad_mixed * slope_ref[...]).astype(BF)
    local = grad_mixed * act_ref[...]
    k, level = 1, 0
    while k < toks:
        local = local + levels[level] * pltpu.roll(local, toks - k, 0)
        k *= 2
        level += 1
    carry_own[0:1] = span_ref[0:1, :] * head
    carry_own[1:2] = local[0:1] * head
    for d in range(1, groups):
        send(carry_own, carry_in.at[d - 1], o_send.at[12], m_recv.at[9], "sp", lax.rem(mine + d, groups))
    plane_relay(blocks, plane_copies, 6)
    for step in range(1, depth - 2):
        advance(last, step, jnp.logical_not(inner))
    for step in range(depth - 1):
        collected(step)
    all_here(blocks.at[:, pl.ds(0, 2)], m_recv.at[6])
    advance(last, depth - 2)
    high = blocks.shape[1] * blocks.shape[2]

    def out_part(t):
        return jnp.dot(blocks[t].reshape(high, toks), mixed_all[t], preferred_element_type=F32)

    near_part = out_part(group[0])
    for d in range(1, groups - CORES):
        near_part = near_part + out_part(group[d])
    outp_ref[...] = near_part
    all_here(carry_in, m_recv.at[9])
    carried = jnp.zeros((1, chans), F32)
    for ahead in range(groups - 1, 0, -1):
        got = carry_in[groups - ahead - 1]
        carried = jnp.where(mine + ahead < groups, got[1:2] + got[0:1] * carried, carried)
    grad_in = local + span_ref[...] * carried
    gin_ref[...] = grad_in
    gdecay_ref[...] = (grad_in * past_ref[...]).astype(BF)
    collected(depth - 1)
    far_part = out_part(group[groups - CORES])
    for d in range(groups - CORES + 1, groups):
        far_part = far_part + out_part(group[d])
    outp_ref[...] += far_part
    for a in range(last + 1):
        settle(a)
    for a in range(2):
        all_sent(rows_x.at[pl.ds(0, groups - 1), :, pl.ds(0, width)], o_send.at[a])
        all_sent(rows_x.at[pl.ds(0, groups * 3 // parts)], o_send.at[2 + a])
    all_sent(cot_turned.at[:, pl.ds(0, parts - 1)], o_send.at[6])
    all_sent(rows_x.at[pl.ds(0, groups * 3 // parts)], o_send.at[7])
    all_sent(back.at[pl.ds(0, groups - 1)], o_send.at[8])
    for i in (9, 10):
        all_sent(flipped.at[:, pl.ds(0, 3)], o_send.at[i])
    all_sent(blocks.at[pl.ds(0, groups - 1), 0], o_send.at[11])
    all_sent(carry_in, o_send.at[12])
    prev_copy.wait_send()


def plane_shards(
    moe_input, cotangent, routes, route_weights, gate_branch, log_decay, states,
    w_gate, w_up, w_down, out_proj,
):
    groups, parts = lax.axis_size("sp"), lax.axis_size("tp")
    tok_rows, picks = routes.shape
    width = moe_input.shape[1]
    model = width * parts
    units = w_gate.shape[2]
    chans = states.shape[1]
    room = tok_rows * picks * 5 // (4 * groups)
    room = (room + 7) // 8 * 8
    depth = groups // CORES
    high = out_proj.shape[0]
    fine = high // parts
    doublings = (tok_rows - 1).bit_length()
    vmem = pl.BlockSpec(memory_space=pltpu.VMEM)
    hbm = pl.BlockSpec(memory_space=pltpu.HBM)
    dma = pltpu.SemaphoreType.DMA

    def run(*refs):
        plane_kernel(groups, parts, room, *refs)

    def buf(*shape, kind=BF):
        return pltpu.VMEM(shape, kind)

    def split(weight):
        return weight.reshape(1, groups, parts, fine, units)

    outs = pl.pallas_call(
        run,
        out_shape=[
            jax.ShapeDtypeStruct((groups, room, model), BF),
            jax.ShapeDtypeStruct((groups, room, model), BF),
            jax.ShapeDtypeStruct((groups, room, units), BF),
            jax.ShapeDtypeStruct((groups, room, units), BF),
            jax.ShapeDtypeStruct((groups, room, units), BF),
            jax.ShapeDtypeStruct((high, chans), F32),
            jax.ShapeDtypeStruct((tok_rows, chans), BF),
            jax.ShapeDtypeStruct((tok_rows, chans), BF),
            jax.ShapeDtypeStruct((tok_rows, chans), F32),
        ],
        in_specs=[hbm] * 11,
        out_specs=[vmem] * 9,
        scratch_shapes=[
            buf(picks, tok_rows, kind=jnp.int32), buf(picks, tok_rows, kind=F32),
            buf(tok_rows, width), buf(tok_rows, width), buf(tok_rows, chans),
            buf(tok_rows, chans, kind=F32), buf(tok_rows, chans, kind=F32),
            buf(groups, parts, fine, units), buf(groups, parts, fine, units), buf(units, model),
            buf(groups, room, width), buf(groups, room, width), buf(groups * room, tok_rows),
            buf(groups, high, chans), buf(groups, tok_rows, chans),
            buf(tok_rows, chans, kind=F32), buf(tok_rows, chans, kind=F32),
            buf(2, groups // 2 * room, units, kind=F32), buf(2, groups // 2 * room, units, kind=F32),
            buf(parts, groups, room, width), buf(parts - 1, groups, room, width),
            buf(groups, room, width), buf(groups, room, width), buf(groups, room, width),
            buf(groups // parts, parts, fine, tok_rows), buf(parts, groups // parts, fine, tok_rows),
            buf(groups, parts, fine, tok_rows), buf(groups, parts, fine, tok_rows),
            buf(doublings, tok_rows, chans, kind=F32), buf(tok_rows, chans, kind=F32),
            buf(tok_rows, chans, kind=F32),
            buf(2, chans, kind=F32), buf(groups - 1, 2, chans, kind=F32), buf(8, chans, kind=F32),
        ]
        + [dma((14,)), dma((2, groups - 1)), dma((2, groups)), dma((2, 2)), dma((groups, 2))]
        + [dma((10,)), dma((3, 2, depth - 1)), dma((3, 2, depth - 1)), dma((2 + 2 * depth,))]
        + [dma(()), dma(()), dma((11,))],
        compiler_params=pltpu.CompilerParams(
            collective_id=0, has_side_effects=True, vmem_limit_bytes=40 * 1024 * 1024),
        name="backward",
    )(
        *(pltpu.with_memory_space_constraint(a, pltpu.HBM) for a in (
            routes.T, route_weights.T, moe_input, cotangent, gate_branch, states, log_decay, out_proj,
            split(w_gate), split(w_up), w_down)),
    )
    rx, rc = (out.reshape(groups * room, model) for out in outs[:2])
    grads = (out.reshape(groups * room, units) for out in outs[2:5])
    return finish(rx, rc, *grads, *outs[5:])


def solution(mesh):
    groups, parts = mesh.shape["sp"], mesh.shape["tp"]
    plane = parts == 4 and groups % parts == 0 and groups & (groups - 1) == 0
    return jax.shard_map(
        plane_shards if plane else shards,
        mesh=mesh,
        in_specs=(
            P("sp", "tp"), P("sp", "tp"), P("sp", None), P("sp", None), P("sp", "tp"),
            P("sp", "tp"), P("sp", "tp"), P("sp", None, "tp"), P("sp", None, "tp"),
            P("sp", "tp", None), P("sp", "tp"),
        ),
        out_specs=(
            P("sp", None, "tp"), P("sp", None, "tp"), P("sp", "tp", None), P("sp", "tp"),
            P("sp", "tp"), P("sp", "tp"), P("sp", "tp"),
        ),
        check_vma=False,
    )
```

```python
import jax
import jax.numpy as jnp
from jax import lax
from jax.experimental import pallas as pl
from jax.experimental.pallas import tpu as pltpu
from jax.sharding import PartitionSpec as P

BF = jnp.bfloat16
F32 = jnp.float32
CORES = 2
GELU_C = 0.7978845608028654
GELU_A = 0.044715


def silu_parts(pre_gate):
    sigmoid_val = jax.nn.sigmoid(pre_gate)
    return (pre_gate * sigmoid_val, sigmoid_val * (1.0 + pre_gate * (1.0 - sigmoid_val)))


def contract_rows(left_mat, right_mat):
    return lax.dot_general(
        left_mat, right_mat, (((0,), (0,)), ((), ())), preferred_element_type=F32
    )


def contract_cols(left_mat, right_mat):
    return lax.dot_general(
        left_mat, right_mat, (((1,), (1,)), ((), ())), preferred_element_type=F32
    )


def gelu_parts(x):
    t = jnp.tanh(GELU_C * (x + GELU_A * (x * x * x)))
    half = 0.5 * (1.0 + t)
    slope = half + 0.5 * x * (1.0 - t * t) * (GELU_C * (1.0 + 3.0 * GELU_A * x * x))
    return x * half, slope


def selection(routes_t, weights_t, groups, room):
    picks, toks = routes_t.shape
    experts = lax.broadcasted_iota(jnp.int32, (groups, toks), 0)
    named = jnp.zeros((groups, toks), F32)
    weight = jnp.zeros((groups, toks), F32)
    for k in range(picks):
        hit = routes_t[k : k + 1, :] == experts
        named = named + jnp.where(hit, 1.0, 0.0)
        weight = weight + jnp.where(hit, weights_t[k : k + 1, :], 0.0)
    rows = lax.broadcasted_iota(jnp.int32, (toks, toks), 0)
    cols = lax.broadcasted_iota(jnp.int32, (toks, toks), 1)
    before = jnp.where(rows < cols, 1.0, 0.0).astype(BF)
    slot = jnp.dot(named.astype(BF), before, preferred_element_type=F32)
    slot = jnp.where(named > 0.5, slot, -1.0)
    place = lax.broadcasted_iota(jnp.int32, (room, toks), 0).astype(F32)
    picked, column = [], []
    for e in range(groups):
        one = jnp.where(slot[e : e + 1, :] == place, 1.0, 0.0)
        picked.append(one)
        column.append(jnp.sum(one * weight[e : e + 1, :], axis=1, keepdims=True))
    return jnp.concatenate(picked, axis=0).astype(BF), jnp.concatenate(column, axis=0)


def greet(groups, parts, mine, col):
    barrier = pltpu.get_barrier_semaphore()
    for d in range(1, groups):
        pl.semaphore_signal(
            barrier, inc=1, device_id={"sp": lax.rem(mine + d, groups)},
            device_id_type=pl.DeviceIdType.MESH,
        )
    for d in range(1, parts):
        pl.semaphore_signal(
            barrier, inc=1, device_id={"tp": lax.rem(col + d, parts)},
            device_id_type=pl.DeviceIdType.MESH,
        )
    pl.semaphore_wait(barrier, groups + parts - 2)


def remote(src, dst, send, recv, axis, peer):
    return pltpu.make_async_remote_copy(
        src_ref=src, dst_ref=dst, send_sem=send, recv_sem=recv,
        device_id={axis: peer}, device_id_type=pl.DeviceIdType.MESH,
    )


def whole_kernel(
    groups, parts, room, chunked,
    routes_ref, weights_ref, x_any, cot_any, gate_any, states_any, decay_any, proj_any,
    wg_any, wu_any, wd_any,
    rows_x, rows_c, hid_ref, gpg_ref, gpu_ref, outp_ref, ggate_ref, gdecay_ref, gin_ref,
    x_ref, cot_ref, gate_ref, states_ref, decay_ref, wg, wu, wd,
    out_x, out_c, proj_all, mixed_all, mix_own,
    terms, shares, summed, back, flipped, blocks, carry_own, carry_in, prev_in,
    a_send, a_recv, t_send, t_recv, z_send, z_recv, c_send, c_recv,
    s_send, s_recv, r_send, r_recv, g_send, g_recv, b_send, b_recv, k_send, k_recv, p_send, p_recv,
    l_sem, w_sem,
):
    mine, col = lax.axis_index("sp"), lax.axis_index("tp")
    toks, width = x_ref.shape
    model = rows_x.shape[2]
    depth = groups // CORES
    z, core = mine // CORES, lax.rem(mine, CORES)
    size = groups * room

    def near(width_of, index):
        return pl.ds(pl.multiple_of(index * width_of, width_of), width_of)

    loads = []
    for i, (s, t) in enumerate((
        (x_any, x_ref), (cot_any, cot_ref), (gate_any, gate_ref), (states_any, states_ref),
        (proj_any, proj_all.at[mine]), (decay_any, decay_ref),
        (wg_any.at[0], wg), (wu_any.at[0], wu), (wd_any.at[0], wd),
    )):
        o = pltpu.make_async_copy(s, t, l_sem.at[i])
        o.start()
        loads.append(o)

    picked, weight = selection(routes_ref[...], weights_ref[...], groups, room)
    loads[0].wait()
    got = jnp.dot(picked, x_ref[...], preferred_element_type=F32).astype(BF)
    for e in range(groups):
        out_x[e] = got[e * room : (e + 1) * room]
    loads[1].wait()
    got_c = jnp.dot(picked, cot_ref[...], preferred_element_type=F32)
    got_c = (got_c * weight).astype(BF)
    for e in range(groups):
        out_c[e] = got_c[e * room : (e + 1) * room]
    greet(groups, parts, mine, col)

    here = near(width, col)
    sends, own = [], []
    arrivals = [[None] * groups for _ in range(2)]
    for a, (src, dst) in enumerate(((out_x, rows_x), (out_c, rows_c))):
        for d in range(1, groups):
            peer = lax.rem(mine + d, groups)
            c = remote(src.at[peer], dst.at[mine, :, here], a_send.at[a, d], a_recv.at[a, d], "sp", peer)
            c.start()
            arrivals[a][d] = c
            sends.append(c)
        o = pltpu.make_async_copy(src.at[mine], dst.at[mine, :, here], w_sem.at[a])
        o.start()
        own.append(o)

    pairs = (proj_all, mixed_all)

    def chain(a, step, wait=False):
        buf = pairs[a]
        right = buf.at[jnp.maximum(z - step, 0) * CORES + core]
        left = buf.at[jnp.minimum(z + step, depth - 1) * CORES + core]
        up = jnp.minimum(z + 1, depth - 1) * CORES + core
        down = jnp.maximum(z - 1, 0) * CORES + core
        for way, ref, peer, ok in (
            (0, right, up, jnp.logical_and(z - step >= 0, z + 1 < depth)),
            (1, left, down, jnp.logical_and(z + step < depth, z >= 1)),
        ):
            @pl.when(ok)
            def _(way=way, ref=ref, peer=peer):
                c = remote(ref, ref, z_send.at[a, way, step], z_recv.at[a, way, step], "sp", peer)
                c.wait_send() if wait else c.start()

    partner = z * CORES + (1 - core)

    def across(a, step, way, mode):
        ok = z - step >= 0 if way == 0 else z + step < depth
        zz = jnp.maximum(z - step, 0) if way == 0 else jnp.minimum(z + step, depth - 1)
        ref = pairs[a].at[zz * CORES + (1 - core if mode == "recv" else core)]

        @pl.when(ok)
        def _():
            c = remote(ref, ref, c_send.at[a, way, step], c_recv.at[a, way, step], "sp", partner)
            if mode == "start":
                c.start()
            elif mode == "send":
                c.wait_send()
            else:
                c.wait_recv()

    def advance(a, step):
        buf = pairs[a]
        from_l = buf.at[jnp.maximum(z - 1 - step, 0) * CORES + core]
        from_r = buf.at[jnp.minimum(z + 1 + step, depth - 1) * CORES + core]
        for way, ok, ref in ((0, z - 1 - step >= 0, from_l), (1, z + 1 + step < depth, from_r)):
            @pl.when(ok)
            def _(way=way, ref=ref):
                remote(ref, ref, z_send.at[a, way, step], z_recv.at[a, way, step],
                       "sp", lax.rem(mine + 1, groups)).wait_recv()
        if step + 1 < depth - 1:
            chain(a, step + 1)
        across(a, step + 1, 0, "start")
        across(a, step + 1, 1, "start")

    def settle(a):
        for step in range(depth - 1):
            chain(a, step, True)
        for step in range(depth):
            for way in range(2):
                if step or not way:
                    across(a, step, way, "send")

    def collected(a):
        for step in range(depth):
            for way in range(2):
                if step or not way:
                    across(a, step, way, "recv")

    loads[4].wait()
    chain(0, 0)
    across(0, 0, 0, "start")

    gathers = [[], []]

    def gather(a, src, dst):
        if chunked:
            for d in range(groups):
                at = lax.rem(mine + groups - d, groups)
                if d:
                    arrivals[a][d].wait_recv()
                for p in range(1, parts):
                    c = remote(dst.at[at, :, here] if d else src.at[mine], dst.at[at, :, here],
                               t_send.at[a, d, p], t_recv.at[a, d, p], "tp", lax.rem(col + p, parts))
                    c.start()
                    gathers[a].append(c)
            own[a].wait()
        else:
            own[a].wait()
            for d in range(1, groups):
                arrivals[a][d].wait_recv()
            for p in range(1, parts):
                c = remote(dst.at[:, :, here], dst.at[:, :, here],
                           t_send.at[a, 0, p], t_recv.at[a, 0, p], "tp", lax.rem(col + p, parts))
                c.start()
                gathers[a].append(c)
        sends.extend(gathers[a])

    gather(0, out_x, rows_x)
    loads[2].wait()
    loads[3].wait()
    act, branch_slope = gelu_parts(gate_ref[...].astype(F32))
    mix_own[...] = (act * states_ref[...]).astype(BF)
    gather(1, out_c, rows_c)
    o = pltpu.make_async_copy(mix_own, mixed_all.at[mine], w_sem.at[3])
    o.start()
    o.wait()
    for i in range(6, 9):
        loads[i].wait()
    for c in gathers[0]:
        c.wait_recv()
    row_data = rows_x[...].reshape(size, model)
    pre_gate = jnp.dot(row_data, wg[...], preferred_element_type=F32)
    pre_up = jnp.dot(row_data, wu[...], preferred_element_type=F32)
    active, slope = silu_parts(pre_gate)
    hidden = (active * pre_up).astype(BF)
    hid_ref[...] = hidden
    lean = pre_up * slope
    advance(0, 0)
    if depth > 2:
        advance(0, 1)
    for c in gathers[1]:
        c.wait_recv()
    grad_hidden = contract_cols(rows_c[...].reshape(size, model), wd[...])
    grad_pre_gate = (grad_hidden * lean).astype(BF)
    grad_pre_up = (grad_hidden * active).astype(BF)
    gpg_ref[...] = grad_pre_gate
    gpu_ref[...] = grad_pre_up
    for d in list(range(1, parts)) + [0]:
        part = near(width, lax.rem(col + d, parts))
        term = contract_cols(grad_pre_gate, wg[part, :]) + contract_cols(grad_pre_up, wu[part, :])
        terms[d] = term.astype(BF).reshape(groups, room, width)

    share_copies = {}
    order = list(range(1, groups)) + [0]
    for d in order if chunked else [0]:
        at = lax.rem(mine + d, groups)
        for p in range(1, parts):
            src = terms.at[p, at] if chunked else terms.at[p]
            dst = shares.at[p - 1, at] if chunked else shares.at[p - 1]
            c = remote(src, dst, s_send.at[d, p], s_recv.at[d, p], "tp", lax.rem(col + p, parts))
            c.start()
            share_copies[d, p] = c
            sends.append(c)
    for step in range(2, depth - 1):
        advance(0, step)
    chain(1, 0)
    across(1, 0, 0, "start")

    back_copies = []
    for d in order:
        at = lax.rem(mine + d, groups)
        if chunked or d == 1:
            for p in range(1, parts):
                share_copies[d if chunked else 0, p].wait_recv()
        total = terms[0, at].astype(F32)
        for p in range(1, parts):
            total = total + shares[p - 1, at].astype(F32)
        if d == 0:
            back[mine] = total.astype(BF)
        else:
            summed[d] = total.astype(BF)
            c = remote(summed.at[d], back.at[mine], r_send.at[d], r_recv.at[d], "sp", at)
            c.start()
            back_copies.append(c)
    nxt = lax.rem(mine + 1, groups)
    prev_copy = remote(states_ref.at[pl.ds(toks - 8, 8)], prev_in, p_send, p_recv, "sp", nxt)
    prev_copy.start()
    advance(1, 0)
    rows = lax.broadcasted_iota(jnp.int32, (toks, toks), 0)
    cols = lax.broadcasted_iota(jnp.int32, (toks, toks), 1)
    eye = jnp.where(rows == cols, 1.0, 0.0).astype(BF)
    total = contract_rows(cot_ref[...], eye)
    for c in back_copies:
        c.wait_recv()
    total = total + contract_rows(back[...].reshape(size, width), picked)
    flipped[here, :] = total.astype(BF)
    grad_copies = []
    for d in range(1, parts):
        part = flipped.at[here]
        c = remote(part, part, g_send.at[d], g_recv.at[d], "tp", lax.rem(col + d, parts))
        c.start()
        grad_copies.append(c)
    for step in range(1, depth - 1):
        advance(1, step)
    collected(0)
    loads[5].wait()
    for c in grad_copies:
        c.wait_recv()
    high = model // groups
    block_copies = []
    for d in range(1, groups):
        peer = lax.rem(mine + d, groups)
        c = remote(flipped.at[near(high, peer)], blocks.at[mine], b_send.at[d], b_recv.at[d], "sp", peer)
        c.start()
        block_copies.append(c)
    grad_mixed = contract_rows(flipped[...], proj_all[...].reshape(model, states_ref.shape[1]))
    states = states_ref[...]
    act, branch_slope = gelu_parts(gate_ref[...].astype(F32))
    decays = jnp.exp(decay_ref[...])
    ggate_ref[...] = (grad_mixed * states * branch_slope).astype(BF)
    local = grad_mixed * act
    line = lax.broadcasted_iota(jnp.int32, local.shape, 0)
    span = jnp.where(line < toks - 1, pltpu.roll(decays, toks - 1, 0), 1.0)
    k = 1
    while k < toks:
        inside = line < toks - k
        local = local + span * jnp.where(inside, pltpu.roll(local, toks - k, 0), 0.0)
        span = span * jnp.where(inside, pltpu.roll(span, toks - k, 0), 1.0)
        k *= 2
    eight = lax.broadcasted_iota(jnp.int32, (8, local.shape[1]), 0)
    whole = span[0:1] * decays[0:1]
    entry = local[0:1] * decays[0:1]
    carry_own[...] = jnp.where(eight == 0, whole, entry)
    carry_copies = []
    for d in range(1, groups):
        peer = lax.rem(mine + d, groups)
        c = remote(carry_own, carry_in.at[d - 1], k_send.at[d], k_recv.at[d], "sp", peer)
        c.start()
        carry_copies.append(c)
    collected(1)
    total = jnp.dot(flipped[near(high, mine), :], mixed_all[mine], preferred_element_type=F32)
    for d in range(1, groups):
        block_copies[d - 1].wait_recv()
        at = lax.rem(mine + groups - d, groups)
        total = total + jnp.dot(blocks[at], mixed_all[at], preferred_element_type=F32)
    outp_ref[...] = total
    prev_copy.wait_recv()
    first = jnp.where(mine > 0, prev_in[7:8, :], 0.0)
    prev = jnp.where(line == 0, first, pltpu.roll(states, 1, 0))
    for c in carry_copies:
        c.wait_recv()
    carried = jnp.zeros_like(whole)
    for ahead in range(groups - 1, 0, -1):
        got = carry_in[groups - ahead - 1]
        carried = jnp.where(mine + ahead < groups, got[1:2] + got[0:1] * carried, carried)
    grad_in = local + span * carried
    gin_ref[...] = grad_in
    gdecay_ref[...] = (grad_in * decays * prev).astype(BF)
    settle(0)
    settle(1)
    for c in [prev_copy] + sends + back_copies + grad_copies + block_copies + carry_copies:
        c.wait_send()


def finish_kernel(
    rx, rc, hid, gpg, gpu, outp, ggate, gdecay, gin,
    gg_out, gu_out, gd_out, outp_out, ggate_out, gdecay_out, gin_out,
    gg, gu, gd, sems, small_sems,
):
    stores = []
    for i, (src, dst) in enumerate((
        (outp, outp_out), (ggate, ggate_out), (gdecay, gdecay_out), (gin, gin_out),
    )):
        o = pltpu.make_async_copy(src, dst, small_sems.at[i])
        o.start()
        stores.append(o)
    step = 256
    steps = rx.shape[1] // step
    units = hid.shape[1]
    down = units // 4
    for i in range(steps):
        part = slice(i * step, (i + 1) * step)
        for kind, grad, buf, out in ((0, gpg, gg, gg_out), (1, gpu, gu, gu_out)):
            buf[part, :] = contract_rows(rx[:, part], grad[...])
            pltpu.make_async_copy(buf.at[part], out.at[part], sems.at[kind]).start()
        if i % (steps // 4) == 0:
            rows = slice(i * 4 // steps * down, (i * 4 // steps + 1) * down)
            gd[rows, :] = contract_rows(hid[:, rows], rc[...])
            pltpu.make_async_copy(gd.at[rows], gd_out.at[rows], sems.at[2]).start()
    for kind, (buf, out) in enumerate(((gg, gg_out), (gu, gu_out), (gd, gd_out))):
        pltpu.make_async_copy(buf, out, sems.at[kind]).wait()
    for o in stores:
        o.wait()


def finish(rx, rc, hid, gpg, gpu, *small):
    size, model = rx.shape
    units = hid.shape[1]
    vmem = pl.BlockSpec(memory_space=pltpu.VMEM)
    hbm = pl.BlockSpec(memory_space=pltpu.HBM)
    grads = [(model, units), (model, units), (units, model)]
    outs = pl.pallas_call(
        finish_kernel,
        out_shape=[jax.ShapeDtypeStruct(g, F32) for g in grads]
        + [jax.ShapeDtypeStruct(a.shape, a.dtype) for a in small],
        in_specs=[vmem] * (5 + len(small)),
        out_specs=[hbm] * (3 + len(small)),
        scratch_shapes=[pltpu.VMEM(g, F32) for g in grads]
        + [pltpu.SemaphoreType.DMA((3,)), pltpu.SemaphoreType.DMA((len(small),))],
        compiler_params=pltpu.CompilerParams(vmem_limit_bytes=40 * 1024 * 1024),
        name="finish",
    )(rx, rc, hid, gpg, gpu, *small)
    return tuple(out[None] for out in outs[:3]) + tuple(outs[3:])


def shards(
    moe_input, cotangent, routes, route_weights, gate_branch, log_decay, states,
    w_gate, w_up, w_down, out_proj,
):
    groups, parts = lax.axis_size("sp"), lax.axis_size("tp")
    tok_rows, picks = routes.shape
    width = moe_input.shape[1]
    model = width * parts
    units = w_gate.shape[2]
    chans = states.shape[1]
    room = tok_rows * picks * 5 // (4 * groups)
    room = (room + 7) // 8 * 8
    depth = groups // CORES
    high = out_proj.shape[0]
    chunked = groups * parts <= 64
    chunks = groups if chunked else 1
    vmem = pl.BlockSpec(memory_space=pltpu.VMEM)
    hbm = pl.BlockSpec(memory_space=pltpu.HBM)
    dma = pltpu.SemaphoreType.DMA

    def run(*refs):
        whole_kernel(groups, parts, room, chunked, *refs)

    def buf(*shape, kind=BF):
        return pltpu.VMEM(shape, kind)

    outs = pl.pallas_call(
        run,
        out_shape=[
            jax.ShapeDtypeStruct((groups, room, model), BF),
            jax.ShapeDtypeStruct((groups, room, model), BF),
            jax.ShapeDtypeStruct((groups * room, units), BF),
            jax.ShapeDtypeStruct((groups * room, units), BF),
            jax.ShapeDtypeStruct((groups * room, units), BF),
            jax.ShapeDtypeStruct((high, chans), F32),
            jax.ShapeDtypeStruct((tok_rows, chans), BF),
            jax.ShapeDtypeStruct((tok_rows, chans), BF),
            jax.ShapeDtypeStruct((tok_rows, chans), F32),
        ],
        in_specs=[vmem] * 2 + [hbm] * 9,
        out_specs=[vmem] * 9,
        scratch_shapes=[
            buf(tok_rows, width), buf(tok_rows, width), buf(tok_rows, chans),
            buf(tok_rows, chans, kind=F32), buf(tok_rows, chans, kind=F32),
            buf(model, units), buf(model, units), buf(units, model),
            buf(groups, room, width), buf(groups, room, width),
            buf(groups, high, chans), buf(groups, tok_rows, chans), buf(tok_rows, chans),
            buf(parts, groups, room, width), buf(parts - 1, groups, room, width),
            buf(groups, room, width), buf(groups, room, width),
            buf(model, tok_rows), buf(groups, high, tok_rows),
            buf(8, chans, kind=F32), buf(groups - 1, 8, chans, kind=F32), buf(8, chans, kind=F32),
        ]
        + [dma((2, groups))] * 2 + [dma((2, chunks, parts))] * 2 + [dma((2, 2, depth))] * 4
        + [dma((chunks, parts))] * 2 + [dma((groups,))] * 2 + [dma((parts,))] * 2
        + [dma((groups,))] * 4 + [dma(())] * 2 + [dma((9,)), dma((4,))],
        compiler_params=pltpu.CompilerParams(
            collective_id=0, has_side_effects=True, vmem_limit_bytes=40 * 1024 * 1024),
        name="backward",
    )(
        routes.T, route_weights.T,
        *(pltpu.with_memory_space_constraint(a, pltpu.HBM) for a in (
            moe_input, cotangent, gate_branch, states, log_decay, out_proj, w_gate, w_up, w_down)),
    )
    rx, rc = (out.reshape(groups * room, model) for out in outs[:2])
    return finish(rx, rc, *outs[2:])


def flip(index, mask, count):
    total, bit = 0, 1
    while bit < count:
        here = lax.rem(lax.div(index, bit), 2)
        total = total + bit * ((1 - here) if mask & bit else here)
        bit *= 2
    return total


def plane_kernel(
    groups, parts, room,
    routes_any, weights_any, x_any, cot_any, gate_any, states_any, decay_any, proj_any,
    wg_any, wu_any, wd_any,
    rows_x, rows_c, hid_ref, gpg_ref, gpu_ref, outp_ref, ggate_ref, gdecay_ref, gin_ref,
    routes_ref, weights_ref, x_ref, cot_ref, gate_ref, states_ref, decay_ref, wg, wu, wd,
    out_x, out_c, picked_ref, proj_all, mixed_all, act_ref, slope_ref, active_ref, lean_ref,
    terms, shares, passed, summed, back, cot_turned, cot_mine, flipped, blocks, levels, span_ref, past_ref,
    carry_own, carry_in, prev_in,
    o_send, a_recv, t_recv, e_recv, s_recv, m_recv, z_send, z_recv, c_recv, p_send, p_recv, l_sem,
):
    mine, col = lax.axis_index("sp"), lax.axis_index("tp")
    toks, width = x_ref.shape
    model = rows_x.shape[2]
    chans = states_ref.shape[1]
    units = hid_ref.shape[2]
    depth = groups // CORES
    z, core = mine // CORES, lax.rem(mine, CORES)
    size = groups * room
    half = groups // 2
    rows_half = half * room
    inner = jnp.logical_and(z >= 1, z + 1 < depth)

    barrier = pltpu.get_barrier_semaphore()
    for d in range(1, groups):
        pl.semaphore_signal(
            barrier, inc=1, device_id={"sp": lax.rem(mine + d, groups)},
            device_id_type=pl.DeviceIdType.MESH,
        )
    for d in range(1, parts):
        pl.semaphore_signal(
            barrier, inc=1, device_id={"tp": lax.rem(col + d, parts)},
            device_id_type=pl.DeviceIdType.MESH,
        )

    loads = []
    for i, (s, t) in enumerate((
        (x_any, x_ref), (cot_any, cot_ref), (gate_any, gate_ref), (states_any, states_ref),
        (proj_any, proj_all.at[mine]), (decay_any, decay_ref),
        (wg_any.at[0], wg), (wu_any.at[0], wu), (wd_any.at[0], wd),
        (routes_any, routes_ref), (weights_any, weights_ref),
    )):
        loads.append(pltpu.make_async_copy(s, t, l_sem.at[i]))
    for i in (9, 10, 0, 1, 4, 2, 3, 6, 7, 8, 5):
        loads[i].start()

    def near(width_of, index):
        return pl.ds(pl.multiple_of(index * width_of, width_of), width_of)

    def send(src, dst, send_sem, recv_sem, axis, peer):
        c = remote(src, dst, send_sem, recv_sem, axis, peer)
        c.start()
        return c

    def all_sent(ref, sem):
        remote(ref, ref, sem, sem, "tp", tile[1]).wait_send()

    def all_here(ref, sem):
        remote(ref, ref, sem, sem, "tp", tile[1]).wait_recv()

    group = [flip(mine, d, groups) for d in range(groups)]
    tile = [flip(col, p, parts) for p in range(parts)]
    here = near(width, col)

    loads[9].wait()
    loads[10].wait()
    picked, weight = selection(routes_ref[...], weights_ref[...], groups, room)
    picked_ref[...] = picked
    arrivals = [[None] * groups for _ in range(2)]
    gathers = [[None] * groups for _ in range(2)]
    sources = ((out_x, rows_x), (out_c, rows_c))

    def spread(a):
        src, dst = sources[a]
        for d in range(1, groups):
            arrivals[a][d] = send(
                src.at[group[d]], dst.at[mine, :, here], o_send.at[a], a_recv.at[a, d - 1], "sp", group[d])
        dst[mine, :, here] = src[mine]

    def share_out(a, d):
        src, dst = sources[a]
        if d:
            arrivals[a][d].wait_recv()
        own = dst.at[group[d], :, here] if d else src.at[mine]
        gathers[a][d] = [
            send(own, dst.at[group[d], :, here], o_send.at[2 + a],
                 t_recv.at[a, d] if k == d % 2 else e_recv.at[a, d // half], "tp", tile[k + 1])
            for k in range(2)
        ]

    def relay(a, d):
        dst = sources[a][1]
        k = d % 2
        gathers[a][d][k].wait_recv()
        ref = dst.at[group[d], :, near(width, tile[k + 1])]
        send(ref, ref, o_send.at[2 + a], e_recv.at[a, d // half], "tp", tile[2 - k])

    def landed(a, h):
        all_here(sources[a][1].at[pl.ds(0, groups // parts)], e_recv.at[a, h])

    loads[0].wait()
    got = jnp.dot(picked, x_ref[...], preferred_element_type=F32).astype(BF)
    for e in range(groups):
        out_x[e] = got[e * room : (e + 1) * room]
    pl.semaphore_wait(barrier, groups + parts - 2)
    spread(0)
    share_out(0, 0)
    loads[1].wait()
    got = jnp.dot(picked, cot_ref[...], preferred_element_type=F32)
    got = (got * weight).astype(BF)
    for e in range(groups):
        out_c[e] = got[e * room : (e + 1) * room]
    spread(1)

    low = proj_all.shape[1] * 3 // 4
    pairs = (
        proj_all.at[:, pl.ds(0, low)], proj_all.at[:, pl.ds(low, proj_all.shape[1] - low)], mixed_all)
    last = len(pairs) - 1
    hop_send = (4, 13, 5)

    def chain(a, step, middle=None):
        buf = pairs[a]
        right = buf.at[jnp.maximum(z - step, 0) * CORES + core]
        left = buf.at[jnp.minimum(z + step, depth - 1) * CORES + core]
        up = jnp.minimum(z + 1, depth - 1) * CORES + core
        down = jnp.maximum(z - 1, 0) * CORES + core
        for way, ref, peer, ok, within in (
            (0, right, up, jnp.logical_and(z - step >= 0, z + 1 < depth),
             jnp.logical_and(z >= 1, z + 2 < depth)),
            (1, left, down, jnp.logical_and(z + step < depth, z >= 1),
             jnp.logical_and(z >= 2, z + 1 < depth)),
        ):
            if middle is not None:
                ok = jnp.logical_and(ok, within if middle else jnp.logical_not(within))

            @pl.when(ok)
            def _(way=way, ref=ref, peer=peer):
                c = remote(ref, ref, z_send.at[a], z_recv.at[a, way, step], "sp", peer)
                c.start()

    partner = z * CORES + (1 - core)

    def across(a, step, way, start=True, also=None):
        ok = z - step >= 0 if way == 0 else z + step < depth
        if also is not None:
            ok = jnp.logical_and(ok, also)
        zz = jnp.maximum(z - step, 0) if way == 0 else jnp.minimum(z + step, depth - 1)
        ref = pairs[a].at[zz * CORES + (core if start else 1 - core)]
        sem = c_recv.at[last + way * depth + step if a == last else a]

        @pl.when(ok)
        def _():
            c = remote(ref, ref, o_send.at[hop_send[a]], sem, "sp", partner)
            c.start() if start else c.wait_recv()

    def advance(a, step, also=None, middle=None):
        for way in range(2):
            if way == 0:
                ok, origin, to = z - 1 - step >= 0, jnp.maximum(z - 1 - step, 0), z + 1
                goes_on, within = z + 1 < depth, jnp.logical_and(z >= 1, z + 2 < depth)
            else:
                ok, origin, to = z + 1 + step < depth, jnp.minimum(z + 1 + step, depth - 1), z - 1
                goes_on, within = z >= 1, jnp.logical_and(z >= 2, z + 1 < depth)
            ref = pairs[a].at[origin * CORES + core]
            peer = jnp.clip(to, 0, depth - 1) * CORES + core
            if also is not None:
                ok = jnp.logical_and(ok, also)
            if middle is not None:
                ok = jnp.logical_and(ok, within if middle else jnp.logical_not(within))

            @pl.when(ok)
            def _(way=way, ref=ref, peer=peer, goes_on=goes_on):
                remote(ref, ref, z_send.at[a], z_recv.at[a, way, step],
                       "sp", lax.rem(mine + 1, groups)).wait_recv()
                if step + 1 < depth - 1:
                    @pl.when(goes_on)
                    def _():
                        remote(ref, ref, z_send.at[a], z_recv.at[a, way, step + 1],
                               "sp", peer).start()

            across(a, step + 1, way, also=ok)

    def settle(a):
        for at in range(depth):
            hops = (min(at + 1, depth - 1) if at + 1 < depth else 0) + (
                min(depth - at, depth - 1) if at else 0)

            @pl.when(z == at)
            def _(hops=hops):
                all_sent(pairs[a].at[pl.ds(0, hops)], z_send.at[a])

        all_sent(pairs[a].at[pl.ds(0, depth)], o_send.at[hop_send[a]])

    def collected(step):
        for way in range(2):
            if step or not way:
                across(last, step, way, start=False)

    loads[4].wait()
    for a in range(last):
        chain(a, 0)
        across(a, 0, 0)
    share_out(1, 0)
    share_out(0, 1)
    loads[3].wait()
    prev_copy = send(
        states_ref.at[pl.ds(toks - 8, 8)], prev_in, p_send, p_recv, "sp", lax.rem(mine + 1, groups))

    loads[2].wait()
    act, branch_slope = gelu_parts(gate_ref[...].astype(F32))
    states = states_ref[...]
    act_ref[...] = act
    slope_ref[...] = branch_slope * states
    mixed_all[mine] = (act * states).astype(BF)
    chain(last, 0, middle=False)
    across(last, 0, 0)
    rows = lax.broadcasted_iota(jnp.int32, (toks, toks), 0)
    cols = lax.broadcasted_iota(jnp.int32, (toks, toks), 1)
    eye = jnp.where(rows == cols, 1.0, 0.0).astype(BF)
    fine = cot_turned.shape[2]
    cot_turned[...] = contract_rows(cot_ref[...], eye).astype(BF).reshape(cot_turned.shape)
    cot_mine[col] = cot_turned[:, col]
    share_out(1, 1)
    for p in range(1, parts):
        send(cot_turned.at[:, tile[p]], cot_mine.at[col], o_send.at[6], m_recv.at[0], "tp", tile[p])
    share_out(0, 2)
    share_out(0, 3)
    for a in range(2):
        relay(a, 0)
        relay(a, 1)
    queue = [(0, d) for d in range(2, groups)] + [(1, d) for d in range(2, groups)]
    ahead = queue[2:]

    def pump(count):
        for _ in range(count):
            for _ in range(2):
                if ahead:
                    share_out(*ahead.pop(0))
            for _ in range(2):
                if queue:
                    relay(*queue.pop(0))

    pump(half)

    first = [lax.div(mine, half) * half, (1 - lax.div(mine, half)) * half]

    def forward(h):
        landed(0, h)
        at = pl.ds(first[h], half)
        data = rows_x[at].reshape(rows_half, model)
        pre_gate = jnp.dot(data, wg[...].reshape(model, units), preferred_element_type=F32)
        pre_up = jnp.dot(data, wu[...].reshape(model, units), preferred_element_type=F32)
        active, slope = silu_parts(pre_gate)
        hid_ref[at] = (active * pre_up).astype(BF).reshape(half, room, units)
        active_ref[h] = active
        lean_ref[h] = pre_up * slope

    def hidden_grads(h):
        landed(1, h)
        at = pl.ds(first[h], half)
        grad_hidden = contract_cols(rows_c[at].reshape(rows_half, model), wd[...])
        gpg_ref[at] = (grad_hidden * lean_ref[h]).astype(BF).reshape(half, room, units)
        gpu_ref[at] = (grad_hidden * active_ref[h]).astype(BF).reshape(half, room, units)

    share_copies = [[None, None] for _ in range(groups)]

    def reduce_out(d, i, p):
        g = group[d]
        share_copies[d][i] = send(
            terms.at[p, g], shares.at[i, g], o_send.at[7], s_recv.at[d, i], "tp", tile[1 + d % 2])

    def input_grads(h, order):
        at = pl.ds(first[h], half)
        gate_part = gpg_ref[at].reshape(rows_half, units)
        up_part = gpu_ref[at].reshape(rows_half, units)
        for p in (3, 1, 2, 0):
            term = contract_cols(gate_part, wg[:, tile[p]].reshape(width, units))
            term = term + contract_cols(up_part, wu[:, tile[p]].reshape(width, units))
            terms[p, at] = term.astype(BF).reshape(half, room, width)
            for d in order:
                if p == 3:
                    reduce_out(d, 0, p)
                elif p == 1 + d % 2:
                    reduce_out(d, 1, p)

    def pass_on(d):
        g, far_tile = group[d], 2 - d % 2
        share_copies[d][0].wait_recv()
        passed[g] = (terms[far_tile, g].astype(F32) + shares[0, g].astype(F32)).astype(BF)
        send(passed.at[g], shares.at[2, g], o_send.at[7], s_recv.at[d, 1], "tp", tile[far_tile])

    def bring_back(d):
        g = group[d]
        all_here(shares.at[pl.ds(1, 2), g], s_recv.at[d, 1])
        total = terms[0, g].astype(F32) + shares[1, g].astype(F32) + shares[2, g].astype(F32)
        if d == 0:
            back[mine] = total.astype(BF)
        else:
            summed[d] = total.astype(BF)
            send(summed.at[d], back.at[mine], o_send.at[8], m_recv.at[1], "sp", g)

    for i in (6, 7, 8):
        loads[i].wait()
    forward(0)
    advance(0, 0)
    pump(1)
    advance(1, 0)
    chain(last, 0, middle=True)
    forward(1)

    hidden_grads(0)
    pump(1)
    order = list(range(2, half)) + [1, 0] + list(range(half, groups))
    input_grads(0, order[:half])
    hidden_grads(1)
    for d in order[:2]:
        pass_on(d)
    input_grads(1, order[half:])
    for d in order[2:half]:
        pass_on(d)

    loads[5].wait()
    prev_copy.wait_recv()
    decays = jnp.exp(decay_ref[...])
    line = lax.broadcasted_iota(jnp.int32, decays.shape, 0)
    before = jnp.where(mine > 0, prev_in[7:8, :], 0.0)
    past_ref[...] = decays * jnp.where(line == 0, before, pltpu.roll(states_ref[...], 1, 0))
    span = jnp.where(line < toks - 1, pltpu.roll(decays, toks - 1, 0), 1.0)
    k, level = 1, 0
    while k < toks:
        inside = line < toks - k
        levels[level] = jnp.where(inside, span, 0.0)
        span = span * jnp.where(inside, pltpu.roll(span, toks - k, 0), 1.0)
        k *= 2
        level += 1
    span_ref[...] = span
    head = decays[0:1]

    for step in range(1, depth - 2):
        advance(0, step)
    late = order[half:]
    for d in order:
        if late:
            pass_on(late.pop(0))
        bring_back(d)
    advance(last, 0, middle=True)
    all_here(cot_turned.at[:, pl.ds(0, parts - 1)], m_recv.at[0])
    total = cot_mine[...].reshape(width, toks).astype(F32)
    all_here(back.at[pl.ds(0, groups - 1)], m_recv.at[1])
    total = total + contract_rows(back[...].reshape(size, width), picked_ref[...])
    flipped[:, col] = total.astype(BF).reshape(groups, fine, toks)

    def plane_part(buf, owner, rows, first_sem, to, relayed=0):
        part = buf.at[pl.ds(rows * half, half), owner]
        return send(
            part, part, o_send.at[first_sem // 3 + 8], m_recv.at[first_sem + relayed], "tp", tile[to])

    def plane_start(buf, first_sem):
        copies = [plane_part(buf, col, p - 1, first_sem, p, p) for p in (1, 2)]
        for p in (1, 2):
            plane_part(buf, col, 2 - p, first_sem, p)
        return copies

    def plane_relay(buf, copies, first_sem):
        for p in (1, 2):
            copies[p - 1].wait_recv()
            plane_part(buf, tile[p], p - 1, first_sem, 3 - p)

    grad_copies = plane_start(flipped, 3)
    for d in range(1, groups):
        send(flipped.at[group[d], col], blocks.at[mine, col], o_send.at[11], m_recv.at[2], "sp", group[d])
    blocks[mine, col] = flipped[mine, col]
    for step in range(1, depth - 2):
        advance(1, step)
    advance(last, 0, middle=False)
    plane_relay(flipped, grad_copies, 3)
    all_here(blocks.at[pl.ds(0, groups - 1), 0], m_recv.at[2])
    plane_copies = plane_start(blocks, 6)
    advance(0, depth - 2)
    for step in range(1, depth - 2):
        advance(last, step, inner)
    all_here(flipped.at[:, pl.ds(0, 2)], m_recv.at[3])
    advance(1, depth - 2)
    for a in range(last):
        all_here(pairs[a].at[pl.ds(0, depth)], c_recv.at[a])
    grad_mixed = contract_rows(flipped[...].reshape(model, toks), proj_all[...].reshape(model, chans))
    ggate_ref[...] = (grad_mixed * slope_ref[...]).astype(BF)
    local = grad_mixed * act_ref[...]
    k, level = 1, 0
    while k < toks:
        local = local + levels[level] * pltpu.roll(local, toks - k, 0)
        k *= 2
        level += 1
    carry_own[0:1] = span_ref[0:1, :] * head
    carry_own[1:2] = local[0:1] * head
    for d in range(1, groups):
        send(carry_own, carry_in.at[d - 1], o_send.at[12], m_recv.at[9], "sp", lax.rem(mine + d, groups))
    plane_relay(blocks, plane_copies, 6)
    for step in range(1, depth - 2):
        advance(last, step, jnp.logical_not(inner))
    for step in range(depth - 1):
        collected(step)
    all_here(blocks.at[:, pl.ds(0, 2)], m_recv.at[6])
    advance(last, depth - 2)
    high = blocks.shape[1] * blocks.shape[2]

    def out_part(t):
        return jnp.dot(blocks[t].reshape(high, toks), mixed_all[t], preferred_element_type=F32)

    near_part = out_part(group[0])
    for d in range(1, groups - CORES):
        near_part = near_part + out_part(group[d])
    outp_ref[...] = near_part
    all_here(carry_in, m_recv.at[9])
    carried = jnp.zeros((1, chans), F32)
    for ahead in range(groups - 1, 0, -1):
        got = carry_in[groups - ahead - 1]
        carried = jnp.where(mine + ahead < groups, got[1:2] + got[0:1] * carried, carried)
    grad_in = local + span_ref[...] * carried
    gin_ref[...] = grad_in
    gdecay_ref[...] = (grad_in * past_ref[...]).astype(BF)
    collected(depth - 1)
    far_part = out_part(group[groups - CORES])
    for d in range(groups - CORES + 1, groups):
        far_part = far_part + out_part(group[d])
    outp_ref[...] += far_part
    for a in range(last + 1):
        settle(a)
    for a in range(2):
        all_sent(rows_x.at[pl.ds(0, groups - 1), :, pl.ds(0, width)], o_send.at[a])
        all_sent(rows_x.at[pl.ds(0, groups * 3 // parts)], o_send.at[2 + a])
    all_sent(cot_turned.at[:, pl.ds(0, parts - 1)], o_send.at[6])
    all_sent(rows_x.at[pl.ds(0, groups * 3 // parts)], o_send.at[7])
    all_sent(back.at[pl.ds(0, groups - 1)], o_send.at[8])
    for i in (9, 10):
        all_sent(flipped.at[:, pl.ds(0, 3)], o_send.at[i])
    all_sent(blocks.at[pl.ds(0, groups - 1), 0], o_send.at[11])
    all_sent(carry_in, o_send.at[12])
    prev_copy.wait_send()


def plane_shards(
    moe_input, cotangent, routes, route_weights, gate_branch, log_decay, states,
    w_gate, w_up, w_down, out_proj,
):
    groups, parts = lax.axis_size("sp"), lax.axis_size("tp")
    tok_rows, picks = routes.shape
    width = moe_input.shape[1]
    model = width * parts
    units = w_gate.shape[2]
    chans = states.shape[1]
    room = tok_rows * picks * 5 // (4 * groups)
    room = (room + 7) // 8 * 8
    depth = groups // CORES
    high = out_proj.shape[0]
    fine = high // parts
    doublings = (tok_rows - 1).bit_length()
    vmem = pl.BlockSpec(memory_space=pltpu.VMEM)
    hbm = pl.BlockSpec(memory_space=pltpu.HBM)
    dma = pltpu.SemaphoreType.DMA

    def run(*refs):
        plane_kernel(groups, parts, room, *refs)

    def buf(*shape, kind=BF):
        return pltpu.VMEM(shape, kind)

    def split(weight):
        return weight.reshape(1, groups, parts, fine, units)

    outs = pl.pallas_call(
        run,
        out_shape=[
            jax.ShapeDtypeStruct((groups, room, model), BF),
            jax.ShapeDtypeStruct((groups, room, model), BF),
            jax.ShapeDtypeStruct((groups, room, units), BF),
            jax.ShapeDtypeStruct((groups, room, units), BF),
            jax.ShapeDtypeStruct((groups, room, units), BF),
            jax.ShapeDtypeStruct((high, chans), F32),
            jax.ShapeDtypeStruct((tok_rows, chans), BF),
            jax.ShapeDtypeStruct((tok_rows, chans), BF),
            jax.ShapeDtypeStruct((tok_rows, chans), F32),
        ],
        in_specs=[hbm] * 11,
        out_specs=[vmem] * 9,
        scratch_shapes=[
            buf(picks, tok_rows, kind=jnp.int32), buf(picks, tok_rows, kind=F32),
            buf(tok_rows, width), buf(tok_rows, width), buf(tok_rows, chans),
            buf(tok_rows, chans, kind=F32), buf(tok_rows, chans, kind=F32),
            buf(groups, parts, fine, units), buf(groups, parts, fine, units), buf(units, model),
            buf(groups, room, width), buf(groups, room, width), buf(groups * room, tok_rows),
            buf(groups, high, chans), buf(groups, tok_rows, chans),
            buf(tok_rows, chans, kind=F32), buf(tok_rows, chans, kind=F32),
            buf(2, groups // 2 * room, units, kind=F32), buf(2, groups // 2 * room, units, kind=F32),
            buf(parts, groups, room, width), buf(parts - 1, groups, room, width),
            buf(groups, room, width), buf(groups, room, width), buf(groups, room, width),
            buf(groups // parts, parts, fine, tok_rows), buf(parts, groups // parts, fine, tok_rows),
            buf(groups, parts, fine, tok_rows), buf(groups, parts, fine, tok_rows),
            buf(doublings, tok_rows, chans, kind=F32), buf(tok_rows, chans, kind=F32),
            buf(tok_rows, chans, kind=F32),
            buf(2, chans, kind=F32), buf(groups - 1, 2, chans, kind=F32), buf(8, chans, kind=F32),
        ]
        + [dma((14,)), dma((2, groups - 1)), dma((2, groups)), dma((2, 2)), dma((groups, 2))]
        + [dma((10,)), dma((3,)), dma((3, 2, depth - 1)), dma((2 + 2 * depth,))]
        + [dma(()), dma(()), dma((11,))],
        compiler_params=pltpu.CompilerParams(
            collective_id=0, has_side_effects=True, vmem_limit_bytes=40 * 1024 * 1024),
        name="backward",
    )(
        *(pltpu.with_memory_space_constraint(a, pltpu.HBM) for a in (
            routes.T, route_weights.T, moe_input, cotangent, gate_branch, states, log_decay, out_proj,
            split(w_gate), split(w_up), w_down)),
    )
    rx, rc = (out.reshape(groups * room, model) for out in outs[:2])
    grads = (out.reshape(groups * room, units) for out in outs[2:5])
    return finish(rx, rc, *grads, *outs[5:])


def solution(mesh):
    groups, parts = mesh.shape["sp"], mesh.shape["tp"]
    plane = parts == 4 and groups % parts == 0 and groups & (groups - 1) == 0
    return jax.shard_map(
        plane_shards if plane else shards,
        mesh=mesh,
        in_specs=(
            P("sp", "tp"), P("sp", "tp"), P("sp", None), P("sp", None), P("sp", "tp"),
            P("sp", "tp"), P("sp", "tp"), P("sp", None, "tp"), P("sp", None, "tp"),
            P("sp", "tp", None), P("sp", "tp"),
        ),
        out_specs=(
            P("sp", None, "tp"), P("sp", None, "tp"), P("sp", "tp", None), P("sp", "tp"),
            P("sp", "tp"), P("sp", "tp"), P("sp", "tp"),
        ),
        check_vma=False,
    )
```
